32 devices in a mesh: sp: 8 (over z, x), dp: 4 (over y, core).
Axes of the slice: x: 2, y: 2, z: 4, core: 2. Of those that a mesh axis runs over, the one named last changes fastest.
Arguments:
- residual_in: bfloat16 [4, 1024, 2048], P('dp', 'sp'), may hold values from -6 to 6
- ssm_input: bfloat16 [4, 1024, 2048], P('dp', 'sp'), may hold values from -6 to 6
- state_b: bfloat16 [4, 1024, 2048], P('dp', 'sp'), may hold values from -6 to 6
- state_c: bfloat16 [4, 1024, 2048], P('dp', 'sp'), may hold values from -6 to 6
- step_raw: bfloat16 [4, 1024, 64], P('dp', 'sp'), may hold values from -4 to 3
- gate_input: bfloat16 [4, 1024, 2048], P('dp', 'sp'), may hold values from -6 to 6
- conv_x: float32 [7, 2048], P(None, 'sp'), may hold values from -2 to 2
- conv_b: float32 [7, 2048], P(None, 'sp'), may hold values from -2 to 2
- conv_c: float32 [7, 2048], P(None, 'sp'), may hold values from -2 to 2
- decay_rate: float32 [2, 32], P(None, 'sp'), may hold values from 0 to 1, as said below
- mix_gain: float32 [2048], replicated, may hold values from 0.1 to 1.9
- out_weight: bfloat16 [2048, 2048], P('dp'), may hold values from -0.125 to 0.125
- ffn_gain: float32 [2048], replicated, may hold values from 0.1 to 1.9
- routing: int32 [4, 1024, 4], P('dp', 'sp'), may hold values from 0 to 31, all different within a row; in each aligned block of 128 rows (0 to 127, 128 to 255, ..., all dimensions but the last counted through in order) at most 32 rows name the same one
- route_weight: float32 [4, 1024, 4], P('dp', 'sp'), may hold values from 0.1 to 0.6
- gate_w: bfloat16 [32, 2048, 1024], P(('sp', 'dp')), may hold values from -60 to 60
- up_w: bfloat16 [32, 2048, 1024], P(('sp', 'dp')), may hold values from -60 to 60
- down_w: bfloat16 [32, 1024, 2048], P(('sp', 'dp')), may hold values from -0.1875 to 0.1875
Outputs:
- block_out: bfloat16 [4, 1024, 2048], P('dp', 'sp')
The draws below stay inside these ranges and needn't reach their ends.
Inputs may be any that keep to these rules, and one draw needn't show every extreme that they name: `routing`: each row names 4 different experts; within the rows of one device no expert is named by more than 32 rows, a bound that some block reaches. `decay_rate`: Positive.
All inputs are finite; a program needn't handle non-finite values.
Results may differ from the reference program's by a relative error of at most 0.0082.
Values may be sent and summed in bfloat16 or wider, within the bound.
A program may use at most 128 MiB of HBM per device.

```python
import math
import jax
import jax.numpy as jnp
import numpy as np
from jax import lax

D = 2048
HEADS = 32
HEAD_DIM = 64
GROUPS = 16
STATE = 128
CONV = 7
BLOCK = 128
NORM_GROUPS = 4
FF = 1024
TOPK = 4
TOK_DEV = 128
SEQ_LEN = 1024
SEQS = 4
EXPERTS = 32
CAP = 32


def draw_step_raw(key, part):
    noise_key, level_key = jax.random.split(key)
    noise = jnp.clip(jax.random.normal(noise_key, (SEQS, SEQ_LEN, 2 * HEADS), jnp.float32), -3.0, 3.0) * 0.5
    levels = jax.random.uniform(level_key, (SEQS, SEQ_LEN // TOK_DEV, 1, 2 * HEADS), jnp.float32, -2.0, 1.0)
    levels = jnp.broadcast_to(levels, (SEQS, SEQ_LEN // TOK_DEV, TOK_DEV, 2 * HEADS)).reshape(SEQS, SEQ_LEN, 2 * HEADS)
    return (noise + levels).astype(jnp.bfloat16)


def draw_decay_rate(key, part):
    pick_key, fast_key, slow_key = jax.random.split(key, 3)
    share = 0.5
    quick = jax.random.bernoulli(pick_key, share, (2, HEADS))
    fast_rate = jnp.exp(jax.random.uniform(fast_key, (2, HEADS), jnp.float32, math.log(0.02), math.log(0.2)))
    slow_rate = jnp.exp(jax.random.uniform(slow_key, (2, HEADS), jnp.float32, math.log(0.05), 0.0)) / SEQ_LEN
    return jnp.where(quick, fast_rate, slow_rate)


def expert_matrix(key):
    base_key, pick_key = jax.random.split(key)
    values = jnp.clip(jax.random.normal(base_key, (EXPERTS, D, FF), jnp.float32), -6.0, 6.0) * D ** (-0.5)
    values = values * 1.0
    return values


def draw_gate_w(key, part):
    return expert_matrix(jax.random.fold_in(key, 11)).astype(jnp.bfloat16)


def draw_up_w(key, part):
    return expert_matrix(jax.random.fold_in(key, 12)).astype(jnp.bfloat16)


def steps_of(rng, shape, pieces, least, top_value):
    level, own = 1.0, jax.random.fold_in(rng, 6)
    for axis_at, blocks in pieces:
        steps = jnp.exp(jax.random.uniform(jax.random.fold_in(own, axis_at), (blocks,), jnp.float32, least / len(pieces), top_value / len(pieces)))
        level = level * jnp.repeat(steps, shape[axis_at] // blocks).reshape([-1 if axis == axis_at else 1 for axis in range(len(shape))])
    return level


def shared_out(own_key, own, number, rows, amount, top, reach, slope):
    sequence = jax.random.permutation(own_key, amount)
    crowded, common = portions_of(amount, rows * top, reach, slope, True), portions_of(amount, rows * top, reach, slope, False)
    places = jnp.arange(amount)

    def named(tallies, turn):
        used = int((tallies > 0).sum())
        fixed = max(1, used // 4)
        moved = fixed + (places - fixed + turn * (used - fixed)) % max(1, amount - fixed)
        return jnp.zeros((amount,), jnp.int32).at[sequence[jnp.where(places < fixed, places, moved)]].set(jnp.asarray(tallies, jnp.int32))

    tallies = jnp.where(number % 4 == 0, named(crowded, number // 4), named(common, number - number // 4 - 1))
    mixed = jax.random.permutation(jax.random.fold_in(own, 3), amount)
    donor, receiver = mixed[0:amount // 2 * 2:2], mixed[1:amount // 2 * 2:2]
    room = jnp.minimum(tallies[donor] - 1, reach - tallies[receiver]) // 2
    room = jnp.where((donor == sequence[0]) | (receiver == sequence[0]) | (tallies[receiver] == 0), 0, jnp.maximum(room, 0))
    moved = jax.random.randint(jax.random.fold_in(own, 4), (amount // 2,), 0, 1 << 20) % (room + 1)
    tallies = tallies.at[donor].add(-moved).at[receiver].add(moved)
    items = jnp.searchsorted(jnp.cumsum(tallies), jnp.arange(rows * top), side="right").astype(jnp.int32)
    listing = items.reshape(top, rows).T
    listing = listing[jax.random.permutation(jax.random.fold_in(own, 1), rows)]
    turn = jax.random.randint(jax.random.fold_in(own, 2), (rows, 1), 0, top)
    return jnp.take_along_axis(listing, (jnp.arange(top)[None, :] + turn) % top, axis=1)


def portions_of(count, total, limit, skew, full):
    weights = [(1 << 20) // math.isqrt(rank ** skew) + 1 for rank in range(1, count + 1)]
    largest = limit if full else min(limit, max(-(-total // count), total * weights[0] // sum(weights)))
    least = 1 if total - largest >= count - 1 else 0
    holding, spare = [largest] + [least] * (count - 1), total - largest - least * (count - 1)
    while spare > 0:
        movable = [i for i in range(1, count) if holding[i] < largest] or [i for i in range(1, count) if holding[i] < limit]
        mass, budget = sum([weights[i] for i in movable]), spare
        for i in movable:
            addition = min(limit - holding[i], max(1, budget * weights[i] // mass), spare)
            holding[i] = holding[i] + addition
            spare = spare - addition
    return np.array(holding)


def gaussian(own_key, shape, width, limit, shards=(), kind=jnp.bfloat16):
    level = steps_of(own_key, shape, shards, -0.22, 0.18) if shards else 1.0
    values = jax.random.normal(own_key, shape, jnp.float32) * width * level
    return jnp.minimum(jnp.maximum(values, -limit), limit).astype(kind)


def setup_inputs(seed: int = 0) -> dict:
    key_of = jax.random.split(jax.random.key(seed), 19)
    residual_in = gaussian(key_of[0], (SEQS, SEQ_LEN, D), 1.0, 6.0, ((0, 4), (1, 8)))
    ssm_input = gaussian(key_of[1], (SEQS, SEQ_LEN, D), 1.0, 6.0, ((0, 4), (1, 8)))
    state_b = gaussian(key_of[2], (SEQS, SEQ_LEN, GROUPS * STATE), 1.0, 6.0, ((0, 4), (1, 8)))
    state_c = gaussian(key_of[3], (SEQS, SEQ_LEN, GROUPS * STATE), 1.0, 6.0, ((0, 4), (1, 8)))
    step_raw = draw_step_raw(jax.random.fold_in(key_of[18], 71), 0)
    gate_input = gaussian(key_of[5], (SEQS, SEQ_LEN, D), 1.0, 6.0, ((0, 4), (1, 8)))
    conv_x = gaussian(key_of[6], (CONV, D), CONV ** -0.5, 2.0, ((1, 8),), jnp.float32)
    conv_b = gaussian(key_of[7], (CONV, GROUPS * STATE), CONV ** -0.5, 2.0, ((1, 8),), jnp.float32)
    conv_c = gaussian(key_of[8], (CONV, GROUPS * STATE), CONV ** -0.5, 2.0, ((1, 8),), jnp.float32)
    decay_rate = draw_decay_rate(jax.random.fold_in(key_of[18], 71), 0)
    mix_gain = jnp.clip(1.0 + 0.18 * jax.random.normal(key_of[10], (D,), jnp.float32), 0.1, 1.9)
    out_weight = gaussian(key_of[11], (D, D), D ** -0.5, 0.125, ((0, 4),))
    ffn_gain = jnp.clip(1.0 + 0.18 * jax.random.normal(key_of[12], (D,), jnp.float32), 0.1, 1.9)
    routing_keys = jax.random.split(jax.random.fold_in(key_of[13], 1), SEQS * SEQ_LEN // TOK_DEV)
    routing_turns = jax.random.permutation(jax.random.fold_in(key_of[13], 3), SEQS * SEQ_LEN // TOK_DEV)
    routing = jax.vmap(lambda own, number: shared_out(jax.random.fold_in(key_of[13], 2), own, number, TOK_DEV, EXPERTS, TOPK, CAP, 2))(routing_keys, routing_turns).reshape((SEQS, SEQ_LEN, TOPK))
    route_weight = jnp.clip(0.1 + 0.5 * jax.random.uniform(key_of[14], (SEQS, SEQ_LEN, TOPK), jnp.float32) ** steps_of(key_of[14], (SEQS, SEQ_LEN, TOPK), ((0, 4), (1, 8)), -0.2, 0.2), 0.1, 0.6)
    gate_w = draw_gate_w(jax.random.fold_in(key_of[18], 71), 0)
    up_w = draw_up_w(jax.random.fold_in(key_of[18], 71), 0)
    down_w = gaussian(key_of[17], (EXPERTS, FF, D), FF ** -0.5, 0.1875, ((0, 32),))
    return {"residual_in": residual_in, "ssm_input": ssm_input, "state_b": state_b, "state_c": state_c, "step_raw": step_raw, "gate_input": gate_input, "conv_x": conv_x, "conv_b": conv_b, "conv_c": conv_c, "decay_rate": decay_rate, "mix_gain": mix_gain, "out_weight": out_weight, "ffn_gain": ffn_gain, "routing": routing, "route_weight": route_weight, "gate_w": gate_w, "up_w": up_w, "down_w": down_w}


highest = lax.Precision.HIGHEST
epsilon = 1e-05
clamp_limit = 7.0
sigmoid_slope = 1.702
group_rows = 256

def centred_conv(values, taps):
    half_width = taps.shape[0] // 2
    padded = jnp.pad(values, ((half_width, half_width), (0, 0)))
    total = jnp.zeros_like(values)
    for offset in range(taps.shape[0]):
        total = total + padded[offset:offset + values.shape[0]] * taps[offset]
    return total

def ssd_direction(signal, step_size, rates, write_map, read_map):
    length = signal.shape[0]
    head_count = signal.shape[1]
    head_width = signal.shape[2]
    group_count = write_map.shape[1]
    state_width = write_map.shape[2]
    per_group = head_count // group_count
    blocks = length // BLOCK
    scaled = (signal * step_size[..., None]).reshape(blocks, BLOCK, group_count, per_group, head_width)
    cumulative = jnp.cumsum((-step_size * rates).reshape(blocks, BLOCK, group_count, per_group), axis=1)
    write_block = write_map.reshape(blocks, BLOCK, group_count, state_width)
    read_block = read_map.reshape(blocks, BLOCK, group_count, state_width)
    spread = cumulative[:, :, None] - cumulative[:, None]
    lower_mask = (lax.iota(jnp.int32, BLOCK)[:, None] >= lax.iota(jnp.int32, BLOCK)[None, :])[None, :, :, None, None]
    weight_in = jnp.exp(jnp.where(lower_mask, spread, -jnp.inf))
    intersect = jnp.einsum('clgn,csgn->clsg', read_block, write_block, precision=highest)
    inside = jnp.einsum('clsgk,csgkp->clgkp', intersect[..., None] * weight_in, scaled, precision=highest)
    to_end = jnp.exp(cumulative[:, -1:] - cumulative)
    states = jnp.einsum('csgn,csgkp->cgkpn', write_block, scaled * to_end[..., None], precision=highest)
    carry_decay = jnp.exp(cumulative[:, -1])

    def advance(running, block_pair):
        block_state, factor = block_pair
        return (factor[..., None, None] * running + block_state, running)
    initial = jnp.zeros((group_count, per_group, head_width, state_width), jnp.float32)
    _, entering = lax.scan(advance, initial, (states, carry_decay))
    carried = jnp.einsum('clgn,cgkpn->clgkp', read_block, entering, precision=highest) * jnp.exp(cumulative)[..., None]
    return (inside + carried).reshape(length, head_count, head_width)

def both_ways(signal, steps_fwd, steps_bwd, rates, write_map, read_map):
    forward = ssd_direction(signal, steps_fwd, rates[0], write_map, read_map)
    backward = ssd_direction(jnp.flip(signal, 0), jnp.flip(steps_bwd, 0), rates[1], jnp.flip(write_map, 0), jnp.flip(read_map, 0))
    return forward + jnp.flip(backward, 0)

def scale_rows(values, gains):
    return values * lax.rsqrt(lax.optimization_barrier(jnp.mean(values * values, axis=-1, keepdims=True)) + epsilon) * gains

def group_scale(values, gains):
    shaped = values.reshape(values.shape[:-1] + (NORM_GROUPS, values.shape[-1] // NORM_GROUPS))
    shaped = shaped * lax.rsqrt(lax.optimization_barrier(jnp.mean(shaped * shaped, axis=-1, keepdims=True)) + epsilon)
    return shaped.reshape(values.shape) * gains

def expert_apply(rows, gate_mat, up_mat, down_mat):
    gate_value = jnp.minimum(jnp.dot(rows, gate_mat, preferred_element_type=jnp.float32), clamp_limit)
    up_value = jnp.clip(jnp.dot(rows, up_mat, preferred_element_type=jnp.float32), -clamp_limit, clamp_limit)
    active = ((up_value + 1.0) * gate_value * jax.nn.sigmoid(sigmoid_slope * gate_value)).astype(jnp.bfloat16)
    return jnp.dot(active, down_mat, preferred_element_type=jnp.float32).astype(jnp.bfloat16)

def reference(residual_in, ssm_input, state_b, state_c, step_raw, gate_input, conv_x, conv_b, conv_c, decay_rate, mix_gain, out_weight, ffn_gain, routing, route_weight, gate_w, up_w, down_w):

    def mix_sequence(operands):
        signal_in, write_in, read_in, step_in = operands
        length = signal_in.shape[0]
        signal = jax.nn.silu(centred_conv(signal_in.astype(jnp.float32), conv_x)).reshape(length, HEADS, HEAD_DIM)
        write_map = jax.nn.silu(centred_conv(write_in.astype(jnp.float32), conv_b)).reshape(length, GROUPS, STATE)
        read_map = jax.nn.silu(centred_conv(read_in.astype(jnp.float32), conv_c)).reshape(length, GROUPS, STATE)
        step_pair = jax.nn.softplus(step_in.astype(jnp.float32).reshape(length, HEADS, 2))
        result = both_ways(signal, step_pair[..., 0], step_pair[..., 1], decay_rate, write_map, read_map)
        return result.reshape(length, D).astype(jnp.bfloat16)
    mixed_heads = lax.map(mix_sequence, (ssm_input, state_b, state_c, step_raw))
    gated = mixed_heads.astype(jnp.float32) * jax.nn.silu(gate_input.astype(jnp.float32))
    mixed = group_scale(gated, mix_gain).astype(jnp.bfloat16).reshape(-1, D)
    stream = residual_in.reshape(-1, D).astype(jnp.float32) + jnp.dot(mixed, out_weight, preferred_element_type=jnp.float32)
    ffn_input = scale_rows(stream, ffn_gain).astype(jnp.bfloat16)
    flat_expert = routing.reshape(-1).astype(jnp.int32)
    assigned = flat_expert.shape[0]
    flat_token = lax.iota(jnp.int32, assigned) // TOPK
    flat_weight = route_weight.reshape(-1)
    order = jnp.argsort(flat_expert, stable=True).astype(jnp.int32)
    sorted_expert = flat_expert[order]
    counts = jnp.bincount(flat_expert, length=EXPERTS).astype(jnp.int32)
    padded = (counts + group_rows - 1) // group_rows * group_rows
    group_start = jnp.cumsum(counts).astype(jnp.int32) - counts
    padded_end = jnp.cumsum(padded).astype(jnp.int32)
    padded_start = padded_end - padded
    target = padded_start[sorted_expert] + (lax.iota(jnp.int32, assigned) - group_start[sorted_expert])
    block_count = (assigned + EXPERTS * (group_rows - 1)) // group_rows + 1
    total_rows = block_count * group_rows
    row_token = jnp.zeros((total_rows,), jnp.int32).at[target].set(flat_token[order])
    row_weight = jnp.zeros((total_rows,), jnp.float32).at[target].set(flat_weight[order])
    block_expert = jnp.minimum(jnp.searchsorted(padded_end, lax.iota(jnp.int32, block_count) * group_rows, side='right'), EXPERTS - 1).astype(jnp.int32)

    def run_block(routed, block_pair):
        block_index, expert_id = block_pair
        rows_token = lax.dynamic_slice_in_dim(row_token, block_index * group_rows, group_rows)
        rows_weight = lax.dynamic_slice_in_dim(row_weight, block_index * group_rows, group_rows)
        answer = expert_apply(ffn_input[rows_token], gate_w[expert_id], up_w[expert_id], down_w[expert_id])
        return (routed.at[rows_token].add(answer.astype(jnp.float32) * rows_weight[:, None]), None)
    routed_init = jnp.zeros(stream.shape, jnp.float32)
    routed, _ = lax.scan(run_block, routed_init, (lax.iota(jnp.int32, block_count), block_expert))
    return (stream + routed).astype(jnp.bfloat16).reshape(SEQS, SEQ_LEN, D)
```

```python
import functools

import jax
import jax.numpy as jnp
from jax import lax
from jax.experimental import pallas as pl
from jax.experimental.pallas import tpu as pltpu
from jax.sharding import PartitionSpec as P

HEAD_DIM = 64
STATE = 128
BLOCK = 128
NORM_GROUPS = 4
MESH = pl.DeviceIdType.MESH

highest = lax.Precision.HIGHEST
epsilon = 1e-05
clamp_limit = 7.0
sigmoid_slope = 1.702


def greet(peers):
    barrier = pltpu.get_barrier_semaphore()
    for peer in peers:
        pl.semaphore_signal(barrier, inc=1, device_id=peer, device_id_type=MESH)
    pl.semaphore_wait(barrier, len(peers))


def to_heads_kernel(n, *refs):
    srcs, dsts = refs[:4], refs[4:8]
    bounce, step_bounce, send, recv, local = refs[8:]
    me = lax.axis_index("sp")
    rows = srcs[0].shape[0]
    width = dsts[0].shape[1]
    peers = [lax.rem(me + i, n) for i in range(1, n)]
    greet([{"sp": peer} for peer in peers])
    copies = []
    mine = pl.ds(pl.multiple_of(me * rows, rows), rows)
    for i, peer in enumerate(peers):
        for k in range(4):
            if k < 3:
                part = srcs[k].at[:, pl.ds(pl.multiple_of(peer * width, width), width)]
                there = dsts[k].at[mine, :]
            else:
                part = srcs[k]
                there = dsts[k].at[mine, :]
            copy = pltpu.make_async_remote_copy(
                src_ref=part,
                dst_ref=there,
                send_sem=send.at[i, k],
                recv_sem=recv.at[i, k],
                device_id={"sp": peer},
                device_id_type=MESH,
            )
            copy.start()
            copies.append(copy)
    own = [srcs[k].at[:, pl.ds(pl.multiple_of(me * width, width), width)] for k in range(3)]
    own.append(srcs[3])
    slots = [bounce.at[k] for k in range(3)] + [step_bounce]
    first = [pltpu.make_async_copy(own[k], slots[k], local.at[0, k]) for k in range(4)]
    second = [
        pltpu.make_async_copy(slots[k], dsts[k].at[mine, :], local.at[1, k]) for k in range(4)
    ]
    for k in range(4):
        first[k].start()
    for k in range(4):
        first[k].wait()
        second[k].start()
    for k in range(4):
        second[k].wait()
    for copy in copies:
        copy.wait()


def to_heads(n, arrays, steps):
    rows, full = arrays[0].shape
    width = full // n
    wide = jax.ShapeDtypeStruct((rows * n, width), arrays[0].dtype)
    step_out = jax.ShapeDtypeStruct((rows * n, steps.shape[1]), steps.dtype)
    anywhere = pl.BlockSpec(memory_space=pl.ANY)
    return pl.pallas_call(
        functools.partial(to_heads_kernel, n),
        out_shape=(wide, wide, wide, step_out),
        in_specs=[anywhere] * 4,
        out_specs=(anywhere,) * 4,
        scratch_shapes=[
            pltpu.VMEM((3, rows, width), arrays[0].dtype),
            pltpu.VMEM(steps.shape, steps.dtype),
            pltpu.SemaphoreType.DMA((n - 1, 4)),
            pltpu.SemaphoreType.DMA((n - 1, 4)),
            pltpu.SemaphoreType.DMA((2, 4)),
        ],
        compiler_params=pltpu.CompilerParams(collective_id=1, has_side_effects=True),
        name="to_heads",
    )(*arrays, steps)


def to_tokens_kernel(n, src, dst, bounce, send, recv, local):
    me = lax.axis_index("sp")
    rows = dst.shape[0]
    width = src.shape[1]
    peers = [lax.rem(me + i, n) for i in range(1, n)]
    greet([{"sp": peer} for peer in peers])
    there = dst.at[:, pl.ds(pl.multiple_of(me * width, width), width)]
    copies = []
    for i, peer in enumerate(peers):
        copy = pltpu.make_async_remote_copy(
            src_ref=src.at[pl.ds(pl.multiple_of(peer * rows, rows), rows), :],
            dst_ref=there,
            send_sem=send.at[i],
            recv_sem=recv.at[i],
            device_id={"sp": peer},
            device_id_type=MESH,
        )
        copy.start()
        copies.append(copy)
    first = pltpu.make_async_copy(
        src.at[pl.ds(pl.multiple_of(me * rows, rows), rows), :], bounce, local.at[0]
    )
    first.start()
    first.wait()
    second = pltpu.make_async_copy(bounce, there, local.at[1])
    second.start()
    second.wait()
    for copy in copies:
        copy.wait()


def to_tokens(n, heads):
    length, width = heads.shape
    rows = length // n
    anywhere = pl.BlockSpec(memory_space=pl.ANY)
    return pl.pallas_call(
        functools.partial(to_tokens_kernel, n),
        out_shape=jax.ShapeDtypeStruct((rows, n * width), heads.dtype),
        in_specs=[anywhere],
        out_specs=anywhere,
        scratch_shapes=[
            pltpu.VMEM((rows, width), heads.dtype),
            pltpu.SemaphoreType.DMA((n - 1,)),
            pltpu.SemaphoreType.DMA((n - 1,)),
            pltpu.SemaphoreType.DMA((2,)),
        ],
        compiler_params=pltpu.CompilerParams(collective_id=2, has_side_effects=True),
        name="to_tokens",
    )(heads)


def plane_order(z, planes, s):
    below, above = z, planes - 1 - z
    both = jnp.minimum(below, above)
    near = (s + 1) // 2
    from_below = jnp.where(s <= 2 * both, s % 2, jnp.where(below > above, 1, 0))
    hops = jnp.where(s <= 2 * both, near, s - both)
    return hops, from_below, z + hops * (1 - 2 * from_below)


def experts_kernel(
    planes, inner, dp_count, top, x_ref, info_ref, gate_hbm, up_hbm, down_hbm, out_ref,
    gate, up, down, tok, infos, rows_out, rows_in, made, back, high, low, active, part, part_in,
    wsem, isend, irecv, zsend, zrecv, dsend, drecv, rsend, rrecv, psend, precv, local,
):
    f32, bf16 = jnp.float32, jnp.bfloat16
    near = inner * dp_count
    tokens, width = x_ref.shape
    cap = rows_out.shape[2]
    sp, dp = lax.axis_index("sp"), lax.axis_index("dp")
    z, x = sp // inner, lax.rem(sp, inner)
    me = x * dp_count + dp

    def place(p):
        return {"sp": z * inner + p // dp_count, "dp": lax.rem(p, dp_count)}

    def plane(other):
        return {"sp": other * inner + x, "dp": dp}

    barrier = pltpu.get_barrier_semaphore()

    def call(i, carry):
        peer = lax.rem(me + i, near)
        pl.semaphore_signal(barrier, inc=1, device_id=place(peer), device_id_type=MESH)
        return carry

    lax.fori_loop(1, near, call, 0)
    for i in range(1, planes):
        pl.semaphore_signal(
            barrier, inc=1, device_id=plane(lax.rem(z + i, planes)), device_id_type=MESH
        )
    loads = [
        pltpu.make_async_copy(gate_hbm.at[0], gate, wsem.at[0]),
        pltpu.make_async_copy(up_hbm.at[0], up, wsem.at[1]),
        pltpu.make_async_copy(down_hbm.at[0], down, wsem.at[2]),
    ]
    for load in loads:
        load.start()
    pl.semaphore_wait(barrier, near - 1 + planes - 1)

    def tell(i):
        return pltpu.make_async_remote_copy(
            src_ref=info_ref,
            dst_ref=infos.at[z],
            send_sem=isend.at[i],
            recv_sem=irecv.at[i],
            device_id=plane(lax.rem(z + i, planes)),
            device_id_type=MESH,
        )

    for i in range(1, planes):
        tell(i).start()

    def along(src, block, step, way):
        return pltpu.make_async_remote_copy(
            src_ref=src,
            dst_ref=tok.at[block],
            send_sem=zsend.at[way, step],
            recv_sem=zrecv.at[way, step],
            device_id=plane(z + 1 - 2 * way),
            device_id_type=MESH,
        )

    up_open, down_open = z < planes - 1, z > 0

    @pl.when(up_open)
    def _():
        along(x_ref, z, 0, 0).start()

    @pl.when(down_open)
    def _():
        along(x_ref, z, 0, 1).start()

    ti = lax.broadcasted_iota(jnp.int32, (tokens, tokens), 0)
    tj = lax.broadcasted_iota(jnp.int32, (tokens, tokens), 1)
    earlier = jnp.where(ti < tj, 1.0, 0.0).astype(bf16)
    expert = (z * near + lax.broadcasted_iota(jnp.int32, (near, tokens), 0)).astype(f32)
    place_in = lax.broadcasted_iota(jnp.int32, (near, cap, tokens), 1).astype(f32)

    def send_rows(block, i):
        peer = lax.rem(me + i, near)
        return pltpu.make_async_remote_copy(
            src_ref=rows_out.at[block, peer],
            dst_ref=rows_in.at[block, me],
            send_sem=dsend.at[block, i],
            recv_sem=drecv.at[block, i],
            device_id=place(peer),
            device_id_type=MESH,
        )

    def keep_rows(block):
        return pltpu.make_async_copy(
            rows_out.at[block, me], rows_in.at[block, me], local.at[0, block]
        )

    def send_back(block, i):
        peer = lax.rem(me + i, near)
        return pltpu.make_async_remote_copy(
            src_ref=made.at[block, peer],
            dst_ref=back.at[block, me],
            send_sem=rsend.at[block, i],
            recv_sem=rrecv.at[block, i],
            device_id=place(peer),
            device_id_type=MESH,
        )

    def keep_back(block):
        return pltpu.make_async_copy(made.at[block, me], back.at[block, me], local.at[1, block])

    def each(what):
        def one(i, carry):
            what(i)
            return carry

        lax.fori_loop(1, near, one, 0)

    def dispatch(block, values, info):
        names, weights = info[0:top, :], info[top : 2 * top, :]
        named, weight = None, None
        for k in range(top):
            hit = names[k : k + 1, :] == expert
            one = jnp.where(hit, 1.0, 0.0)
            share = jnp.where(hit, weights[k : k + 1, :], 0.0)
            named = one if named is None else named + one
            weight = share if weight is None else weight + share
        slot = jnp.dot(named.astype(bf16), earlier, preferred_element_type=f32)
        slot = jnp.where(named > 0.5, slot, -1.0)
        pick = slot[:, None, :] == place_in
        rough = weight.astype(bf16).astype(f32)
        rest = weight - rough

        def table(v):
            return jnp.where(pick, v, 0.0).reshape(near * cap, tokens).astype(bf16)

        high[block] = table(rough[:, None, :])
        low[block] = table(rest[:, None, :])
        select = table(jnp.ones((near, 1, tokens), f32))
        chunk = 512
        for at in range(0, width, chunk):
            rows = jnp.dot(select, values[:, at : at + chunk], preferred_element_type=f32)
            rows_out[block, :, :, at : at + chunk] = rows.astype(bf16).reshape(near, cap, chunk)
        each(lambda i: send_rows(block, i).start())
        keep_rows(block).start()

    def arrive(s):
        hops, from_below, block = plane_order(z, planes, s)
        way = 1 - from_below
        along(tok.at[block], block, hops - 1, way).wait_recv()
        onward = jnp.where(from_below == 1, z + 1, z - 1)

        @pl.when((onward >= 0) & (onward < planes))
        def _():
            along(tok.at[block], block, hops, way).start()

        source = lax.rem(z - block + planes, planes)
        tell(source).wait_recv()
        dispatch(block, tok[block], infos[block])
        return block

    hidden = gate.shape[1]
    flat = near * cap

    def serve(block):
        keep_rows(block).wait()
        each(lambda i: send_rows(block, i).wait_recv())
        tile = 256

        def lift(n, carry):
            cols = pl.ds(pl.multiple_of(n * tile, tile), tile)
            rows = rows_in[block].reshape(flat, width)
            g = jnp.minimum(jnp.dot(rows, gate[:, cols], preferred_element_type=f32), clamp_limit)
            u = jnp.dot(rows, up[:, cols], preferred_element_type=f32)
            u = jnp.clip(u, -clamp_limit, clamp_limit)
            active[:, cols] = ((u + 1.0) * g * jax.nn.sigmoid(sigmoid_slope * g)).astype(bf16)
            return carry

        lax.fori_loop(0, hidden // tile, lift, 0)

        def lower(n, carry):
            cols = pl.ds(pl.multiple_of(n * tile, tile), tile)
            y = jnp.dot(active[...], down[:, cols], preferred_element_type=f32)
            made[block, :, :, cols] = y.astype(bf16).reshape(near, cap, tile)
            return carry

        lax.fori_loop(0, width // tile, lower, 0)

    def give(block):
        each(lambda i: send_back(block, i).start())
        keep_back(block).start()

    def gathered(block, at, chunk):
        rows = back[block, :, :, at : at + chunk].reshape(flat, chunk)
        dims = (((0,), (0,)), ((), ()))
        return lax.dot_general(
            high[block], rows, dims, preferred_element_type=f32
        ) + lax.dot_general(low[block], rows, dims, preferred_element_type=f32)

    def send_part(block, i):
        return pltpu.make_async_remote_copy(
            src_ref=part.at[block],
            dst_ref=part_in.at[z],
            send_sem=psend.at[i],
            recv_sem=precv.at[i],
            device_id=plane(block),
            device_id_type=MESH,
        )

    def landed(block):
        keep_back(block).wait()
        each(lambda i: send_back(block, i).wait_recv())

    def collect(block):
        landed(block)
        chunk = 512
        for at in range(0, width, chunk):
            part[block, :, at : at + chunk] = gathered(block, at, chunk).astype(bf16)
        send_part(block, lax.rem(block - z + planes, planes)).start()

    blocks = [z]
    dispatch(z, x_ref[...], info_ref[...])
    served = 0
    for s in range(1, planes):
        blocks.append(arrive(s))
        if s == planes - 2:
            for load in loads:
                load.wait()
            serve(blocks[0])
            served = 1
    if not served:
        for load in loads:
            load.wait()
        serve(blocks[0])
    for s in range(1, planes):
        serve(blocks[s])
        give(blocks[s])
    give(blocks[0])
    for s in range(1, planes):
        collect(blocks[s])
    landed(z)
    chunk = 512
    for at in range(0, width, chunk):
        out_ref[:, at : at + chunk] = gathered(z, at, chunk)
    for i in range(1, planes):
        send_part(lax.rem(z + i, planes), i).wait_recv()
        out_ref[...] += part_in[lax.rem(z - i + planes, planes)].astype(f32)

    for i in range(1, planes):
        tell(i).wait_send()
        send_part(lax.rem(z + i, planes), i).wait_send()
    for block in range(planes):
        each(lambda i: send_rows(block, i).wait_send())
        each(lambda i: send_back(block, i).wait_send())

    @pl.when(up_open)
    def _():
        along(x_ref, z, 0, 0).wait_send()

    @pl.when(down_open)
    def _():
        along(x_ref, z, 0, 1).wait_send()

    for step in range(1, planes):

        @pl.when(up_open & (z - step >= 0))
        def _():
            along(tok.at[z], z, step, 0).wait_send()

        @pl.when(down_open & (z + step < planes))
        def _():
            along(tok.at[z], z, step, 1).wait_send()


def experts(planes, inner, dp_count, cap, top, tokens_in, info, gate_w, up_w, down_w):
    near = inner * dp_count
    tokens, width = tokens_in.shape
    hidden = gate_w.shape[2]
    bf16, f32 = jnp.bfloat16, jnp.float32
    anywhere = pl.BlockSpec(memory_space=pl.ANY)
    inside = pl.BlockSpec(memory_space=pltpu.VMEM)
    dma = pltpu.SemaphoreType.DMA
    rows = pltpu.VMEM((planes, near, cap, width), bf16)
    table = pltpu.VMEM((planes, near * cap, tokens), bf16)
    blocks = pltpu.VMEM((planes, tokens, width), bf16)
    return pl.pallas_call(
        functools.partial(experts_kernel, planes, inner, dp_count, top),
        out_shape=jax.ShapeDtypeStruct((tokens, width), f32),
        in_specs=[inside, inside, anywhere, anywhere, anywhere],
        out_specs=inside,
        scratch_shapes=[
            pltpu.VMEM((width, hidden), bf16),
            pltpu.VMEM((width, hidden), bf16),
            pltpu.VMEM((hidden, width), bf16),
            blocks,
            pltpu.VMEM((planes,) + info.shape, f32),
            rows, rows, rows, rows, table, table,
            pltpu.VMEM((near * cap, hidden), bf16),
            blocks, blocks,
            dma((3,)), dma((planes,)), dma((planes,)), dma((2, planes)), dma((2, planes)),
            dma((planes, near)), dma((planes, near)), dma((planes, near)), dma((planes, near)),
            dma((planes,)), dma((planes,)), dma((2, planes)),
        ],
        compiler_params=pltpu.CompilerParams(
            collective_id=3, has_side_effects=True, vmem_limit_bytes=60 * 1024 * 1024
        ),
        cost_estimate=pl.CostEstimate(flops=10**11, bytes_accessed=10**8, transcendentals=0),
        name="experts",
    )(tokens_in, info, gate_w, up_w, down_w)


def mixer_kernel(
    x_ref, b_ref, c_ref, tx_ref, tb_ref, tc_ref, st_ref, stt_ref, rate_ref, ratet_ref,
    o_ref, pad, reads, inside_ref, fade_f, fade_b, sums, carry,
):
    length = x_ref.shape[0]
    lanes = x_ref.shape[1]
    blocks = length // BLOCK
    per_group = st_ref.shape[2] // 2
    taps = tx_ref.shape[0]
    half = taps // 2
    f32, bf16 = jnp.float32, jnp.bfloat16
    for k, ref in enumerate((x_ref, b_ref, c_ref)):
        pad[k, 0:8, :] = jnp.zeros((8, lanes), f32)
        pad[k, length + 8 : length + 16, :] = jnp.zeros((8, lanes), f32)
        pad[k, 8 : length + 8, :] = ref[...].astype(f32)

    def conv(k, taps_ref, base):
        total = None
        for j in range(taps):
            term = pad[k, base + 8 - half + j : base + 8 - half + j + BLOCK, :] * taps_ref[j : j + 1, :]
            total = term if total is None else total + term
        return total * jax.nn.sigmoid(total)

    def softplus(v):
        return jnp.maximum(v, 0.0) + jnp.log(1.0 + jnp.exp(-jnp.abs(v)))

    li = lax.broadcasted_iota(jnp.int32, (BLOCK, BLOCK), 0)
    si = lax.broadcasted_iota(jnp.int32, (BLOCK, BLOCK), 1)
    at_or_after = li >= si
    lower = jnp.where(at_or_after, 1.0, 0.0).astype(f32)
    upper = jnp.where(si >= li, 1.0, 0.0).astype(f32)
    lane_head = lax.broadcasted_iota(jnp.int32, (1, lanes), 1) // HEAD_DIM

    def spread_heads(columns):
        out = columns[0]
        for h in range(1, per_group):
            out = jnp.where(lane_head == h, columns[h], out)
        return jnp.broadcast_to(out, (out.shape[0], lanes))

    for c in range(blocks):
        base = c * BLOCK
        rows = slice(base, base + BLOCK)
        x = conv(0, tx_ref, base)
        write = conv(1, tb_ref, base).astype(bf16)
        read = conv(2, tc_ref, base).astype(bf16)
        reads[rows, :] = read
        dt = softplus(st_ref[0, rows, :])
        dtt = softplus(stt_ref[0, :, rows])
        a = dt * rate_ref[0]
        at = dtt * ratet_ref[0]
        inc = jnp.dot(lower, a, precision=highest, preferred_element_type=f32)
        inct = jnp.dot(at, upper, precision=highest, preferred_element_type=f32)
        exc = inc - a
        exct = inct - at
        tot = inc[BLOCK - 1 : BLOCK, :]
        scores = lax.dot_general(
            read, write, (((1,), (1,)), ((), ())), preferred_element_type=f32
        )
        inside = None
        xb = x.astype(bf16)
        for h in range(per_group):
            f, b = 2 * h, 2 * h + 1
            power = jnp.where(
                at_or_after,
                inct[f : f + 1, :] - inc[:, f : f + 1],
                exc[:, b : b + 1] - exct[b : b + 1, :],
            )
            df, db = dtt[f : f + 1, :], dtt[b : b + 1, :]
            scale = jnp.where(li > si, df, jnp.where(li == si, df + db, db))
            weights = (scores * jnp.exp(power) * scale).astype(bf16)
            xh = jnp.where(lane_head == h, x, 0.0).astype(bf16)
            term = jnp.dot(weights, xh, preferred_element_type=f32)
            inside = term if inside is None else inside + term
        inside_ref[rows, :] = inside
        heads = range(per_group)
        fwd = [inc[:, 2 * h : 2 * h + 1] for h in heads]
        bwd = [exc[:, 2 * h + 1 : 2 * h + 2] for h in heads]
        tot_f = [tot[:, 2 * h : 2 * h + 1] for h in heads]
        tot_b = [tot[:, 2 * h + 1 : 2 * h + 2] for h in heads]
        wf = spread_heads([dt[:, 2 * h : 2 * h + 1] * jnp.exp(fwd[h] - tot_f[h]) for h in heads])
        wb = spread_heads([dt[:, 2 * h + 1 : 2 * h + 2] * jnp.exp(-bwd[h]) for h in heads])
        fade_f[rows, :] = spread_heads([jnp.exp(-fwd[h]) for h in heads])
        fade_b[rows, :] = spread_heads([jnp.exp(bwd[h] - tot_b[h]) for h in heads])
        both = jnp.concatenate([(x * wf).astype(bf16), (x * wb).astype(bf16)], axis=1)
        sums[c] = lax.dot_general(
            write, both, (((0,), (0,)), ((), ())), preferred_element_type=f32
        )
        carry[c : c + 1, :] = jnp.concatenate(
            [
                spread_heads([jnp.exp(-tot_f[h]) for h in heads]),
                spread_heads([jnp.exp(-tot_b[h]) for h in heads]),
            ],
            axis=1,
        )

    state = jnp.zeros((sums.shape[1], lanes), f32)
    for c in range(blocks):
        own = sums[c, :, 0:lanes]
        sums[c, :, 0:lanes] = state
        state = carry[c : c + 1, 0:lanes] * state + own
    state = jnp.zeros((sums.shape[1], lanes), f32)
    for c in reversed(range(blocks)):
        own = sums[c, :, lanes : 2 * lanes]
        sums[c, :, lanes : 2 * lanes] = state
        state = carry[c : c + 1, lanes : 2 * lanes] * state + own
    for c in range(blocks):
        rows = slice(c * BLOCK, (c + 1) * BLOCK)
        moved = jnp.dot(reads[rows, :], sums[c].astype(bf16), preferred_element_type=f32)
        total = (
            inside_ref[rows, :]
            + moved[:, 0:lanes] * fade_f[rows, :]
            + moved[:, lanes : 2 * lanes] * fade_b[rows, :]
        )
        o_ref[rows, :] = total.astype(o_ref.dtype)


def mixer(signal, write, read, conv_x, conv_b, conv_c, steps, rates):
    length, width = signal.shape
    groups = write.shape[1] // STATE
    lanes = width // groups
    columns = steps.shape[1] // groups
    taps = conv_x.shape[0]
    blocks = length // BLOCK
    st = steps.astype(jnp.float32).reshape(length, groups, columns).transpose(1, 0, 2)
    stt = st.transpose(0, 2, 1)
    rate = rates.T.reshape(groups, 1, columns)
    ratet = rates.T.reshape(groups, columns, 1)
    wide = pl.BlockSpec((length, lanes), lambda g: (0, g))
    state = pl.BlockSpec((length, STATE), lambda g: (0, g))
    tap_x = pl.BlockSpec((taps, lanes), lambda g: (0, g))
    tap_s = pl.BlockSpec((taps, STATE), lambda g: (0, g))

    def whole(shape):
        return pl.BlockSpec((1,) + shape, lambda g: (g, 0, 0))

    f32 = jnp.float32
    return pl.pallas_call(
        mixer_kernel,
        grid=(groups,),
        out_shape=jax.ShapeDtypeStruct((length, width), jnp.bfloat16),
        in_specs=[
            wide, state, state, tap_x, tap_s, tap_s,
            whole((length, columns)), whole((columns, length)),
            whole((1, columns)), whole((columns, 1)),
        ],
        out_specs=wide,
        scratch_shapes=[
            pltpu.VMEM((3, length + 16, lanes), f32),
            pltpu.VMEM((length, STATE), jnp.bfloat16),
            pltpu.VMEM((length, lanes), f32),
            pltpu.VMEM((length, lanes), f32),
            pltpu.VMEM((length, lanes), f32),
            pltpu.VMEM((blocks, STATE, 2 * lanes), f32),
            pltpu.VMEM((blocks, 2 * lanes), f32),
        ],
        compiler_params=pltpu.CompilerParams(vmem_limit_bytes=40 * 1024 * 1024),
        cost_estimate=pl.CostEstimate(
            flops=40 * 10**9, bytes_accessed=4 * length * width * 2, transcendentals=0
        ),
        name="mixer",
    )(signal, write, read, conv_x, conv_b, conv_c, st, stt, rate, ratet)


def scale_rows(values, gains):
    return values * lax.rsqrt(jnp.mean(values * values, axis=-1, keepdims=True) + epsilon) * gains


def group_scale(values, gains):
    shaped = values.reshape(values.shape[:-1] + (NORM_GROUPS, values.shape[-1] // NORM_GROUPS))
    shaped = shaped * lax.rsqrt(jnp.mean(shaped * shaped, axis=-1, keepdims=True) + epsilon)
    return shaped.reshape(values.shape) * gains


def gather_rows(weight, count):
    parts = {0: weight}
    step = count // 2
    while step >= 1:
        pairs = [(d, d ^ step) for d in range(count)]
        for offset, block in list(parts.items()):
            parts[offset ^ step] = lax.ppermute(block, "dp", pairs)
        step //= 2
    return parts


def per_device(
    residual_in, ssm_input, state_b, state_c, step_raw, gate_input, conv_x, conv_b, conv_c,
    decay_rate, mix_gain, out_weight, ffn_gain, routing, route_weight, gate_w, up_w, down_w,
):
    sp_count = lax.axis_size("sp")
    dp_count = lax.axis_size("dp")
    bf16, f32 = jnp.bfloat16, jnp.float32
    parts = gather_rows(out_weight, dp_count)
    signal, write, read, steps = to_heads(
        sp_count, (ssm_input[0], state_b[0], state_c[0]), step_raw[0]
    )
    columns = steps.shape[1] // sp_count
    steps = lax.dynamic_slice_in_dim(steps, lax.axis_index("sp") * columns, columns, axis=1)
    mixed_heads = mixer(signal, write, read, conv_x, conv_b, conv_c, steps, decay_rate)
    mixed_tokens = to_tokens(sp_count, mixed_heads)

    token_count = residual_in.shape[1]
    model_width = residual_in.shape[2]
    gated = mixed_tokens.astype(f32) * jax.nn.silu(gate_input[0].astype(f32))
    mixed = group_scale(gated, mix_gain).astype(bf16)
    depth = out_weight.shape[0]
    me = lax.axis_index("dp")
    stream = residual_in[0].astype(f32)
    for offset, block in parts.items():
        piece = lax.dynamic_slice_in_dim(mixed, (me ^ offset) * depth, depth, axis=1)
        stream = stream + jnp.dot(piece, block, preferred_element_type=f32)
    ffn_input = scale_rows(stream, ffn_gain).astype(bf16)

    top_count = routing.shape[2]
    inner = dp_count // 2
    planes = sp_count // inner
    capacity = 4 * token_count * top_count // (2 * sp_count * dp_count)
    info = jnp.concatenate([routing[0].T.astype(f32), route_weight[0].T], axis=0)
    routed = experts(
        planes, inner, dp_count, capacity, top_count, ffn_input, info, gate_w, up_w, down_w
    )
    return (stream + routed).astype(bf16)[None]


def solution(mesh):
    return jax.shard_map(
        per_device,
        mesh=mesh,
        in_specs=(
            P("dp", "sp", None),
            P("dp", "sp", None),
            P("dp", "sp", None),
            P("dp", "sp", None),
            P("dp", "sp", None),
            P("dp", "sp", None),
            P(None, "sp"),
            P(None, "sp"),
            P(None, "sp"),
            P(None, "sp"),
            P(),
            P("dp", None),
            P(),
            P("dp", "sp", None),
            P("dp", "sp", None),
            P(("sp", "dp"), None, None),
            P(("sp", "dp"), None, None),
            P(("sp", "dp"), None, None),
        ),
        out_specs=P("dp", "sp", None),
        check_vma=False,
    )
```

```python
import functools

import jax
import jax.numpy as jnp
from jax import lax
from jax.experimental import pallas as pl
from jax.experimental.pallas import tpu as pltpu
from jax.sharding import PartitionSpec as P

HEAD_DIM = 64
STATE = 128
BLOCK = 128
NORM_GROUPS = 4
MESH = pl.DeviceIdType.MESH

highest = lax.Precision.HIGHEST
epsilon = 1e-05
clamp_limit = 7.0
sigmoid_slope = 1.702


def greet(peers):
    barrier = pltpu.get_barrier_semaphore()
    for peer in peers:
        pl.semaphore_signal(barrier, inc=1, device_id=peer, device_id_type=MESH)
    pl.semaphore_wait(barrier, len(peers))


def plane_order(z, planes, s):
    below, above = z, planes - 1 - z
    both = jnp.minimum(below, above)
    near = (s + 1) // 2
    from_below = jnp.where(s <= 2 * both, s % 2, jnp.where(below > above, 1, 0))
    hops = jnp.where(s <= 2 * both, near, s - both)
    return hops, from_below, z + hops * (1 - 2 * from_below)


def experts_kernel(
    planes, inner, dp_count, top, x_ref, info_ref, gate_hbm, up_hbm, down_hbm, out_ref,
    gate, up, down, tok, infos, rows_out, rows_in, made, back, high, low, active, part, part_in,
    wsem, isend, irecv, zsend, zrecv, dsend, drecv, rsend, rrecv, psend, precv, local,
):
    f32, bf16 = jnp.float32, jnp.bfloat16
    near = inner * dp_count
    tokens, width = x_ref.shape
    cap = rows_out.shape[2]
    sp, dp = lax.axis_index("sp"), lax.axis_index("dp")
    z, x = sp // inner, lax.rem(sp, inner)
    me = x * dp_count + dp

    def place(p):
        return {"sp": z * inner + p // dp_count, "dp": lax.rem(p, dp_count)}

    def plane(other):
        return {"sp": other * inner + x, "dp": dp}

    barrier = pltpu.get_barrier_semaphore()

    def call(i, carry):
        peer = lax.rem(me + i, near)
        pl.semaphore_signal(barrier, inc=1, device_id=place(peer), device_id_type=MESH)
        return carry

    lax.fori_loop(1, near, call, 0)
    for i in range(1, planes):
        pl.semaphore_signal(
            barrier, inc=1, device_id=plane(lax.rem(z + i, planes)), device_id_type=MESH
        )
    loads = [
        pltpu.make_async_copy(gate_hbm.at[0], gate, wsem.at[0]),
        pltpu.make_async_copy(up_hbm.at[0], up, wsem.at[1]),
        pltpu.make_async_copy(down_hbm.at[0], down, wsem.at[2]),
    ]
    for load in loads:
        load.start()
    pl.semaphore_wait(barrier, near - 1 + planes - 1)

    def tell(i):
        return pltpu.make_async_remote_copy(
            src_ref=info_ref,
            dst_ref=infos.at[z],
            send_sem=isend.at[i],
            recv_sem=irecv.at[i],
            device_id=plane(lax.rem(z + i, planes)),
            device_id_type=MESH,
        )

    for i in range(1, planes):
        tell(i).start()

    def along(src, block, step, way):
        return pltpu.make_async_remote_copy(
            src_ref=src,
            dst_ref=tok.at[block],
            send_sem=zsend.at[way, step],
            recv_sem=zrecv.at[way, step],
            device_id=plane(z + 1 - 2 * way),
            device_id_type=MESH,
        )

    up_open, down_open = z < planes - 1, z > 0

    @pl.when(up_open)
    def _():
        along(x_ref, z, 0, 0).start()

    @pl.when(down_open)
    def _():
        along(x_ref, z, 0, 1).start()

    ti = lax.broadcasted_iota(jnp.int32, (tokens, tokens), 0)
    tj = lax.broadcasted_iota(jnp.int32, (tokens, tokens), 1)
    earlier = jnp.where(ti < tj, 1.0, 0.0).astype(bf16)
    expert = (z * near + lax.broadcasted_iota(jnp.int32, (near, tokens), 0)).astype(f32)
    place_in = lax.broadcasted_iota(jnp.int32, (near, cap, tokens), 1).astype(f32)

    def send_rows(block, i):
        peer = lax.rem(me + i, near)
        return pltpu.make_async_remote_copy(
            src_ref=rows_out.at[block, peer],
            dst_ref=rows_in.at[block, me],
            send_sem=dsend.at[block, i],
            recv_sem=drecv.at[block, i],
            device_id=place(peer),
            device_id_type=MESH,
        )

    def keep_rows(block):
        return pltpu.make_async_copy(
            rows_out.at[block, me], rows_in.at[block, me], local.at[0, block]
        )

    def send_back(block, i):
        peer = lax.rem(me + i, near)
        return pltpu.make_async_remote_copy(
            src_ref=made.at[block, peer],
            dst_ref=back.at[block, me],
            send_sem=rsend.at[block, i],
            recv_sem=rrecv.at[block, i],
            device_id=place(peer),
            device_id_type=MESH,
        )

    def keep_back(block):
        return pltpu.make_async_copy(made.at[block, me], back.at[block, me], local.at[1, block])

    def each(what):
        def one(i, carry):
            what(i)
            return carry

        lax.fori_loop(1, near, one, 0)

    def dispatch(block, values, info):
        names, weights = info[0:top, :], info[top : 2 * top, :]
        named, weight = None, None
        for k in range(top):
            hit = names[k : k + 1, :] == expert
            one = jnp.where(hit, 1.0, 0.0)
            share = jnp.where(hit, weights[k : k + 1, :], 0.0)
            named = one if named is None else named + one
            weight = share if weight is None else weight + share
        slot = jnp.dot(named.astype(bf16), earlier, preferred_element_type=f32)
        slot = jnp.where(named > 0.5, slot, -1.0)
        pick = slot[:, None, :] == place_in
        rough = weight.astype(bf16).astype(f32)
        rest = weight - rough

        def table(v):
            return jnp.where(pick, v, 0.0).reshape(near * cap, tokens).astype(bf16)

        high[block] = table(rough[:, None, :])
        low[block] = table(rest[:, None, :])
        select = table(jnp.ones((near, 1, tokens), f32))
        chunk = 512
        for at in range(0, width, chunk):
            rows = jnp.dot(select, values[:, at : at + chunk], preferred_element_type=f32)
            rows_out[block, :, :, at : at + chunk] = rows.astype(bf16).reshape(near, cap, chunk)
        each(lambda i: send_rows(block, i).start())
        keep_rows(block).start()

    def arrive(s):
        hops, from_below, block = plane_order(z, planes, s)
        way = 1 - from_below
        along(tok.at[block], block, hops - 1, way).wait_recv()
        onward = jnp.where(from_below == 1, z + 1, z - 1)

        @pl.when((onward >= 0) & (onward < planes))
        def _():
            along(tok.at[block], block, hops, way).start()

        source = lax.rem(z - block + planes, planes)
        tell(source).wait_recv()
        dispatch(block, tok[block], infos[block])
        return block

    hidden = gate.shape[1]
    flat = near * cap

    def serve(block):
        keep_rows(block).wait()
        each(lambda i: send_rows(block, i).wait_recv())
        tile = 256

        def lift(n, carry):
            cols = pl.ds(pl.multiple_of(n * tile, tile), tile)
            rows = rows_in[block].reshape(flat, width)
            g = jnp.minimum(jnp.dot(rows, gate[:, cols], preferred_element_type=f32), clamp_limit)
            u = jnp.dot(rows, up[:, cols], preferred_element_type=f32)
            u = jnp.clip(u, -clamp_limit, clamp_limit)
            active[:, cols] = ((u + 1.0) * g * jax.nn.sigmoid(sigmoid_slope * g)).astype(bf16)
            return carry

        lax.fori_loop(0, hidden // tile, lift, 0)

        def lower(n, carry):
            cols = pl.ds(pl.multiple_of(n * tile, tile), tile)
            y = jnp.dot(active[...], down[:, cols], preferred_element_type=f32)
            made[block, :, :, cols] = y.astype(bf16).reshape(near, cap, tile)
            return carry

        lax.fori_loop(0, width // tile, lower, 0)

    def give(block):
        each(lambda i: send_back(block, i).start())
        keep_back(block).start()

    def gathered(block, at, chunk):
        rows = back[block, :, :, at : at + chunk].reshape(flat, chunk)
        dims = (((0,), (0,)), ((), ()))
        return lax.dot_general(
            high[block], rows, dims, preferred_element_type=f32
        ) + lax.dot_general(low[block], rows, dims, preferred_element_type=f32)

    def send_part(block, i):
        return pltpu.make_async_remote_copy(
            src_ref=part.at[block],
            dst_ref=part_in.at[z],
            send_sem=psend.at[i],
            recv_sem=precv.at[i],
            device_id=plane(block),
            device_id_type=MESH,
        )

    def landed(block):
        keep_back(block).wait()
        each(lambda i: send_back(block, i).wait_recv())

    def collect(block):
        landed(block)
        chunk = 512
        for at in range(0, width, chunk):
            part[block, :, at : at + chunk] = gathered(block, at, chunk).astype(bf16)
        send_part(block, lax.rem(block - z + planes, planes)).start()

    blocks = [z]
    dispatch(z, x_ref[...], info_ref[...])
    served = 0
    for s in range(1, planes):
        blocks.append(arrive(s))
        if s == planes - 2:
            for load in loads:
                load.wait()
            serve(blocks[0])
            served = 1
    if not served:
        for load in loads:
            load.wait()
        serve(blocks[0])
    for s in range(1, planes):
        serve(blocks[s])
        give(blocks[s])
    give(blocks[0])
    for s in range(1, planes):
        collect(blocks[s])
    landed(z)
    chunk = 512
    for at in range(0, width, chunk):
        out_ref[:, at : at + chunk] = gathered(z, at, chunk)
    for i in range(1, planes):
        send_part(lax.rem(z + i, planes), i).wait_recv()
        out_ref[...] += part_in[lax.rem(z - i + planes, planes)].astype(f32)

    for i in range(1, planes):
        tell(i).wait_send()
        send_part(lax.rem(z + i, planes), i).wait_send()
    for block in range(planes):
        each(lambda i: send_rows(block, i).wait_send())
        each(lambda i: send_back(block, i).wait_send())

    @pl.when(up_open)
    def _():
        along(x_ref, z, 0, 0).wait_send()

    @pl.when(down_open)
    def _():
        along(x_ref, z, 0, 1).wait_send()

    for step in range(1, planes):

        @pl.when(up_open & (z - step >= 0))
        def _():
            along(tok.at[z], z, step, 0).wait_send()

        @pl.when(down_open & (z + step < planes))
        def _():
            along(tok.at[z], z, step, 1).wait_send()


def experts(planes, inner, dp_count, cap, top, tokens_in, info, gate_w, up_w, down_w):
    near = inner * dp_count
    tokens, width = tokens_in.shape
    hidden = gate_w.shape[2]
    bf16, f32 = jnp.bfloat16, jnp.float32
    anywhere = pl.BlockSpec(memory_space=pl.ANY)
    inside = pl.BlockSpec(memory_space=pltpu.VMEM)
    dma = pltpu.SemaphoreType.DMA
    rows = pltpu.VMEM((planes, near, cap, width), bf16)
    table = pltpu.VMEM((planes, near * cap, tokens), bf16)
    blocks = pltpu.VMEM((planes, tokens, width), bf16)
    return pl.pallas_call(
        functools.partial(experts_kernel, planes, inner, dp_count, top),
        out_shape=jax.ShapeDtypeStruct((tokens, width), f32),
        in_specs=[inside, inside, anywhere, anywhere, anywhere],
        out_specs=inside,
        scratch_shapes=[
            pltpu.VMEM((width, hidden), bf16),
            pltpu.VMEM((width, hidden), bf16),
            pltpu.VMEM((hidden, width), bf16),
            blocks,
            pltpu.VMEM((planes,) + info.shape, f32),
            rows, rows, rows, rows, table, table,
            pltpu.VMEM((near * cap, hidden), bf16),
            blocks, blocks,
            dma((3,)), dma((planes,)), dma((planes,)), dma((2, planes)), dma((2, planes)),
            dma((planes, near)), dma((planes, near)), dma((planes, near)), dma((planes, near)),
            dma((planes,)), dma((planes,)), dma((2, planes)),
        ],
        compiler_params=pltpu.CompilerParams(
            collective_id=3, has_side_effects=True, vmem_limit_bytes=60 * 1024 * 1024
        ),
        cost_estimate=pl.CostEstimate(flops=10**11, bytes_accessed=10**8, transcendentals=0),
        name="experts",
    )(tokens_in, info, gate_w, up_w, down_w)


def mixer_kernel(
    n, taps_n, x_ref, b_ref, c_ref, z_ref, gain_ref, step_ref, edge_ref, tap_ref, out_ref,
    taps, edges, halo, pad, reads, inside_ref, fade_f, fade_b, own_f, own_b, carry,
    send_f, send_b, got_f, got_b, gated, cols, rows_t, squares,
    tsend, trecv, esend, erecv, fsend, frecv, bsend, brecv, local,
):
    f32, bf16 = jnp.float32, jnp.bfloat16
    me = lax.axis_index("sp")
    groups = own_f.shape[0]
    lanes = x_ref.shape[1] // groups
    per_group = lanes // HEAD_DIM
    columns = 2 * per_group
    half = taps_n // 2
    wide = tap_ref.shape[1]
    greet([{"sp": lax.rem(me + i, n)} for i in range(1, n)])
    mine = pl.ds(pl.multiple_of(me * wide, wide), wide)

    def tell(i):
        return pltpu.make_async_remote_copy(
            src_ref=tap_ref,
            dst_ref=taps.at[:, mine],
            send_sem=tsend.at[i],
            recv_sem=trecv.at[i],
            device_id={"sp": lax.rem(me + i, n)},
            device_id_type=MESH,
        )

    def edge(way):
        return pltpu.make_async_remote_copy(
            src_ref=edge_ref.at[way],
            dst_ref=edges.at[way],
            send_sem=esend.at[way],
            recv_sem=erecv.at[way],
            device_id={"sp": me + 1 - 2 * way},
            device_id_type=MESH,
        )

    has_next, has_last = me < n - 1, me > 0

    @pl.when(has_next)
    def _():
        edge(0).start()

    @pl.when(has_last)
    def _():
        edge(1).start()

    for i in range(1, n):
        tell(i).start()
    keep = pltpu.make_async_copy(tap_ref, taps.at[:, mine], local.at[0])
    keep.start()

    @pl.when(jnp.logical_not(has_last))
    def _():
        halo[0] = jnp.zeros(halo.shape[1:], f32)
        got_f[...] = jnp.zeros(got_f.shape, bf16)

    @pl.when(jnp.logical_not(has_next))
    def _():
        halo[1] = jnp.zeros(halo.shape[1:], f32)
        got_b[...] = jnp.zeros(got_b.shape, bf16)

    li = lax.broadcasted_iota(jnp.int32, (BLOCK, BLOCK), 0)
    si = lax.broadcasted_iota(jnp.int32, (BLOCK, BLOCK), 1)
    lower = jnp.where(li >= si, 1.0, 0.0).astype(f32)
    lane_head = lax.broadcasted_iota(jnp.int32, (1, lanes), 1) // HEAD_DIM

    def spread_heads(values):
        out = values[0]
        for h in range(1, per_group):
            out = jnp.where(lane_head == h, values[h], out)
        return jnp.broadcast_to(out, (out.shape[0], lanes))

    v = step_ref[...]
    dt = jnp.maximum(v, 0.0) + jnp.log(1.0 + jnp.exp(-jnp.abs(v)))
    keep.wait()
    for i in range(1, n):
        tell(i).wait_recv()
    rate = taps[3 * taps_n : 3 * taps_n + 1, 0 : v.shape[1]]
    for i in range(1, n):
        rate = rate + taps[3 * taps_n : 3 * taps_n + 1, i * wide : i * wide + v.shape[1]]
    a = dt * rate
    inc = jnp.dot(lower, a, precision=highest, preferred_element_type=f32)
    exc = inc - a
    for k, value in enumerate((inc, exc, dt)):
        turned = value.T
        for g in range(groups):
            at = slice(g * columns, (g + 1) * columns)
            cols[k, g, :, 0:columns] = value[:, at]
            rows_t[k, g, 0:columns, :] = turned[at, :]

    @pl.when(has_last)
    def _():
        edge(0).wait_recv()
        halo[0] = edges[0].astype(f32)

    @pl.when(has_next)
    def _():
        edge(1).wait_recv()
        halo[1] = edges[1].astype(f32)

    def pass_f(g):
        return pltpu.make_async_remote_copy(
            src_ref=send_f.at[g],
            dst_ref=got_f.at[g],
            send_sem=fsend.at[g],
            recv_sem=frecv.at[g],
            device_id={"sp": me + 1},
            device_id_type=MESH,
        )

    def pass_b(g):
        return pltpu.make_async_remote_copy(
            src_ref=send_b.at[g],
            dst_ref=got_b.at[g],
            send_sem=bsend.at[g],
            recv_sem=brecv.at[g],
            device_id={"sp": me - 1},
            device_id_type=MESH,
        )

    def local_part(g, unused):
        at = pl.ds(pl.multiple_of(g * lanes, lanes), lanes)

        def conv(k, ref):
            pad[k, 8 - half : 8, :] = halo[0, k * half : (k + 1) * half, at]
            pad[k, BLOCK + 8 : BLOCK + 8 + half, :] = halo[1, k * half : (k + 1) * half, at]
            pad[k, 8 : BLOCK + 8, :] = ref[:, at].astype(f32)
            total = None
            for j in range(taps_n):
                first = 8 - half + j
                tap = taps[k * taps_n + j : k * taps_n + j + 1, at]
                term = pad[k, first : first + BLOCK, :] * tap
                total = term if total is None else total + term
            return total * jax.nn.sigmoid(total)

        x = conv(0, x_ref)
        write = conv(1, b_ref).astype(bf16)
        read = conv(2, c_ref).astype(bf16)
        reads[g] = read
        inc, exc, dt = (cols[k, g, :, 0:columns] for k in range(3))
        inct, exct, dtt = (rows_t[k, g, 0:columns, :] for k in range(3))
        tot = inc[BLOCK - 1 : BLOCK, :]
        heads = range(per_group)
        fwd = [inc[:, 2 * h : 2 * h + 1] for h in heads]
        bwd = [exc[:, 2 * h + 1 : 2 * h + 2] for h in heads]
        tot_f = [tot[:, 2 * h : 2 * h + 1] for h in heads]
        tot_b = [tot[:, 2 * h + 1 : 2 * h + 2] for h in heads]
        wf = spread_heads([dt[:, 2 * h : 2 * h + 1] * jnp.exp(fwd[h] - tot_f[h]) for h in heads])
        wb = spread_heads([dt[:, 2 * h + 1 : 2 * h + 2] * jnp.exp(-bwd[h]) for h in heads])
        both = jnp.concatenate([(x * wf).astype(bf16), (x * wb).astype(bf16)], axis=1)
        sums = lax.dot_general(write, both, (((0,), (0,)), ((), ())), preferred_element_type=f32)
        own_f[g] = sums[:, 0:lanes]
        own_b[g] = sums[:, lanes : 2 * lanes]
        carry[g, 0:1, :] = spread_heads([jnp.exp(-tot_f[h]) for h in heads])
        carry[g, 1:2, :] = spread_heads([jnp.exp(-tot_b[h]) for h in heads])

        @pl.when(jnp.logical_not(has_last))
        def _():
            send_f[g] = own_f[g].astype(bf16)
            pass_f(g).start()

        @pl.when(jnp.logical_not(has_next))
        def _():
            send_b[g] = own_b[g].astype(bf16)
            pass_b(g).start()

        fade_f[g] = spread_heads([jnp.exp(-fwd[h]) for h in heads])
        fade_b[g] = spread_heads([jnp.exp(bwd[h] - tot_b[h]) for h in heads])
        scores = lax.dot_general(read, write, (((1,), (1,)), ((), ())), preferred_element_type=f32)
        inside = None
        for h in heads:
            f, b = 2 * h, 2 * h + 1
            power = jnp.where(
                li >= si,
                inct[f : f + 1, :] - inc[:, f : f + 1],
                exc[:, b : b + 1] - exct[b : b + 1, :],
            )
            df, db = dtt[f : f + 1, :], dtt[b : b + 1, :]
            scale = jnp.where(li > si, df, jnp.where(li == si, df + db, db))
            weights = (scores * jnp.exp(power) * scale).astype(bf16)
            xh = jnp.where(lane_head == h, x, 0.0).astype(bf16)
            term = jnp.dot(weights, xh, preferred_element_type=f32)
            inside = term if inside is None else inside + term
        inside_ref[g] = inside
        return unused

    lax.fori_loop(0, groups, local_part, 0)

    slack = 2
    late_f = slack * jnp.maximum(2 * me - (n - 1), 0)
    late_b = slack * jnp.maximum((n - 1) - 2 * me, 0)
    late = jnp.maximum(late_f, late_b)
    per_norm = groups // NORM_GROUPS
    squares[...] = jnp.zeros(squares.shape, f32)

    def relay(k, unused):
        f, b, g = k - late_f, k - late_b, k - late

        @pl.when(has_last & (f >= 0) & (f < groups))
        def _():
            pass_f(f).wait_recv()

            @pl.when(has_next)
            def _():
                send_f[f] = (carry[f, 0:1, :] * got_f[f].astype(f32) + own_f[f]).astype(bf16)
                pass_f(f).start()

        @pl.when(has_next & (b >= 0) & (b < groups))
        def _():
            pass_b(b).wait_recv()

            @pl.when(has_last)
            def _():
                send_b[b] = (carry[b, 1:2, :] * got_b[b].astype(f32) + own_b[b]).astype(bf16)
                pass_b(b).start()

        @pl.when((g >= 0) & (g < groups))
        def _():
            entering = jnp.concatenate([got_f[g], got_b[g]], axis=1)
            moved = jnp.dot(reads[g], entering, preferred_element_type=f32)
            total = (
                inside_ref[g]
                + moved[:, 0:lanes] * fade_f[g]
                + moved[:, lanes : 2 * lanes] * fade_b[g]
            )
            at = pl.ds(pl.multiple_of(g * lanes, lanes), lanes)
            gate = z_ref[:, at].astype(f32)
            value = total.astype(bf16).astype(f32) * (gate * jax.nn.sigmoid(gate))
            gated[g] = value
            squares[g // per_norm] += jnp.sum(value * value, axis=1, keepdims=True)

        return unused

    lax.fori_loop(0, groups + slack * (n - 1), relay, 0)

    def scale(g, unused):
        at = pl.ds(pl.multiple_of(g * lanes, lanes), lanes)
        mean = squares[g // per_norm] * (1.0 / (per_norm * lanes))
        value = gated[g] * lax.rsqrt(mean + epsilon) * gain_ref[:, at]
        out_ref[:, at] = value.astype(bf16)
        return unused

    lax.fori_loop(0, groups, scale, 0)

    for i in range(1, n):
        tell(i).wait_send()

    @pl.when(has_next)
    def _():
        edge(0).wait_send()

        def one(g, unused):
            pass_f(g).wait_send()
            return unused

        lax.fori_loop(0, groups, one, 0)

    @pl.when(has_last)
    def _():
        edge(1).wait_send()

        def one(g, unused):
            pass_b(g).wait_send()
            return unused

        lax.fori_loop(0, groups, one, 0)


def mixer(n, signal, write, read, gate, gain, steps, conv_x, conv_b, conv_c, rates):
    f32, bf16 = jnp.float32, jnp.bfloat16
    tokens, width = signal.shape
    groups = write.shape[1] // STATE
    lanes = width // groups
    taps_n, wide = conv_x.shape
    half = taps_n // 2
    columns = steps.shape[1]
    padded = max(columns, BLOCK)
    own = rates.T.reshape(1, -1)
    row = jnp.zeros((1, wide), f32)
    row = lax.dynamic_update_slice(row, own, (0, lax.axis_index("sp") * own.shape[1]))
    lines = 3 * taps_n + 1
    spare = -lines % 8
    taps = jnp.concatenate([conv_x, conv_b, conv_c, row, jnp.zeros((spare, wide), f32)], axis=0)
    few = [signal, write, read]
    blank = jnp.zeros((16 - 3 * half, width), bf16)
    edges = jnp.stack(
        [
            jnp.concatenate([v[tokens - half :] for v in few] + [blank], axis=0),
            jnp.concatenate([v[:half] for v in few] + [blank], axis=0),
        ]
    )
    step = jnp.pad(steps.astype(f32), ((0, 0), (0, padded - columns)))
    inside = pl.BlockSpec(memory_space=pltpu.VMEM)
    dma = pltpu.SemaphoreType.DMA
    tile = pltpu.VMEM((groups, tokens, lanes), f32)
    state = pltpu.VMEM((groups, STATE, lanes), f32)
    small = pltpu.VMEM((groups, STATE, lanes), bf16)
    return pl.pallas_call(
        functools.partial(mixer_kernel, n, taps_n),
        out_shape=jax.ShapeDtypeStruct((tokens, width), bf16),
        in_specs=[inside] * 8,
        out_specs=inside,
        scratch_shapes=[
            pltpu.VMEM((lines + spare, n * wide), f32),
            pltpu.VMEM(edges.shape, bf16),
            pltpu.VMEM(edges.shape, f32),
            pltpu.VMEM((3, tokens + 16, lanes), f32),
            pltpu.VMEM((groups, tokens, STATE), bf16),
            tile, tile, tile, state, state,
            pltpu.VMEM((groups, 8, lanes), f32),
            small, small, small, small, tile,
            pltpu.VMEM((3, groups, tokens, 8), f32),
            pltpu.VMEM((3, groups, 8, tokens), f32),
            pltpu.VMEM((NORM_GROUPS, tokens, 1), f32),
            dma((n,)), dma((n,)), dma((2,)), dma((2,)),
            dma((groups,)), dma((groups,)), dma((groups,)), dma((groups,)), dma((1,)),
        ],
        compiler_params=pltpu.CompilerParams(
            collective_id=1, has_side_effects=True, vmem_limit_bytes=40 * 1024 * 1024
        ),
        cost_estimate=pl.CostEstimate(
            flops=40 * 10**9, bytes_accessed=4 * tokens * width * 2, transcendentals=0
        ),
        name="mixer",
    )(signal, write, read, gate, gain.reshape(1, width), step, edges, taps)


def scale_rows(values, gains):
    return values * lax.rsqrt(jnp.mean(values * values, axis=-1, keepdims=True) + epsilon) * gains


def gather_rows(weight, count):
    parts = {0: weight}
    step = count // 2
    while step >= 1:
        pairs = [(d, d ^ step) for d in range(count)]
        for offset, block in list(parts.items()):
            parts[offset ^ step] = lax.ppermute(block, "dp", pairs)
        step //= 2
    return parts


def per_device(
    residual_in, ssm_input, state_b, state_c, step_raw, gate_input, conv_x, conv_b, conv_c,
    decay_rate, mix_gain, out_weight, ffn_gain, routing, route_weight, gate_w, up_w, down_w,
):
    sp_count = lax.axis_size("sp")
    dp_count = lax.axis_size("dp")
    bf16, f32 = jnp.bfloat16, jnp.float32
    parts = gather_rows(out_weight, dp_count)
    mixed = mixer(
        sp_count, ssm_input[0], state_b[0], state_c[0], gate_input[0], mix_gain, step_raw[0],
        conv_x, conv_b, conv_c, decay_rate,
    )

    token_count = residual_in.shape[1]
    depth = out_weight.shape[0]
    me = lax.axis_index("dp")
    stream = residual_in[0].astype(f32)
    for offset, block in parts.items():
        piece = lax.dynamic_slice_in_dim(mixed, (me ^ offset) * depth, depth, axis=1)
        stream = stream + jnp.dot(piece, block, preferred_element_type=f32)
    ffn_input = scale_rows(stream, ffn_gain).astype(bf16)

    top_count = routing.shape[2]
    inner = dp_count // 2
    planes = sp_count // inner
    capacity = 4 * token_count * top_count // (2 * sp_count * dp_count)
    info = jnp.concatenate([routing[0].T.astype(f32), route_weight[0].T], axis=0)
    routed = experts(
        planes, inner, dp_count, capacity, top_count, ffn_input, info, gate_w, up_w, down_w
    )
    return (stream + routed).astype(bf16)[None]


def solution(mesh):
    return jax.shard_map(
        per_device,
        mesh=mesh,
        in_specs=(
            P("dp", "sp", None),
            P("dp", "sp", None),
            P("dp", "sp", None),
            P("dp", "sp", None),
            P("dp", "sp", None),
            P("dp", "sp", None),
            P(None, "sp"),
            P(None, "sp"),
            P(None, "sp"),
            P(None, "sp"),
            P(),
            P("dp", None),
            P(),
            P("dp", "sp", None),
            P("dp", "sp", None),
            P(("sp", "dp"), None, None),
            P(("sp", "dp"), None, None),
            P(("sp", "dp"), None, None),
        ),
        out_specs=P("dp", "sp", None),
        check_vma=False,
    )
```

```python
import functools

import jax
import jax.numpy as jnp
from jax import lax
from jax.experimental import pallas as pl
from jax.experimental.pallas import tpu as pltpu
from jax.sharding import PartitionSpec as P

HEAD_DIM = 64
STATE = 128
BLOCK = 128
NORM_GROUPS = 4
MESH = pl.DeviceIdType.MESH

highest = lax.Precision.HIGHEST
epsilon = 1e-05
clamp_limit = 7.0
sigmoid_slope = 1.702


def greet(peers):
    barrier = pltpu.get_barrier_semaphore()
    for peer in peers:
        pl.semaphore_signal(barrier, inc=1, device_id=peer, device_id_type=MESH)
    pl.semaphore_wait(barrier, len(peers))


def plane_order(z, planes, s):
    below, above = z, planes - 1 - z
    both = jnp.minimum(below, above)
    near = (s + 1) // 2
    from_below = jnp.where(s <= 2 * both, s % 2, jnp.where(below > above, 1, 0))
    hops = jnp.where(s <= 2 * both, near, s - both)
    return hops, from_below, z + hops * (1 - 2 * from_below)


def experts_kernel(
    planes, inner, dp_count, top, x_ref, info_ref, gate_hbm, up_hbm, down_hbm, out_ref,
    gate, up, down, tok, infos, rows_out, rows_in, made, back, high, low, active, part, part_in,
    wsem, isend, irecv, zsend, zrecv, dsend, drecv, rsend, rrecv, psend, precv, local,
):
    f32, bf16 = jnp.float32, jnp.bfloat16
    near = inner * dp_count
    tokens, width = x_ref.shape
    cap = rows_out.shape[2]
    sp, dp = lax.axis_index("sp"), lax.axis_index("dp")
    z, x = sp // inner, lax.rem(sp, inner)
    me = x * dp_count + dp

    def place(p):
        return {"sp": z * inner + p // dp_count, "dp": lax.rem(p, dp_count)}

    def plane(other):
        return {"sp": other * inner + x, "dp": dp}

    barrier = pltpu.get_barrier_semaphore()

    def call(i, carry):
        peer = lax.rem(me + i, near)
        pl.semaphore_signal(barrier, inc=1, device_id=place(peer), device_id_type=MESH)
        return carry

    lax.fori_loop(1, near, call, 0)
    for i in range(1, planes):
        pl.semaphore_signal(
            barrier, inc=1, device_id=plane(lax.rem(z + i, planes)), device_id_type=MESH
        )
    loads = [
        pltpu.make_async_copy(gate_hbm.at[0], gate, wsem.at[0]),
        pltpu.make_async_copy(up_hbm.at[0], up, wsem.at[1]),
        pltpu.make_async_copy(down_hbm.at[0], down, wsem.at[2]),
    ]
    for load in loads:
        load.start()
    pl.semaphore_wait(barrier, near - 1 + planes - 1)

    def tell(i):
        return pltpu.make_async_remote_copy(
            src_ref=info_ref,
            dst_ref=infos.at[z],
            send_sem=isend.at[i],
            recv_sem=irecv.at[i],
            device_id=plane(lax.rem(z + i, planes)),
            device_id_type=MESH,
        )

    for i in range(1, planes):
        tell(i).start()

    def along(src, block, step, way):
        return pltpu.make_async_remote_copy(
            src_ref=src,
            dst_ref=tok.at[block],
            send_sem=zsend.at[way, step],
            recv_sem=zrecv.at[way, step],
            device_id=plane(z + 1 - 2 * way),
            device_id_type=MESH,
        )

    up_open, down_open = z < planes - 1, z > 0

    @pl.when(up_open)
    def _():
        along(x_ref, z, 0, 0).start()

    @pl.when(down_open)
    def _():
        along(x_ref, z, 0, 1).start()

    ti = lax.broadcasted_iota(jnp.int32, (tokens, tokens), 0)
    tj = lax.broadcasted_iota(jnp.int32, (tokens, tokens), 1)
    earlier = jnp.where(ti < tj, 1.0, 0.0).astype(bf16)
    expert = (z * near + lax.broadcasted_iota(jnp.int32, (near, tokens), 0)).astype(f32)
    place_in = lax.broadcasted_iota(jnp.int32, (near, cap, tokens), 1).astype(f32)

    def send_rows(block, i):
        peer = lax.rem(me + i, near)
        return pltpu.make_async_remote_copy(
            src_ref=rows_out.at[block, peer],
            dst_ref=rows_in.at[block, me],
            send_sem=dsend.at[block, i],
            recv_sem=drecv.at[block, i],
            device_id=place(peer),
            device_id_type=MESH,
        )

    def keep_rows(block):
        return pltpu.make_async_copy(
            rows_out.at[block, me], rows_in.at[block, me], local.at[0, block]
        )

    def send_back(block, i):
        peer = lax.rem(me + i, near)
        return pltpu.make_async_remote_copy(
            src_ref=made.at[block, peer],
            dst_ref=back.at[block, me],
            send_sem=rsend.at[block, i],
            recv_sem=rrecv.at[block, i],
            device_id=place(peer),
            device_id_type=MESH,
        )

    def keep_back(block):
        return pltpu.make_async_copy(made.at[block, me], back.at[block, me], local.at[1, block])

    def each(what):
        def one(i, carry):
            what(i)
            return carry

        lax.fori_loop(1, near, one, 0)

    def dispatch(block, values, info):
        names, weights = info[0:top, :], info[top : 2 * top, :]
        named, weight = None, None
        for k in range(top):
            hit = names[k : k + 1, :] == expert
            one = jnp.where(hit, 1.0, 0.0)
            share = jnp.where(hit, weights[k : k + 1, :], 0.0)
            named = one if named is None else named + one
            weight = share if weight is None else weight + share
        slot = jnp.dot(named.astype(bf16), earlier, preferred_element_type=f32)
        slot = jnp.where(named > 0.5, slot, -1.0)
        pick = slot[:, None, :] == place_in
        rough = weight.astype(bf16).astype(f32)
        rest = weight - rough

        def table(v):
            return jnp.where(pick, v, 0.0).reshape(near * cap, tokens).astype(bf16)

        high[block] = table(rough[:, None, :])
        low[block] = table(rest[:, None, :])
        select = table(jnp.ones((near, 1, tokens), f32))
        chunk = 512
        for at in range(0, width, chunk):
            rows = jnp.dot(select, values[:, at : at + chunk], preferred_element_type=f32)
            rows_out[block, :, :, at : at + chunk] = rows.astype(bf16).reshape(near, cap, chunk)
        each(lambda i: send_rows(block, i).start())
        keep_rows(block).start()

    def arrive(s):
        hops, from_below, block = plane_order(z, planes, s)
        way = 1 - from_below
        along(tok.at[block], block, hops - 1, way).wait_recv()
        onward = jnp.where(from_below == 1, z + 1, z - 1)

        @pl.when((onward >= 0) & (onward < planes))
        def _():
            along(tok.at[block], block, hops, way).start()

        source = lax.rem(z - block + planes, planes)
        tell(source).wait_recv()
        dispatch(block, tok[block], infos[block])
        return block

    hidden = gate.shape[1]
    flat = near * cap

    def serve(block):
        keep_rows(block).wait()
        each(lambda i: send_rows(block, i).wait_recv())
        tile = 256

        def lift(n, carry):
            cols = pl.ds(pl.multiple_of(n * tile, tile), tile)
            rows = rows_in[block].reshape(flat, width)
            g = jnp.minimum(jnp.dot(rows, gate[:, cols], preferred_element_type=f32), clamp_limit)
            u = jnp.dot(rows, up[:, cols], preferred_element_type=f32)
            u = jnp.clip(u, -clamp_limit, clamp_limit)
            active[:, cols] = ((u + 1.0) * g * jax.nn.sigmoid(sigmoid_slope * g)).astype(bf16)
            return carry

        lax.fori_loop(0, hidden // tile, lift, 0)

        def lower(n, carry):
            cols = pl.ds(pl.multiple_of(n * tile, tile), tile)
            y = jnp.dot(active[...], down[:, cols], preferred_element_type=f32)
            made[block, :, :, cols] = y.astype(bf16).reshape(near, cap, tile)
            return carry

        lax.fori_loop(0, width // tile, lower, 0)

    def give(block):
        each(lambda i: send_back(block, i).start())
        keep_back(block).start()

    def gathered(block, at, chunk):
        rows = back[block, :, :, at : at + chunk].reshape(flat, chunk)
        dims = (((0,), (0,)), ((), ()))
        return lax.dot_general(
            high[block], rows, dims, preferred_element_type=f32
        ) + lax.dot_general(low[block], rows, dims, preferred_element_type=f32)

    def send_part(block, i):
        return pltpu.make_async_remote_copy(
            src_ref=part.at[block],
            dst_ref=part_in.at[z],
            send_sem=psend.at[i],
            recv_sem=precv.at[i],
            device_id=plane(block),
            device_id_type=MESH,
        )

    def landed(block):
        keep_back(block).wait()
        each(lambda i: send_back(block, i).wait_recv())

    def collect(block):
        landed(block)
        chunk = 512
        for at in range(0, width, chunk):
            part[block, :, at : at + chunk] = gathered(block, at, chunk).astype(bf16)
        send_part(block, lax.rem(block - z + planes, planes)).start()

    blocks = [z]
    dispatch(z, x_ref[...], info_ref[...])
    served = 0
    for s in range(1, planes):
        blocks.append(arrive(s))
        if s == planes - 2:
            for load in loads:
                load.wait()
            serve(blocks[0])
            served = 1
    if not served:
        for load in loads:
            load.wait()
        serve(blocks[0])
    for s in range(1, planes):
        serve(blocks[s])
        give(blocks[s])
    give(blocks[0])
    for s in range(1, planes):
        collect(blocks[s])
    landed(z)
    chunk = 512
    for at in range(0, width, chunk):
        out_ref[:, at : at + chunk] = gathered(z, at, chunk)
    for i in range(1, planes):
        send_part(lax.rem(z + i, planes), i).wait_recv()
        out_ref[...] += part_in[lax.rem(z - i + planes, planes)].astype(f32)

    for i in range(1, planes):
        tell(i).wait_send()
        send_part(lax.rem(z + i, planes), i).wait_send()
    for block in range(planes):
        each(lambda i: send_rows(block, i).wait_send())
        each(lambda i: send_back(block, i).wait_send())

    @pl.when(up_open)
    def _():
        along(x_ref, z, 0, 0).wait_send()

    @pl.when(down_open)
    def _():
        along(x_ref, z, 0, 1).wait_send()

    for step in range(1, planes):

        @pl.when(up_open & (z - step >= 0))
        def _():
            along(tok.at[z], z, step, 0).wait_send()

        @pl.when(down_open & (z + step < planes))
        def _():
            along(tok.at[z], z, step, 1).wait_send()


def experts(planes, inner, dp_count, cap, top, tokens_in, info, gate_w, up_w, down_w):
    near = inner * dp_count
    tokens, width = tokens_in.shape
    hidden = gate_w.shape[2]
    bf16, f32 = jnp.bfloat16, jnp.float32
    anywhere = pl.BlockSpec(memory_space=pl.ANY)
    inside = pl.BlockSpec(memory_space=pltpu.VMEM)
    dma = pltpu.SemaphoreType.DMA
    rows = pltpu.VMEM((planes, near, cap, width), bf16)
    table = pltpu.VMEM((planes, near * cap, tokens), bf16)
    blocks = pltpu.VMEM((planes, tokens, width), bf16)
    return pl.pallas_call(
        functools.partial(experts_kernel, planes, inner, dp_count, top),
        out_shape=jax.ShapeDtypeStruct((tokens, width), f32),
        in_specs=[inside, inside, anywhere, anywhere, anywhere],
        out_specs=inside,
        scratch_shapes=[
            pltpu.VMEM((width, hidden), bf16),
            pltpu.VMEM((width, hidden), bf16),
            pltpu.VMEM((hidden, width), bf16),
            blocks,
            pltpu.VMEM((planes,) + info.shape, f32),
            rows, rows, rows, rows, table, table,
            pltpu.VMEM((near * cap, hidden), bf16),
            blocks, blocks,
            dma((3,)), dma((planes,)), dma((planes,)), dma((2, planes)), dma((2, planes)),
            dma((planes, near)), dma((planes, near)), dma((planes, near)), dma((planes, near)),
            dma((planes,)), dma((planes,)), dma((2, planes)),
        ],
        compiler_params=pltpu.CompilerParams(
            collective_id=3, has_side_effects=True, vmem_limit_bytes=60 * 1024 * 1024
        ),
        cost_estimate=pl.CostEstimate(flops=10**11, bytes_accessed=10**8, transcendentals=0),
        name="experts",
    )(tokens_in, info, gate_w, up_w, down_w)


def lowest(offset):
    return offset & -offset


def mixer_kernel(
    n, inner, dp_count, x_hbm, b_hbm, c_hbm, z_hbm, r_hbm, w_hbm, step_ref, tx_ref, tb_ref, tc_ref,
    rate_ref, gain_ref, ffn_gain_ref, stream_ref, ffn_ref,
    ins, gate_v, res_v, w_all, steps, taps, rates, halo_in, halo, pad, reads, inside_ref,
    fade_f, fade_b, own_f, own_b, carry, send_f, send_b, got_f, got_b, ybuf, ytok, gated, mixed,
    cols, rows_t, squares,
    in_s, in_r, step_s, step_r, tap_s, tap_r, rate_s, rate_r, halo_s, halo_r,
    f_s, f_r, b_s, b_r, y_s, y_r, w_s, w_r, own_in, local,
):
    f32, bf16 = jnp.float32, jnp.bfloat16
    sp, dp = lax.axis_index("sp"), lax.axis_index("dp")
    z, x = sp // inner, lax.rem(sp, inner)
    planes = n // inner
    tokens, width = stream_ref.shape
    span = ins.shape[3]
    locals_n = own_f.shape[0]
    lanes = span // locals_n
    groups = locals_n * inner
    per_group = lanes // HEAD_DIM
    columns = 2 * per_group
    taps_n, wide = tx_ref.shape
    half = taps_n // 2
    depth = w_hbm.shape[0]
    piece = min(depth, 128)
    pieces = depth // piece
    bits = [1 << i for i in range(dp_count.bit_length() - 1)]
    flows = (x_hbm, b_hbm, c_hbm)
    tap_refs = (tx_ref, tb_ref, tc_ref)

    def mate(bit):
        return dp + bit * (1 - 2 * lax.rem(dp // bit, 2))

    greet([{"sp": lax.rem(sp + i, n)} for i in range(1, n)] + [{"dp": mate(b)} for b in bits])

    def remote(src, dst, send, recv, where):
        return pltpu.make_async_remote_copy(
            src_ref=src, dst_ref=dst, send_sem=send, recv_sem=recv,
            device_id=where, device_id_type=MESH,
        )

    def spot(start, size):
        return pl.ds(pl.multiple_of(start, size), size)

    def give_step(i):
        return remote(
            step_ref, steps.at[x], step_s.at[i], step_r.at[i],
            {"sp": z * inner + lax.rem(x + i, inner)},
        )

    mine = spot(sp * wide, wide)

    def give_tap(k, i):
        return remote(
            tap_refs[k], taps.at[k, 0:taps_n, mine], tap_s.at[k, i], tap_r.at[k, i],
            {"sp": lax.rem(sp + i, n)},
        )

    def give_rate(i):
        return remote(
            rate_ref, rates.at[sp], rate_s.at[i], rate_r.at[i], {"sp": lax.rem(sp + i, n)}
        )

    def give_halo(way, k, to):
        first = 0 if way else tokens - 8
        return remote(
            flows[k].at[first : first + 8, to * span : (to + 1) * span],
            halo_in.at[way, k], halo_s.at[way, k, to], halo_r.at[way, k],
            {"sp": (z + 1 - 2 * way) * inner + to},
        )

    def give_in(k, q, i):
        peer = lax.rem(x + i, inner)
        return remote(
            flows[k].at[:, spot(peer * span + q * lanes, lanes)],
            ins.at[k, x, :, spot(q * lanes, lanes)],
            in_s.at[k, q, i], in_r.at[k, q, i], {"sp": z * inner + peer},
        )

    def give_weight(offset, bit, c):
        rows = slice(c * piece, (c + 1) * piece)
        src = w_hbm.at[rows] if offset == 0 else w_all.at[offset, rows]
        return remote(
            src, w_all.at[offset + bit, rows],
            w_s.at[offset, bits.index(bit), c], w_r.at[offset + bit, c], {"dp": mate(bit)},
        )

    has_above, has_below = z < planes - 1, z > 0
    sends_up = has_above & (x == inner - 1)
    sends_down = has_below & (x == 0)

    for i in range(1, inner):
        give_step(i).start()
    for i in range(1, n):
        for k in range(3):
            give_tap(k, i).start()
        give_rate(i).start()

    @pl.when(sends_up)
    def _():
        for k in range(3):
            for to in range(inner):
                give_halo(0, k, to).start()

    @pl.when(sends_down)
    def _():
        for k in range(3):
            for to in range(inner):
                give_halo(1, k, to).start()

    def begin(q, unused):
        for k in range(3):
            for i in range(1, inner):
                give_in(k, q, i).start()
        return unused

    lax.fori_loop(0, locals_n, begin, 0)
    owned = [
        pltpu.make_async_copy(
            flows[k].at[:, spot(x * span, span)], ins.at[k, x], own_in.at[k]
        )
        for k in range(3)
    ]
    for copy in owned:
        copy.start()
    for bit in reversed(bits):
        for c in range(pieces):
            give_weight(0, bit, c).start()
    keeps = [
        pltpu.make_async_copy(tap_refs[k], taps.at[k, 0:taps_n, mine], local.at[k])
        for k in range(3)
    ]
    keeps.append(pltpu.make_async_copy(rate_ref, rates.at[sp], local.at[3]))
    keeps.append(pltpu.make_async_copy(step_ref, steps.at[x], local.at[4]))
    for copy in keeps:
        copy.start()
    late_loads = [
        pltpu.make_async_copy(z_hbm, gate_v, local.at[5]),
        pltpu.make_async_copy(r_hbm, res_v, local.at[6]),
        pltpu.make_async_copy(w_hbm, w_all.at[0], local.at[7]),
    ]
    for copy in late_loads:
        copy.start()

    @pl.when(jnp.logical_not(has_below))
    def _():
        halo[0] = jnp.zeros(halo.shape[1:], f32)
        got_f[...] = jnp.zeros(got_f.shape, bf16)

    @pl.when(jnp.logical_not(has_above))
    def _():
        halo[1] = jnp.zeros(halo.shape[1:], f32)
        got_b[...] = jnp.zeros(got_b.shape, bf16)

    li = lax.broadcasted_iota(jnp.int32, (BLOCK, BLOCK), 0)
    si = lax.broadcasted_iota(jnp.int32, (BLOCK, BLOCK), 1)
    lower = jnp.where(li >= si, 1.0, 0.0).astype(f32)
    lane = lax.broadcasted_iota(jnp.int32, (1, lanes), 1)
    lane_head = lane // HEAD_DIM

    def spread_heads(values):
        out = values[0]
        for h in range(1, per_group):
            out = jnp.where(lane_head == h, values[h], out)
        return jnp.broadcast_to(out, (out.shape[0], lanes))

    for copy in keeps:
        copy.wait()
    for i in range(1, n):
        give_rate(i).wait_recv()
    step_columns = step_ref.shape[1]
    window = step_columns // inner
    held = rate_ref.shape[1]
    rate = jnp.zeros((1, BLOCK), f32)
    row_lane = lax.broadcasted_iota(jnp.int32, (1, BLOCK), 1)
    for t in range(planes):
        pair = rates[x * planes + t]
        for h in range(held):
            for d in range(2):
                rate = jnp.where(
                    row_lane == 2 * (t * held + h) + d, pair[d : d + 1, h : h + 1], rate
                )
    choose_row = lax.broadcasted_iota(jnp.int32, (step_columns, BLOCK), 0)
    choose_col = lax.broadcasted_iota(jnp.int32, (step_columns, BLOCK), 1)
    choose = jnp.where((choose_row == x * window + choose_col) & (choose_col < window), 1.0, 0.0)
    choose = choose.astype(bf16)
    for i in range(1, inner):
        give_step(i).wait_recv()
    for i in range(inner):
        v = jnp.dot(steps[i], choose, preferred_element_type=f32)
        dt = jnp.maximum(v, 0.0) + jnp.log(1.0 + jnp.exp(-jnp.abs(v)))
        a = dt * rate
        inc = jnp.dot(lower, a, precision=highest, preferred_element_type=f32)
        exc = inc - a
        for k, value in enumerate((inc, exc, dt)):
            turned = value.T
            for q in range(locals_n):
                at = slice(q * columns, (q + 1) * columns)
                cols[k, i, q, :, 0:columns] = value[:, at]
                rows_t[k, i, q, 0:columns, :] = turned[at, :]

    for i in range(1, n):
        for k in range(3):
            give_tap(k, i).wait_recv()

    @pl.when(has_below)
    def _():
        for k in range(3):
            give_halo(0, k, 0).wait_recv()
        halo[0] = halo_in[0].astype(f32)

    @pl.when(has_above)
    def _():
        for k in range(3):
            give_halo(1, k, 0).wait_recv()
        halo[1] = halo_in[1].astype(f32)

    for copy in owned:
        copy.wait()

    def pass_f(q):
        return remote(
            send_f.at[q], got_f.at[q], f_s.at[q], f_r.at[q], {"sp": sp + inner}
        )

    def pass_b(q):
        return remote(
            send_b.at[q], got_b.at[q], b_s.at[q], b_r.at[q], {"sp": sp - inner}
        )

    def onward_f(q, value):
        for i in range(inner):
            value = carry[q, i, 0:1, :] * value + own_f[q, i]
        send_f[q] = value.astype(bf16)
        pass_f(q).start()

    def onward_b(q, value):
        for i in reversed(range(inner)):
            value = carry[q, i, 1:2, :] * value + own_b[q, i]
        send_b[q] = value.astype(bf16)
        pass_b(q).start()

    def local_part(q):
        at = spot(q * lanes, lanes)
        wide_at = spot(x * span + q * lanes, lanes)
        length = inner * tokens
        for k in range(3):
            pad[k, 8 - half : 8, :] = halo[0, k, 8 - half : 8, at]
            pad[k, length + 8 : length + 8 + half, :] = halo[1, k, 0:half, at]
            for i in range(inner):
                pad[k, i * tokens + 8 : (i + 1) * tokens + 8, :] = ins[k, i, :, at].astype(f32)

        def conv(k, i):
            total = None
            for j in range(taps_n):
                first = i * tokens + 8 - half + j
                term = pad[k, first : first + tokens, :] * taps[k, j : j + 1, wide_at]
                total = term if total is None else total + term
            return total * jax.nn.sigmoid(total)

        for i in range(inner):
            xs = conv(0, i)
            write = conv(1, i).astype(bf16)
            read = conv(2, i).astype(bf16)
            reads[q, i] = read
            inc, exc, dt = (cols[k, i, q, :, 0:columns] for k in range(3))
            inct, exct, dtt = (rows_t[k, i, q, 0:columns, :] for k in range(3))
            tot = inc[BLOCK - 1 : BLOCK, :]
            heads = range(per_group)
            fwd = [inc[:, 2 * h : 2 * h + 1] for h in heads]
            bwd = [exc[:, 2 * h + 1 : 2 * h + 2] for h in heads]
            tot_f = [tot[:, 2 * h : 2 * h + 1] for h in heads]
            tot_b = [tot[:, 2 * h + 1 : 2 * h + 2] for h in heads]
            wf = spread_heads(
                [dt[:, 2 * h : 2 * h + 1] * jnp.exp(fwd[h] - tot_f[h]) for h in heads]
            )
            wb = spread_heads([dt[:, 2 * h + 1 : 2 * h + 2] * jnp.exp(-bwd[h]) for h in heads])
            both = jnp.concatenate([(xs * wf).astype(bf16), (xs * wb).astype(bf16)], axis=1)
            sums = lax.dot_general(
                write, both, (((0,), (0,)), ((), ())), preferred_element_type=f32
            )
            own_f[q, i] = sums[:, 0:lanes]
            own_b[q, i] = sums[:, lanes : 2 * lanes]
            carry[q, i, 0:1, :] = spread_heads([jnp.exp(-tot_f[h]) for h in heads])
            carry[q, i, 1:2, :] = spread_heads([jnp.exp(-tot_b[h]) for h in heads])
            fade_f[q, i] = spread_heads([jnp.exp(-fwd[h]) for h in heads])
            fade_b[q, i] = spread_heads([jnp.exp(bwd[h] - tot_b[h]) for h in heads])
            scores = lax.dot_general(
                read, write, (((1,), (1,)), ((), ())), preferred_element_type=f32
            )
            inside = None
            for h in heads:
                f, b = 2 * h, 2 * h + 1
                power = jnp.where(
                    li >= si,
                    inct[f : f + 1, :] - inc[:, f : f + 1],
                    exc[:, b : b + 1] - exct[b : b + 1, :],
                )
                df, db = dtt[f : f + 1, :], dtt[b : b + 1, :]
                scale = jnp.where(li > si, df, jnp.where(li == si, df + db, db))
                weights = (scores * jnp.exp(power) * scale).astype(bf16)
                xh = jnp.where(lane_head == h, xs, 0.0).astype(bf16)
                term = jnp.dot(weights, xh, preferred_element_type=f32)
                inside = term if inside is None else inside + term
            inside_ref[q, i] = inside

        @pl.when(has_above & jnp.logical_not(has_below))
        def _():
            onward_f(q, jnp.zeros((STATE, lanes), f32))

        @pl.when(has_below & jnp.logical_not(has_above))
        def _():
            onward_b(q, jnp.zeros((STATE, lanes), f32))

    def give_y(q, to):
        i = lax.rem(to - x + inner, inner)
        return remote(
            ybuf.at[q, to], ytok.at[:, spot((x * locals_n + q) * lanes, lanes)],
            y_s.at[i, q], y_r.at[i, q], {"sp": z * inner + to},
        )

    def finish(q):
        enter_f, enter_b = [], [None] * inner
        value = got_f[q].astype(f32)
        for i in range(inner):
            enter_f.append(value.astype(bf16))
            if i < inner - 1:
                value = carry[q, i, 0:1, :] * value + own_f[q, i]
        value = got_b[q].astype(f32)
        for i in reversed(range(inner)):
            enter_b[i] = value.astype(bf16)
            if i > 0:
                value = carry[q, i, 1:2, :] * value + own_b[q, i]
        for i in range(inner):
            entering = jnp.concatenate([enter_f[i], enter_b[i]], axis=1)
            moved = jnp.dot(reads[q, i], entering, preferred_element_type=f32)
            total = (
                inside_ref[q, i]
                + moved[:, 0:lanes] * fade_f[q, i]
                + moved[:, lanes : 2 * lanes] * fade_b[q, i]
            )
            ybuf[q, i] = total.astype(bf16)

            @pl.when(x == i)
            def _():
                ytok[:, spot((x * locals_n + q) * lanes, lanes)] = ybuf[q, i]

            @pl.when(x != i)
            def _():
                give_y(q, i).start()

    late_f = (3 * z + 1) // 2
    late_b = (3 * (planes - 1 - z) + 1) // 2
    late = jnp.maximum(late_f, late_b)

    def turn(t, unused):
        f, b, g = t - late_f, t - late_b, t - late

        @pl.when(t < locals_n)
        def _():
            for k in range(3):
                for i in range(1, inner):
                    give_in(k, t, i).wait_recv()
            local_part(t)

        @pl.when(has_below & (f >= 0) & (f < locals_n))
        def _():
            pass_f(f).wait_recv()

            @pl.when(has_above)
            def _():
                onward_f(f, got_f[f].astype(f32))

        @pl.when(has_above & (b >= 0) & (b < locals_n))
        def _():
            pass_b(b).wait_recv()

            @pl.when(has_below)
            def _():
                onward_b(b, got_b[b].astype(f32))

        @pl.when((g >= 0) & (g < locals_n))
        def _():
            finish(g)

        return unused

    lax.fori_loop(0, locals_n + (3 * (planes - 1) + 1) // 2, turn, 0)

    per_norm = groups // NORM_GROUPS
    squares[...] = jnp.zeros(squares.shape, f32)
    for copy in late_loads:
        copy.wait()

    def gate_group(g, unused):
        owner, q = g // locals_n, lax.rem(g, locals_n)

        @pl.when(owner != x)
        def _():
            i = lax.rem(x - owner + inner, inner)
            remote(
                ybuf.at[q, 0], ytok.at[:, spot(g * lanes, lanes)],
                y_s.at[i, q], y_r.at[i, q], {"sp": z * inner + owner},
            ).wait_recv()

        at = spot(g * lanes, lanes)
        gate = gate_v[:, at].astype(f32)
        value = ytok[:, at].astype(f32) * (gate * jax.nn.sigmoid(gate))
        gated[g] = value
        squares[g // per_norm] += jnp.sum(value * value, axis=1, keepdims=True)
        return unused

    lax.fori_loop(0, groups, gate_group, 0)

    def scale(g, unused):
        at = spot(g * lanes, lanes)
        mean = squares[g // per_norm] * (1.0 / (per_norm * lanes))
        value = gated[g] * lax.rsqrt(mean + epsilon) * gain_ref[:, at]
        mixed[:, at] = value.astype(bf16)
        return unused

    lax.fori_loop(0, groups, scale, 0)

    stream_ref[...] = res_v[...].astype(f32)
    order = sorted(range(1, dp_count), key=lambda o: (-lowest(o), o))
    for offset in [0] + order:
        if offset:
            for c in range(pieces):
                give_weight(offset - lowest(offset), lowest(offset), c).wait_recv()
                for bit in bits:
                    if bit < lowest(offset):
                        give_weight(offset, bit, c).start()
        block = dp
        for bit in bits:
            if offset & bit:
                block = block + bit * (1 - 2 * lax.rem(dp // bit, 2))
        part = mixed[:, spot(block * depth, depth)]

        def project(t, unused):
            at = spot(t * 512, 512)
            stream_ref[:, at] += jnp.dot(
                part, w_all[offset, :, at], preferred_element_type=f32
            )
            return unused

        lax.fori_loop(0, width // 512, project, 0)
    total = jnp.zeros((tokens, 1), f32)
    for at in range(0, width, 512):
        value = stream_ref[:, at : at + 512]
        total = total + jnp.sum(value * value, axis=1, keepdims=True)
    root = lax.rsqrt(total * (1.0 / width) + epsilon)
    for at in range(0, width, 512):
        value = stream_ref[:, at : at + 512] * root * ffn_gain_ref[:, at : at + 512]
        ffn_ref[:, at : at + 512] = value.astype(bf16)

    for i in range(1, inner):
        give_step(i).wait_send()
    for i in range(1, n):
        for k in range(3):
            give_tap(k, i).wait_send()
        give_rate(i).wait_send()

    @pl.when(sends_up)
    def _():
        for k in range(3):
            for to in range(inner):
                give_halo(0, k, to).wait_send()

    @pl.when(sends_down)
    def _():
        for k in range(3):
            for to in range(inner):
                give_halo(1, k, to).wait_send()

    def drain(q, unused):
        for k in range(3):
            for i in range(1, inner):
                give_in(k, q, i).wait_send()
        for i in range(1, inner):
            give_y(q, lax.rem(x + i, inner)).wait_send()

        @pl.when(has_above)
        def _():
            pass_f(q).wait_send()

        @pl.when(has_below)
        def _():
            pass_b(q).wait_send()

        return unused

    lax.fori_loop(0, locals_n, drain, 0)
    for offset in range(dp_count):
        for bit in bits:
            if offset == 0 or bit < lowest(offset):
                for c in range(pieces):
                    give_weight(offset, bit, c).wait_send()


def mixer(
    n, inner, dp_count, signal, write, read, gate, residual, weight, steps,
    conv_x, conv_b, conv_c, rates, gain, ffn_gain,
):
    f32, bf16 = jnp.float32, jnp.bfloat16
    tokens, width = signal.shape
    groups = write.shape[1] // STATE
    lanes = width // groups
    own = groups // inner
    span = width // inner
    depth = weight.shape[0]
    pieces = depth // min(depth, 128)
    bits = dp_count.bit_length() - 1
    inside = pl.BlockSpec(memory_space=pltpu.VMEM)
    anywhere = pl.BlockSpec(memory_space=pl.ANY)
    dma = pltpu.SemaphoreType.DMA
    vmem = pltpu.VMEM
    tile = vmem((own, inner, tokens, lanes), f32)
    state = vmem((own, inner, STATE, lanes), f32)
    small = vmem((own, STATE, lanes), bf16)
    flat = vmem((tokens, width), bf16)
    return pl.pallas_call(
        functools.partial(mixer_kernel, n, inner, dp_count),
        out_shape=(
            jax.ShapeDtypeStruct((tokens, width), f32),
            jax.ShapeDtypeStruct((tokens, width), bf16),
        ),
        in_specs=[anywhere] * 6 + [inside] * 7,
        out_specs=(inside, inside),
        scratch_shapes=[
            vmem((3, inner, tokens, span), bf16), flat, flat,
            vmem((dp_count, depth, width), bf16),
            vmem((inner,) + steps.shape, bf16),
            vmem((3, 8, width), f32),
            vmem((n,) + rates.shape, f32),
            vmem((2, 3, 8, span), bf16),
            vmem((2, 3, 8, span), f32),
            vmem((3, inner * tokens + 16, lanes), f32),
            vmem((own, inner, tokens, STATE), bf16),
            tile, tile, tile, state, state,
            vmem((own, inner, 8, lanes), f32),
            small, small, small, small,
            vmem((own, inner, tokens, lanes), bf16), flat,
            vmem((groups, tokens, lanes), f32), flat,
            vmem((3, inner, own, tokens, 8), f32),
            vmem((3, inner, own, 8, tokens), f32),
            vmem((NORM_GROUPS, tokens, 1), f32),
            dma((3, own, inner)), dma((3, own, inner)), dma((inner,)), dma((inner,)),
            dma((3, n)), dma((3, n)), dma((n,)), dma((n,)), dma((2, 3, inner)), dma((2, 3)),
            dma((own,)), dma((own,)), dma((own,)), dma((own,)),
            dma((inner, own)), dma((inner, own)),
            dma((dp_count, bits, pieces)), dma((dp_count, pieces)), dma((3,)), dma((8,)),
        ],
        compiler_params=pltpu.CompilerParams(
            collective_id=1, has_side_effects=True, vmem_limit_bytes=56 * 1024 * 1024
        ),
        cost_estimate=pl.CostEstimate(
            flops=40 * 10**9, bytes_accessed=4 * tokens * width * 2, transcendentals=0
        ),
        name="mixer",
    )(
        signal, write, read, gate, residual, weight, steps, conv_x, conv_b, conv_c, rates,
        gain.reshape(1, width), ffn_gain.reshape(1, width),
    )


def per_device(
    residual_in, ssm_input, state_b, state_c, step_raw, gate_input, conv_x, conv_b, conv_c,
    decay_rate, mix_gain, out_weight, ffn_gain, routing, route_weight, gate_w, up_w, down_w,
):
    sp_count = lax.axis_size("sp")
    dp_count = lax.axis_size("dp")
    bf16, f32 = jnp.bfloat16, jnp.float32
    inner = dp_count // 2
    token_count = residual_in.shape[1]
    stream, ffn_input = mixer(
        sp_count, inner, dp_count, ssm_input[0], state_b[0], state_c[0], gate_input[0],
        residual_in[0], out_weight, step_raw[0], conv_x, conv_b, conv_c, decay_rate,
        mix_gain, ffn_gain,
    )
    top_count = routing.shape[2]
    planes = sp_count // inner
    capacity = 4 * token_count * top_count // (2 * sp_count * dp_count)
    info = jnp.concatenate([routing[0].T.astype(f32), route_weight[0].T], axis=0)
    routed = experts(
        planes, inner, dp_count, capacity, top_count, ffn_input, info, gate_w, up_w, down_w
    )
    return (stream + routed).astype(bf16)[None]


def solution(mesh):
    return jax.shard_map(
        per_device,
        mesh=mesh,
        in_specs=(
            P("dp", "sp", None),
            P("dp", "sp", None),
            P("dp", "sp", None),
            P("dp", "sp", None),
            P("dp", "sp", None),
            P("dp", "sp", None),
            P(None, "sp"),
            P(None, "sp"),
            P(None, "sp"),
            P(None, "sp"),
            P(),
            P("dp", None),
            P(),
            P("dp", "sp", None),
            P("dp", "sp", None),
            P(("sp", "dp"), None, None),
            P(("sp", "dp"), None, None),
            P(("sp", "dp"), None, None),
        ),
        out_specs=P("dp", "sp", None),
        check_vma=False,
    )
```

```python
import functools

import jax
import jax.numpy as jnp
from jax import lax
from jax.experimental import pallas as pl
from jax.experimental.pallas import tpu as pltpu
from jax.sharding import PartitionSpec as P

HEAD_DIM = 64
STATE = 128
BLOCK = 128
NORM_GROUPS = 4
MESH = pl.DeviceIdType.MESH

highest = lax.Precision.HIGHEST
epsilon = 1e-05
clamp_limit = 7.0
sigmoid_slope = 1.702


def greet(peers):
    barrier = pltpu.get_barrier_semaphore()
    for peer in peers:
        pl.semaphore_signal(barrier, inc=1, device_id=peer, device_id_type=MESH)
    pl.semaphore_wait(barrier, len(peers))


def plane_order(z, planes, s):
    below, above = z, planes - 1 - z
    both = jnp.minimum(below, above)
    near = (s + 1) // 2
    low = jnp.where(below < above, 1, 0)
    turn = jnp.where(low == 1, s % 2, 1 - s % 2)
    from_below = jnp.where(s <= 2 * both, turn, 1 - low)
    hops = jnp.where(s <= 2 * both, near, s - both)
    return hops, from_below, z + hops * (1 - 2 * from_below)


def experts_kernel(
    planes, inner, dp_count, top, x_ref, stream_ref, names_ref, shares_ref, gate_hbm, up_hbm,
    down_hbm, out_ref, gate, up, down, tok, names_in, shares_in, rows_out, rows_in, made, back, high, low, active, part, part_in,
    total, passing, wsem, isend, irecv, zsend, zrecv, dsend, drecv, rsend, rrecv, psend, precv,
    csend, crecv, local,
):
    f32, bf16 = jnp.float32, jnp.bfloat16
    near = inner * dp_count
    tokens, width = x_ref.shape
    cap = rows_out.shape[2]
    sp, dp = lax.axis_index("sp"), lax.axis_index("dp")
    z, x = sp // inner, lax.rem(sp, inner)
    me = x * dp_count + dp

    def place(p):
        return {"sp": z * inner + p // dp_count, "dp": lax.rem(p, dp_count)}

    def plane(other):
        return {"sp": other * inner + x, "dp": dp}

    barrier = pltpu.get_barrier_semaphore()

    def call(i, carry):
        peer = lax.rem(me + i, near)
        pl.semaphore_signal(barrier, inc=1, device_id=place(peer), device_id_type=MESH)
        return carry

    lax.fori_loop(1, near, call, 0)
    for i in range(1, planes):
        pl.semaphore_signal(
            barrier, inc=1, device_id=plane(lax.rem(z + i, planes)), device_id_type=MESH
        )
    loads = [
        pltpu.make_async_copy(gate_hbm.at[0], gate, wsem.at[0]),
        pltpu.make_async_copy(up_hbm.at[0], up, wsem.at[1]),
        pltpu.make_async_copy(down_hbm.at[0], down, wsem.at[2]),
    ]
    for load in loads:
        load.start()
    pl.semaphore_wait(barrier, near - 1 + planes - 1)

    def tell(kind, i):
        return pltpu.make_async_remote_copy(
            src_ref=(names_ref, shares_ref)[kind],
            dst_ref=(names_in, shares_in)[kind].at[z],
            send_sem=isend.at[kind, i],
            recv_sem=irecv.at[kind, i],
            device_id=plane(lax.rem(z + i, planes)),
            device_id_type=MESH,
        )

    for i in range(1, planes):
        for kind in range(2):
            tell(kind, i).start()

    def along(src, block, step, way):
        return pltpu.make_async_remote_copy(
            src_ref=src,
            dst_ref=tok.at[block],
            send_sem=zsend.at[way, step],
            recv_sem=zrecv.at[way, step],
            device_id=plane(z + 1 - 2 * way),
            device_id_type=MESH,
        )

    up_open, down_open = z < planes - 1, z > 0

    @pl.when(up_open)
    def _():
        along(x_ref, z, 0, 0).start()

    @pl.when(down_open)
    def _():
        along(x_ref, z, 0, 1).start()

    ti = lax.broadcasted_iota(jnp.int32, (tokens, tokens), 0)
    tj = lax.broadcasted_iota(jnp.int32, (tokens, tokens), 1)
    earlier = jnp.where(ti < tj, 1.0, 0.0).astype(bf16)
    expert = z * near + lax.broadcasted_iota(jnp.int32, (near, tokens), 0)
    place_in = lax.broadcasted_iota(jnp.int32, (near, cap, tokens), 1).astype(f32)

    def send_rows(block, i):
        peer = lax.rem(me + i, near)
        return pltpu.make_async_remote_copy(
            src_ref=rows_out.at[block, peer],
            dst_ref=rows_in.at[block, me],
            send_sem=dsend.at[block, i],
            recv_sem=drecv.at[block, i],
            device_id=place(peer),
            device_id_type=MESH,
        )

    def keep_rows(block):
        return pltpu.make_async_copy(
            rows_out.at[block, me], rows_in.at[block, me], local.at[0, block]
        )

    def send_back(block, i):
        peer = lax.rem(me + i, near)
        return pltpu.make_async_remote_copy(
            src_ref=made.at[block, peer],
            dst_ref=back.at[block, me],
            send_sem=rsend.at[block, i],
            recv_sem=rrecv.at[block, i],
            device_id=place(peer),
            device_id_type=MESH,
        )

    def keep_back(block):
        return pltpu.make_async_copy(made.at[block, me], back.at[block, me], local.at[1, block])

    def each(what):
        def one(i, carry):
            what(i)
            return carry

        lax.fori_loop(1, near, one, 0)

    def dispatch(block, values, names, weights):
        named, weight = None, None
        for k in range(top):
            hit = names[k : k + 1, :] == expert
            one = jnp.where(hit, 1.0, 0.0)
            share = jnp.where(hit, weights[k : k + 1, :], 0.0)
            named = one if named is None else named + one
            weight = share if weight is None else weight + share
        slot = jnp.dot(named.astype(bf16), earlier, preferred_element_type=f32)
        slot = jnp.where(named > 0.5, slot, -1.0)
        pick = slot[:, None, :] == place_in
        rough = weight.astype(bf16).astype(f32)
        rest = weight - rough

        def table(v):
            return jnp.where(pick, v, 0.0).reshape(near * cap, tokens).astype(bf16)

        high[block] = table(rough[:, None, :])
        low[block] = table(rest[:, None, :])
        select = table(jnp.ones((near, 1, tokens), f32))
        chunk = 512
        for at in range(0, width, chunk):
            rows = jnp.dot(select, values[:, at : at + chunk], preferred_element_type=f32)
            rows_out[block, :, :, at : at + chunk] = rows.astype(bf16).reshape(near, cap, chunk)
        each(lambda i: send_rows(block, i).start())
        keep_rows(block).start()

    def arrive(s):
        hops, from_below, block = plane_order(z, planes, s)
        way = 1 - from_below
        along(tok.at[block], block, hops - 1, way).wait_recv()
        onward = jnp.where(from_below == 1, z + 1, z - 1)

        @pl.when((onward >= 0) & (onward < planes))
        def _():
            along(tok.at[block], block, hops, way).start()

        source = lax.rem(z - block + planes, planes)
        for kind in range(2):
            tell(kind, source).wait_recv()
        dispatch(block, tok[block], names_in[block], shares_in[block])
        return block

    hidden = gate.shape[1]
    flat = near * cap

    def serve(block):
        keep_rows(block).wait()
        each(lambda i: send_rows(block, i).wait_recv())
        tile = 256

        def lift(n, carry):
            cols = pl.ds(pl.multiple_of(n * tile, tile), tile)
            rows = rows_in[block].reshape(flat, width)
            g = jnp.minimum(jnp.dot(rows, gate[:, cols], preferred_element_type=f32), clamp_limit)
            u = jnp.dot(rows, up[:, cols], preferred_element_type=f32)
            u = jnp.clip(u, -clamp_limit, clamp_limit)
            active[:, cols] = ((u + 1.0) * g * jax.nn.sigmoid(sigmoid_slope * g)).astype(bf16)
            return carry

        lax.fori_loop(0, hidden // tile, lift, 0)

        def lower(n, carry):
            cols = pl.ds(pl.multiple_of(n * tile, tile), tile)
            y = jnp.dot(active[...], down[:, cols], preferred_element_type=f32)
            made[block, :, :, cols] = y.astype(bf16).reshape(near, cap, tile)
            return carry

        lax.fori_loop(0, width // tile, lower, 0)

    def give(block):
        each(lambda i: send_back(block, i).start())
        keep_back(block).start()

    def gathered(block, at, chunk):
        rows = back[block, :, :, at : at + chunk].reshape(flat, chunk)
        dims = (((0,), (0,)), ((), ()))
        return lax.dot_general(
            high[block], rows, dims, preferred_element_type=f32
        ) + lax.dot_general(low[block], rows, dims, preferred_element_type=f32)

    chunk = 512
    chunks = width // chunk

    def send_part(block, i, c):
        return pltpu.make_async_remote_copy(
            src_ref=part.at[block, :, c * chunk : (c + 1) * chunk],
            dst_ref=part_in.at[z, :, c * chunk : (c + 1) * chunk],
            send_sem=psend.at[i, c],
            recv_sem=precv.at[i, c],
            device_id=plane(block),
            device_id_type=MESH,
        )

    middle = planes // 2
    in_low = z < middle
    outermost = (z == 0) | (z == planes - 1)
    innermost = (z == middle - 1) | (z == middle)
    inward = jnp.where(in_low, z + 1, z - 1)

    def is_far(block):
        return in_low == (block >= middle)

    def pass_on(block, c):
        slot = lax.rem(block, middle)
        return pltpu.make_async_remote_copy(
            src_ref=part.at[block, :, c * chunk : (c + 1) * chunk],
            dst_ref=passing.at[slot, :, c * chunk : (c + 1) * chunk],
            send_sem=csend.at[slot, c],
            recv_sem=crecv.at[slot, c],
            device_id=plane(inward),
            device_id_type=MESH,
        )

    def landed(block):
        keep_back(block).wait()
        each(lambda i: send_back(block, i).wait_recv())

    def collect(block):
        landed(block)
        adds = is_far(block) & jnp.logical_not(outermost)
        inner_far = is_far(block) & jnp.logical_not(innermost)
        slot = lax.rem(block, middle)
        for c in range(chunks):
            at = c * chunk

            @pl.when(adds)
            def _():
                pass_on(block, c).wait_recv()
                value = gathered(block, at, chunk) + passing[slot, :, at : at + chunk].astype(f32)
                part[block, :, at : at + chunk] = value.astype(bf16)

            @pl.when(jnp.logical_not(adds))
            def _():
                part[block, :, at : at + chunk] = gathered(block, at, chunk).astype(bf16)

            @pl.when(inner_far)
            def _():
                pass_on(block, c).start()

            @pl.when(jnp.logical_not(inner_far))
            def _():
                send_part(block, lax.rem(block - z + planes, planes), c).start()

    blocks = [z]
    dispatch(z, x_ref[...], names_ref[...], shares_ref[...])
    served = 0
    for s in range(1, planes):
        blocks.append(arrive(s))
        if s == planes - 2:
            for load in loads:
                load.wait()
            serve(blocks[0])
            served = 1
    if not served:
        for load in loads:
            load.wait()
        serve(blocks[0])
    last = list(range(middle, planes))
    first = list(range(1, middle))
    for s in last[:-1]:
        serve(blocks[s])
        give(blocks[s])
    for s in first:
        serve(blocks[s])
    for s in last[-1:]:
        serve(blocks[s])
        give(blocks[s])
    for s in first:
        give(blocks[s])
    give(blocks[0])
    for s in last + first:
        collect(blocks[s])
    landed(z)
    for at in range(0, width, chunk):
        cols = slice(at, at + chunk)
        total[:, cols] = stream_ref[:, cols] + gathered(z, at, chunk)

    def comes(source):
        near_by = jnp.logical_not(is_far(source))
        edge = (source == middle - 1) | (source == middle)
        return near_by | edge

    for i in range(1, planes):
        source = lax.rem(z - i + planes, planes)

        @pl.when(comes(source))
        def _():
            for c in range(chunks):
                cols = slice(c * chunk, (c + 1) * chunk)
                send_part(lax.rem(z + i, planes), i, c).wait_recv()
                total[:, cols] += part_in[source, :, cols].astype(f32)

    out_ref[...] = total[...].astype(bf16)
    for i in range(1, planes):
        for kind in range(2):
            tell(kind, i).wait_send()
        block = lax.rem(z + i, planes)
        inner_far = is_far(block) & jnp.logical_not(innermost)

        @pl.when(inner_far)
        def _():
            for c in range(chunks):
                pass_on(block, c).wait_send()

        @pl.when(jnp.logical_not(inner_far))
        def _():
            for c in range(chunks):
                send_part(block, i, c).wait_send()

    for block in range(planes):
        each(lambda i: send_rows(block, i).wait_send())
        each(lambda i: send_back(block, i).wait_send())

    @pl.when(up_open)
    def _():
        along(x_ref, z, 0, 0).wait_send()

    @pl.when(down_open)
    def _():
        along(x_ref, z, 0, 1).wait_send()

    for step in range(1, planes):

        @pl.when(up_open & (z - step >= 0))
        def _():
            along(tok.at[z], z, step, 0).wait_send()

        @pl.when(down_open & (z + step < planes))
        def _():
            along(tok.at[z], z, step, 1).wait_send()


def experts(
    planes, inner, dp_count, cap, tokens_in, stream, names, shares, gate_w, up_w, down_w
):
    near = inner * dp_count
    tokens, width = tokens_in.shape
    hidden = gate_w.shape[2]
    bf16, f32 = jnp.bfloat16, jnp.float32
    anywhere = pl.BlockSpec(memory_space=pl.ANY)
    inside = pl.BlockSpec(memory_space=pltpu.VMEM)
    dma = pltpu.SemaphoreType.DMA
    rows = pltpu.VMEM((planes, near, cap, width), bf16)
    table = pltpu.VMEM((planes, near * cap, tokens), bf16)
    blocks = pltpu.VMEM((planes, tokens, width), bf16)
    return pl.pallas_call(
        functools.partial(experts_kernel, planes, inner, dp_count, names.shape[0]),
        out_shape=jax.ShapeDtypeStruct((tokens, width), bf16),
        in_specs=[inside] * 4 + [anywhere] * 3,
        out_specs=inside,
        scratch_shapes=[
            pltpu.VMEM((width, hidden), bf16),
            pltpu.VMEM((width, hidden), bf16),
            pltpu.VMEM((hidden, width), bf16),
            blocks,
            pltpu.VMEM((planes,) + names.shape, names.dtype),
            pltpu.VMEM((planes,) + shares.shape, f32),
            rows, rows, rows, rows, table, table,
            pltpu.VMEM((near * cap, hidden), bf16),
            blocks, blocks,
            pltpu.VMEM((tokens, width), f32),
            pltpu.VMEM((planes // 2, tokens, width), bf16),
            dma((3,)), dma((2, planes)), dma((2, planes)), dma((2, planes)), dma((2, planes)),
            dma((planes, near)), dma((planes, near)), dma((planes, near)), dma((planes, near)),
            dma((planes, width // 512)), dma((planes, width // 512)),
            dma((planes // 2, width // 512)), dma((planes // 2, width // 512)), dma((2, planes)),
        ],
        compiler_params=pltpu.CompilerParams(
            collective_id=3, has_side_effects=True, vmem_limit_bytes=60 * 1024 * 1024
        ),
        cost_estimate=pl.CostEstimate(flops=10**11, bytes_accessed=10**8, transcendentals=0),
        name="experts",
    )(tokens_in, stream, names, shares, gate_w, up_w, down_w)


def lowest(offset):
    return offset & -offset


def mixer_kernel(
    n, inner, dp_count, x_hbm, b_hbm, c_hbm, z_hbm, r_hbm, w_hbm, step_ref, tx_ref, tb_ref, tc_ref,
    rate_ref, gain_ref, ffn_gain_ref, stream_ref, ffn_ref,
    ins, gate_v, res_v, w_all, steps, taps, rates, halo_in, halo, pad, reads, inside_ref,
    fade_f, fade_b, own_f, own_b, carry, send_f, send_b, got_f, got_b, ybuf, ytok, gated, mixed,
    cols, rows_t, squares,
    in_s, in_r, step_s, step_r, tap_s, tap_r, rate_s, rate_r, halo_s, halo_r,
    f_s, f_r, b_s, b_r, y_s, y_r, w_s, w_r, own_in, local,
):
    f32, bf16 = jnp.float32, jnp.bfloat16
    sp, dp = lax.axis_index("sp"), lax.axis_index("dp")
    z, x = sp // inner, lax.rem(sp, inner)
    planes = n // inner
    tokens, width = stream_ref.shape
    span = ins.shape[3]
    locals_n = own_f.shape[0]
    lanes = span // locals_n
    groups = locals_n * inner
    per_group = lanes // HEAD_DIM
    columns = 2 * per_group
    taps_n, wide = tx_ref.shape
    half = taps_n // 2
    depth = w_hbm.shape[0]
    piece = min(depth, 128)
    pieces = depth // piece
    bits = [1 << i for i in range(dp_count.bit_length() - 1)]
    flows = (x_hbm, b_hbm, c_hbm)
    tap_refs = (tx_ref, tb_ref, tc_ref)

    def mate(bit):
        return dp + bit * (1 - 2 * lax.rem(dp // bit, 2))

    greet([{"sp": lax.rem(sp + i, n)} for i in range(1, n)] + [{"dp": mate(b)} for b in bits])

    def remote(src, dst, send, recv, where):
        return pltpu.make_async_remote_copy(
            src_ref=src, dst_ref=dst, send_sem=send, recv_sem=recv,
            device_id=where, device_id_type=MESH,
        )

    def spot(start, size):
        return pl.ds(pl.multiple_of(start, size), size)

    def give_step(i):
        return remote(
            step_ref, steps.at[x], step_s.at[i], step_r.at[i],
            {"sp": z * inner + lax.rem(x + i, inner)},
        )

    mine = spot(sp * wide, wide)

    def give_tap(k, i):
        return remote(
            tap_refs[k], taps.at[k, 0:taps_n, mine], tap_s.at[k, i], tap_r.at[k, i],
            {"sp": lax.rem(sp + i, n)},
        )

    def give_rate(i):
        return remote(
            rate_ref, rates.at[sp], rate_s.at[i], rate_r.at[i], {"sp": lax.rem(sp + i, n)}
        )

    def give_halo(way, k, to):
        first = 0 if way else tokens - 8
        return remote(
            flows[k].at[first : first + 8, to * span : (to + 1) * span],
            halo_in.at[way, k], halo_s.at[way, k, to], halo_r.at[way, k],
            {"sp": (z + 1 - 2 * way) * inner + to},
        )

    def give_in(k, q, i):
        peer = lax.rem(x + i, inner)
        return remote(
            flows[k].at[:, spot(peer * span + q * lanes, lanes)],
            ins.at[k, x, :, spot(q * lanes, lanes)],
            in_s.at[k, q, i], in_r.at[k, q, i], {"sp": z * inner + peer},
        )

    def give_weight(offset, bit, c):
        rows = slice(c * piece, (c + 1) * piece)
        src = w_hbm.at[rows] if offset == 0 else w_all.at[offset, rows]
        return remote(
            src, w_all.at[offset + bit, rows],
            w_s.at[offset, bits.index(bit), c], w_r.at[offset + bit, c], {"dp": mate(bit)},
        )

    has_above, has_below = z < planes - 1, z > 0
    sends_up = has_above & (x == inner - 1)
    sends_down = has_below & (x == 0)

    for i in range(1, inner):
        give_step(i).start()
    for i in range(1, n):
        for k in range(3):
            give_tap(k, i).start()
        give_rate(i).start()

    @pl.when(sends_up)
    def _():
        for k in range(3):
            for to in range(inner):
                give_halo(0, k, to).start()

    @pl.when(sends_down)
    def _():
        for k in range(3):
            for to in range(inner):
                give_halo(1, k, to).start()

    def begin(q, unused):
        for k in range(3):
            for i in range(1, inner):
                give_in(k, q, i).start()
        return unused

    lax.fori_loop(0, locals_n, begin, 0)
    owned = [
        pltpu.make_async_copy(
            flows[k].at[:, spot(x * span, span)], ins.at[k, x], own_in.at[k]
        )
        for k in range(3)
    ]
    for copy in owned:
        copy.start()
    for bit in reversed(bits):
        for c in range(pieces):
            give_weight(0, bit, c).start()
    keeps = [
        pltpu.make_async_copy(tap_refs[k], taps.at[k, 0:taps_n, mine], local.at[k])
        for k in range(3)
    ]
    keeps.append(pltpu.make_async_copy(rate_ref, rates.at[sp], local.at[3]))
    keeps.append(pltpu.make_async_copy(step_ref, steps.at[x], local.at[4]))
    for copy in keeps:
        copy.start()
    late_loads = [
        pltpu.make_async_copy(z_hbm, gate_v, local.at[5]),
        pltpu.make_async_copy(r_hbm, res_v, local.at[6]),
        pltpu.make_async_copy(w_hbm, w_all.at[0], local.at[7]),
    ]
    for copy in late_loads:
        copy.start()

    @pl.when(jnp.logical_not(has_below))
    def _():
        halo[0] = jnp.zeros(halo.shape[1:], f32)
        got_f[...] = jnp.zeros(got_f.shape, bf16)

    @pl.when(jnp.logical_not(has_above))
    def _():
        halo[1] = jnp.zeros(halo.shape[1:], f32)
        got_b[...] = jnp.zeros(got_b.shape, bf16)

    li = lax.broadcasted_iota(jnp.int32, (BLOCK, BLOCK), 0)
    si = lax.broadcasted_iota(jnp.int32, (BLOCK, BLOCK), 1)
    lower = jnp.where(li >= si, 1.0, 0.0).astype(f32)
    lane = lax.broadcasted_iota(jnp.int32, (1, lanes), 1)
    lane_head = lane // HEAD_DIM

    def spread_heads(values):
        out = values[0]
        for h in range(1, per_group):
            out = jnp.where(lane_head == h, values[h], out)
        return jnp.broadcast_to(out, (out.shape[0], lanes))

    for copy in keeps:
        copy.wait()
    for i in range(1, n):
        give_rate(i).wait_recv()
    step_columns = step_ref.shape[0]
    window = step_columns // inner
    held = rate_ref.shape[1]
    rate = jnp.zeros((1, BLOCK), f32)
    row_lane = lax.broadcasted_iota(jnp.int32, (1, BLOCK), 1)
    for t in range(planes):
        pair = rates[x * planes + t]
        for h in range(held):
            for d in range(2):
                rate = jnp.where(
                    row_lane == 2 * (t * held + h) + d, pair[d : d + 1, h : h + 1], rate
                )
    choose_row = lax.broadcasted_iota(jnp.int32, (step_columns, BLOCK), 0)
    choose_col = lax.broadcasted_iota(jnp.int32, (step_columns, BLOCK), 1)
    choose = jnp.where((choose_row == x * window + choose_col) & (choose_col < window), 1.0, 0.0)
    choose = choose.astype(bf16)
    for i in range(1, inner):
        give_step(i).wait_recv()
    for i in range(inner):
        v = lax.dot_general(
            steps[i], choose, (((0,), (0,)), ((), ())), preferred_element_type=f32
        )
        dt = jnp.maximum(v, 0.0) + jnp.log(1.0 + jnp.exp(-jnp.abs(v)))
        a = dt * rate
        inc = jnp.dot(lower, a, precision=highest, preferred_element_type=f32)
        exc = inc - a
        for k, value in enumerate((inc, exc, dt)):
            turned = value.T
            for q in range(locals_n):
                at = slice(q * columns, (q + 1) * columns)
                cols[k, i, q, :, 0:columns] = value[:, at]
                rows_t[k, i, q, 0:columns, :] = turned[at, :]

    for i in range(1, n):
        for k in range(3):
            give_tap(k, i).wait_recv()

    @pl.when(has_below)
    def _():
        for k in range(3):
            give_halo(0, k, 0).wait_recv()
        halo[0] = halo_in[0].astype(f32)

    @pl.when(has_above)
    def _():
        for k in range(3):
            give_halo(1, k, 0).wait_recv()
        halo[1] = halo_in[1].astype(f32)

    for copy in owned:
        copy.wait()

    def pass_f(q):
        return remote(
            send_f.at[q], got_f.at[q], f_s.at[q], f_r.at[q], {"sp": sp + inner}
        )

    def pass_b(q):
        return remote(
            send_b.at[q], got_b.at[q], b_s.at[q], b_r.at[q], {"sp": sp - inner}
        )

    def onward_f(q, value):
        for i in range(inner):
            value = carry[q, i, 0:1, :] * value + own_f[q, i]
        send_f[q] = value.astype(bf16)
        pass_f(q).start()

    def onward_b(q, value):
        for i in reversed(range(inner)):
            value = carry[q, i, 1:2, :] * value + own_b[q, i]
        send_b[q] = value.astype(bf16)
        pass_b(q).start()

    def local_part(q):
        at = spot(q * lanes, lanes)
        wide_at = spot(x * span + q * lanes, lanes)
        length = inner * tokens
        for k in range(3):
            pad[k, 8 - half : 8, :] = halo[0, k, 8 - half : 8, at]
            pad[k, length + 8 : length + 8 + half, :] = halo[1, k, 0:half, at]
            for i in range(inner):
                pad[k, i * tokens + 8 : (i + 1) * tokens + 8, :] = ins[k, i, :, at].astype(f32)

        def conv(k, i):
            total = None
            for j in range(taps_n):
                first = i * tokens + 8 - half + j
                term = pad[k, first : first + tokens, :] * taps[k, j : j + 1, wide_at]
                total = term if total is None else total + term
            return total * jax.nn.sigmoid(total)

        for i in range(inner):
            xs = conv(0, i)
            write = conv(1, i).astype(bf16)
            read = conv(2, i).astype(bf16)
            reads[q, i] = read
            inc, exc, dt = (cols[k, i, q, :, 0:columns] for k in range(3))
            inct, exct, dtt = (rows_t[k, i, q, 0:columns, :] for k in range(3))
            tot = inc[BLOCK - 1 : BLOCK, :]
            heads = range(per_group)
            fwd = [inc[:, 2 * h : 2 * h + 1] for h in heads]
            bwd = [exc[:, 2 * h + 1 : 2 * h + 2] for h in heads]
            tot_f = [tot[:, 2 * h : 2 * h + 1] for h in heads]
            tot_b = [tot[:, 2 * h + 1 : 2 * h + 2] for h in heads]
            wf = spread_heads(
                [dt[:, 2 * h : 2 * h + 1] * jnp.exp(fwd[h] - tot_f[h]) for h in heads]
            )
            wb = spread_heads([dt[:, 2 * h + 1 : 2 * h + 2] * jnp.exp(-bwd[h]) for h in heads])
            both = jnp.concatenate([(xs * wf).astype(bf16), (xs * wb).astype(bf16)], axis=1)
            sums = lax.dot_general(
                write, both, (((0,), (0,)), ((), ())), preferred_element_type=f32
            )
            own_f[q, i] = sums[:, 0:lanes]
            own_b[q, i] = sums[:, lanes : 2 * lanes]
            carry[q, i, 0:1, :] = spread_heads([jnp.exp(-tot_f[h]) for h in heads])
            carry[q, i, 1:2, :] = spread_heads([jnp.exp(-tot_b[h]) for h in heads])
            fade_f[q, i] = spread_heads([jnp.exp(-fwd[h]) for h in heads])
            fade_b[q, i] = spread_heads([jnp.exp(bwd[h] - tot_b[h]) for h in heads])
            scores = lax.dot_general(
                read, write, (((1,), (1,)), ((), ())), preferred_element_type=f32
            )
            inside = None
            for h in heads:
                f, b = 2 * h, 2 * h + 1
                power = jnp.where(
                    li >= si,
                    inct[f : f + 1, :] - inc[:, f : f + 1],
                    exc[:, b : b + 1] - exct[b : b + 1, :],
                )
                df, db = dtt[f : f + 1, :], dtt[b : b + 1, :]
                scale = jnp.where(li > si, df, jnp.where(li == si, df + db, db))
                weights = (scores * jnp.exp(power) * scale).astype(bf16)
                xh = jnp.where(lane_head == h, xs, 0.0).astype(bf16)
                term = jnp.dot(weights, xh, preferred_element_type=f32)
                inside = term if inside is None else inside + term
            inside_ref[q, i] = inside

        @pl.when(has_above & jnp.logical_not(has_below))
        def _():
            onward_f(q, jnp.zeros((STATE, lanes), f32))

        @pl.when(has_below & jnp.logical_not(has_above))
        def _():
            onward_b(q, jnp.zeros((STATE, lanes), f32))

    def give_y(q, to):
        i = lax.rem(to - x + inner, inner)
        return remote(
            ybuf.at[q, to], ytok.at[:, spot((x * locals_n + q) * lanes, lanes)],
            y_s.at[i, q], y_r.at[i, q], {"sp": z * inner + to},
        )

    def finish(q):
        enter_f, enter_b = [], [None] * inner
        value = got_f[q].astype(f32)
        for i in range(inner):
            enter_f.append(value.astype(bf16))
            if i < inner - 1:
                value = carry[q, i, 0:1, :] * value + own_f[q, i]
        value = got_b[q].astype(f32)
        for i in reversed(range(inner)):
            enter_b[i] = value.astype(bf16)
            if i > 0:
                value = carry[q, i, 1:2, :] * value + own_b[q, i]
        for i in range(inner):
            entering = jnp.concatenate([enter_f[i], enter_b[i]], axis=1)
            moved = jnp.dot(reads[q, i], entering, preferred_element_type=f32)
            total = (
                inside_ref[q, i]
                + moved[:, 0:lanes] * fade_f[q, i]
                + moved[:, lanes : 2 * lanes] * fade_b[q, i]
            )
            ybuf[q, i] = total.astype(bf16)

            @pl.when(x == i)
            def _():
                ytok[:, spot((x * locals_n + q) * lanes, lanes)] = ybuf[q, i]

            @pl.when(x != i)
            def _():
                give_y(q, i).start()

    gap = 2
    late_f = gap * z
    late_b = gap * (planes - 1 - z)
    late = jnp.maximum(late_f, late_b)

    def turn(t, unused):
        f, b, g = t - late_f, t - late_b, t - late

        @pl.when(t < locals_n)
        def _():
            for k in range(3):
                for i in range(1, inner):
                    give_in(k, t, i).wait_recv()
            local_part(t)

        @pl.when(has_below & (f >= 0) & (f < locals_n))
        def _():
            pass_f(f).wait_recv()

            @pl.when(has_above)
            def _():
                onward_f(f, got_f[f].astype(f32))

        @pl.when(has_above & (b >= 0) & (b < locals_n))
        def _():
            pass_b(b).wait_recv()

            @pl.when(has_below)
            def _():
                onward_b(b, got_b[b].astype(f32))

        @pl.when((g >= 0) & (g < locals_n))
        def _():
            finish(g)

        return unused

    lax.fori_loop(0, locals_n + gap * (planes - 1), turn, 0)

    per_norm = groups // NORM_GROUPS
    squares[...] = jnp.zeros(squares.shape, f32)
    for copy in late_loads:
        copy.wait()

    def gate_group(g, unused):
        owner, q = g // locals_n, lax.rem(g, locals_n)

        @pl.when(owner != x)
        def _():
            i = lax.rem(x - owner + inner, inner)
            remote(
                ybuf.at[q, 0], ytok.at[:, spot(g * lanes, lanes)],
                y_s.at[i, q], y_r.at[i, q], {"sp": z * inner + owner},
            ).wait_recv()

        at = spot(g * lanes, lanes)
        gate = gate_v[:, at].astype(f32)
        value = ytok[:, at].astype(f32) * (gate * jax.nn.sigmoid(gate))
        gated[g] = value
        squares[g // per_norm] += jnp.sum(value * value, axis=1, keepdims=True)
        return unused

    lax.fori_loop(0, groups, gate_group, 0)

    def scale(g, unused):
        at = spot(g * lanes, lanes)
        mean = squares[g // per_norm] * (1.0 / (per_norm * lanes))
        value = gated[g] * lax.rsqrt(mean + epsilon) * gain_ref[:, at]
        mixed[:, at] = value.astype(bf16)
        return unused

    lax.fori_loop(0, groups, scale, 0)

    stream_ref[...] = res_v[...].astype(f32)
    order = sorted(range(1, dp_count), key=lambda o: (-lowest(o), o))

    def come(offset, c):
        give_weight(offset - lowest(offset), lowest(offset), c).wait_recv()
        for bit in bits:
            if bit < lowest(offset):
                give_weight(offset, bit, c).start()

    def project(offset, first, last):
        block = dp
        for bit in bits:
            if offset & bit:
                block = block + bit * (1 - 2 * lax.rem(dp // bit, 2))
        part = mixed[:, pl.ds(pl.multiple_of(block * depth + first, 128), last - first)]

        def tile(t, unused):
            at = spot(t * 512, 512)
            stream_ref[:, at] += jnp.dot(
                part, w_all[offset, first:last, at], preferred_element_type=f32
            )
            return unused

        lax.fori_loop(0, width // 512, tile, 0)

    early = depth - piece
    for offset in order:
        for c in range(pieces - 1):
            come(offset, c)
    project(0, 0, depth)
    for offset in order:
        if early:
            project(offset, 0, early)
    for offset in order:
        come(offset, pieces - 1)
        project(offset, early, depth)
    total = jnp.zeros((tokens, 1), f32)
    for at in range(0, width, 512):
        value = stream_ref[:, at : at + 512]
        total = total + jnp.sum(value * value, axis=1, keepdims=True)
    root = lax.rsqrt(total * (1.0 / width) + epsilon)
    for at in range(0, width, 512):
        value = stream_ref[:, at : at + 512] * root * ffn_gain_ref[:, at : at + 512]
        ffn_ref[:, at : at + 512] = value.astype(bf16)

    for i in range(1, inner):
        give_step(i).wait_send()
    for i in range(1, n):
        for k in range(3):
            give_tap(k, i).wait_send()
        give_rate(i).wait_send()

    @pl.when(sends_up)
    def _():
        for k in range(3):
            for to in range(inner):
                give_halo(0, k, to).wait_send()

    @pl.when(sends_down)
    def _():
        for k in range(3):
            for to in range(inner):
                give_halo(1, k, to).wait_send()

    def drain(q, unused):
        for k in range(3):
            for i in range(1, inner):
                give_in(k, q, i).wait_send()
        for i in range(1, inner):
            give_y(q, lax.rem(x + i, inner)).wait_send()

        @pl.when(has_above)
        def _():
            pass_f(q).wait_send()

        @pl.when(has_below)
        def _():
            pass_b(q).wait_send()

        return unused

    lax.fori_loop(0, locals_n, drain, 0)
    for offset in range(dp_count):
        for bit in bits:
            if offset == 0 or bit < lowest(offset):
                for c in range(pieces):
                    give_weight(offset, bit, c).wait_send()


def mixer(
    n, inner, dp_count, signal, write, read, gate, residual, weight, steps,
    conv_x, conv_b, conv_c, rates, gain, ffn_gain,
):
    f32, bf16 = jnp.float32, jnp.bfloat16
    tokens, width = signal.shape
    groups = write.shape[1] // STATE
    lanes = width // groups
    own = groups // inner
    span = width // inner
    depth = weight.shape[0]
    pieces = depth // min(depth, 128)
    bits = dp_count.bit_length() - 1
    inside = pl.BlockSpec(memory_space=pltpu.VMEM)
    anywhere = pl.BlockSpec(memory_space=pl.ANY)
    dma = pltpu.SemaphoreType.DMA
    vmem = pltpu.VMEM
    tile = vmem((own, inner, tokens, lanes), f32)
    state = vmem((own, inner, STATE, lanes), f32)
    small = vmem((own, STATE, lanes), bf16)
    flat = vmem((tokens, width), bf16)
    return pl.pallas_call(
        functools.partial(mixer_kernel, n, inner, dp_count),
        out_shape=(
            jax.ShapeDtypeStruct((tokens, width), f32),
            jax.ShapeDtypeStruct((tokens, width), bf16),
        ),
        in_specs=[anywhere] * 6 + [inside] * 7,
        out_specs=(inside, inside),
        scratch_shapes=[
            vmem((3, inner, tokens, span), bf16), flat, flat,
            vmem((dp_count, depth, width), bf16),
            vmem((inner,) + steps.shape, bf16),
            vmem((3, 8, width), f32),
            vmem((n,) + rates.shape, f32),
            vmem((2, 3, 8, span), bf16),
            vmem((2, 3, 8, span), f32),
            vmem((3, inner * tokens + 16, lanes), f32),
            vmem((own, inner, tokens, STATE), bf16),
            tile, tile, tile, state, state,
            vmem((own, inner, 8, lanes), f32),
            small, small, small, small,
            vmem((own, inner, tokens, lanes), bf16), flat,
            vmem((groups, tokens, lanes), f32), flat,
            vmem((3, inner, own, tokens, 8), f32),
            vmem((3, inner, own, 8, tokens), f32),
            vmem((NORM_GROUPS, tokens, 1), f32),
            dma((3, own, inner)), dma((3, own, inner)), dma((inner,)), dma((inner,)),
            dma((3, n)), dma((3, n)), dma((n,)), dma((n,)), dma((2, 3, inner)), dma((2, 3)),
            dma((own,)), dma((own,)), dma((own,)), dma((own,)),
            dma((inner, own)), dma((inner, own)),
            dma((dp_count, bits, pieces)), dma((dp_count, pieces)), dma((3,)), dma((8,)),
        ],
        compiler_params=pltpu.CompilerParams(
            collective_id=1, has_side_effects=True, vmem_limit_bytes=56 * 1024 * 1024
        ),
        cost_estimate=pl.CostEstimate(
            flops=40 * 10**9, bytes_accessed=4 * tokens * width * 2, transcendentals=0
        ),
        name="mixer",
    )(
        signal, write, read, gate, residual, weight, steps, conv_x, conv_b, conv_c, rates,
        gain.reshape(1, width), ffn_gain.reshape(1, width),
    )


def per_device(
    residual_in, ssm_input, state_b, state_c, step_raw, gate_input, conv_x, conv_b, conv_c,
    decay_rate, mix_gain, out_weight, ffn_gain, routing, route_weight, gate_w, up_w, down_w,
):
    sp_count = lax.axis_size("sp")
    dp_count = lax.axis_size("dp")
    inner = dp_count // 2
    token_count = residual_in.shape[1]
    stream, ffn_input = mixer(
        sp_count, inner, dp_count, ssm_input[0], state_b[0], state_c[0], gate_input[0],
        residual_in[0], out_weight, step_raw[0].T, conv_x, conv_b, conv_c, decay_rate,
        mix_gain, ffn_gain,
    )
    top_count = routing.shape[2]
    planes = sp_count // inner
    capacity = 4 * token_count * top_count // (2 * sp_count * dp_count)
    return experts(
        planes, inner, dp_count, capacity, ffn_input, stream, routing[0].T, route_weight[0].T,
        gate_w, up_w, down_w,
    )[None]


def solution(mesh):
    return jax.shard_map(
        per_device,
        mesh=mesh,
        in_specs=(
            P("dp", "sp", None),
            P("dp", "sp", None),
            P("dp", "sp", None),
            P("dp", "sp", None),
            P("dp", "sp", None),
            P("dp", "sp", None),
            P(None, "sp"),
            P(None, "sp"),
            P(None, "sp"),
            P(None, "sp"),
            P(),
            P("dp", None),
            P(),
            P("dp", "sp", None),
            P("dp", "sp", None),
            P(("sp", "dp"), None, None),
            P(("sp", "dp"), None, None),
            P(("sp", "dp"), None, None),
        ),
        out_specs=P("dp", "sp", None),
        check_vma=False,
    )
```

```python
import functools

import jax
import jax.numpy as jnp
from jax import lax
from jax.experimental import pallas as pl
from jax.experimental.pallas import tpu as pltpu
from jax.sharding import PartitionSpec as P

HEAD_DIM = 64
STATE = 128
BLOCK = 128
NORM_GROUPS = 4
MESH = pl.DeviceIdType.MESH

highest = lax.Precision.HIGHEST
epsilon = 1e-05
clamp_limit = 7.0
sigmoid_slope = 1.702


def greet(peers):
    barrier = pltpu.get_barrier_semaphore()
    for peer in peers:
        pl.semaphore_signal(barrier, inc=1, device_id=peer, device_id_type=MESH)
    pl.semaphore_wait(barrier, len(peers))


def plane_order(z, planes, s):
    below, above = z, planes - 1 - z
    both = jnp.minimum(below, above)
    near = (s + 1) // 2
    low = jnp.where(below < above, 1, 0)
    turn = jnp.where(low == 1, s % 2, 1 - s % 2)
    from_below = jnp.where(s <= 2 * both, turn, 1 - low)
    hops = jnp.where(s <= 2 * both, near, s - both)
    return hops, from_below, z + hops * (1 - 2 * from_below)


def experts_kernel(
    planes, inner, dp_count, top, x_ref, stream_ref, names_ref, shares_ref, gate_hbm, up_hbm,
    down_hbm, out_ref, gate, up, down, tok, names_in, shares_in, rows_out, rows_in, made, back, high, low, active, part, part_in,
    total, passing, wsem, isend, irecv, zsend, zrecv, dsend, drecv, rsend, rrecv, psend, precv,
    csend, crecv, local,
):
    f32, bf16 = jnp.float32, jnp.bfloat16
    near = inner * dp_count
    tokens, width = x_ref.shape
    cap = rows_out.shape[2]
    sp, dp = lax.axis_index("sp"), lax.axis_index("dp")
    z, x = sp // inner, lax.rem(sp, inner)
    me = x * dp_count + dp

    def place(p):
        return {"sp": z * inner + p // dp_count, "dp": lax.rem(p, dp_count)}

    def plane(other):
        return {"sp": other * inner + x, "dp": dp}

    barrier = pltpu.get_barrier_semaphore()

    def call(i, carry):
        peer = lax.rem(me + i, near)
        pl.semaphore_signal(barrier, inc=1, device_id=place(peer), device_id_type=MESH)
        return carry

    lax.fori_loop(1, near, call, 0)
    for i in range(1, planes):
        pl.semaphore_signal(
            barrier, inc=1, device_id=plane(lax.rem(z + i, planes)), device_id_type=MESH
        )
    loads = [
        pltpu.make_async_copy(gate_hbm.at[0], gate, wsem.at[0]),
        pltpu.make_async_copy(up_hbm.at[0], up, wsem.at[1]),
        pltpu.make_async_copy(down_hbm.at[0], down, wsem.at[2]),
    ]
    for load in loads:
        load.start()
    pl.semaphore_wait(barrier, near - 1 + planes - 1)

    def tell(kind, i):
        return pltpu.make_async_remote_copy(
            src_ref=(names_ref, shares_ref)[kind],
            dst_ref=(names_in, shares_in)[kind].at[z],
            send_sem=isend.at[kind, i],
            recv_sem=irecv.at[kind, i],
            device_id=plane(lax.rem(z + i, planes)),
            device_id_type=MESH,
        )

    for i in range(1, planes):
        for kind in range(2):
            tell(kind, i).start()

    parts_n = 2
    share = width // parts_n

    def along(src, block, step, way, c):
        cut = slice(c * share, (c + 1) * share)
        return pltpu.make_async_remote_copy(
            src_ref=src.at[:, cut],
            dst_ref=tok.at[block, :, cut],
            send_sem=zsend.at[way, step, c],
            recv_sem=zrecv.at[way, step, c],
            device_id=plane(z + 1 - 2 * way),
            device_id_type=MESH,
        )

    up_open, down_open = z < planes - 1, z > 0

    @pl.when(up_open)
    def _():
        for c in range(parts_n):
            along(x_ref, z, 0, 0, c).start()

    @pl.when(down_open)
    def _():
        for c in range(parts_n):
            along(x_ref, z, 0, 1, c).start()

    ti = lax.broadcasted_iota(jnp.int32, (tokens, tokens), 0)
    tj = lax.broadcasted_iota(jnp.int32, (tokens, tokens), 1)
    earlier = jnp.where(ti < tj, 1.0, 0.0).astype(bf16)
    expert = z * near + lax.broadcasted_iota(jnp.int32, (near, tokens), 0)
    place_in = lax.broadcasted_iota(jnp.int32, (near, cap, tokens), 1).astype(f32)

    def send_rows(block, i, c):
        peer = lax.rem(me + i, near)
        cut = slice(c * share, (c + 1) * share)
        return pltpu.make_async_remote_copy(
            src_ref=rows_out.at[block, peer, :, cut],
            dst_ref=rows_in.at[block, me, :, cut],
            send_sem=dsend.at[block, i, c],
            recv_sem=drecv.at[block, i, c],
            device_id=place(peer),
            device_id_type=MESH,
        )

    def keep_rows(block):
        return pltpu.make_async_copy(
            rows_out.at[block, me], rows_in.at[block, me], local.at[0, block]
        )

    def send_back(block, i):
        peer = lax.rem(me + i, near)
        return pltpu.make_async_remote_copy(
            src_ref=made.at[block, peer],
            dst_ref=back.at[block, me],
            send_sem=rsend.at[block, i],
            recv_sem=rrecv.at[block, i],
            device_id=place(peer),
            device_id_type=MESH,
        )

    def keep_back(block):
        return pltpu.make_async_copy(made.at[block, me], back.at[block, me], local.at[1, block])

    def each(what):
        def one(i, carry):
            what(i)
            return carry

        lax.fori_loop(1, near, one, 0)

    def choose(block, names, weights):
        named, weight = None, None
        for k in range(top):
            hit = names[k : k + 1, :] == expert
            one = jnp.where(hit, 1.0, 0.0)
            share = jnp.where(hit, weights[k : k + 1, :], 0.0)
            named = one if named is None else named + one
            weight = share if weight is None else weight + share
        slot = jnp.dot(named.astype(bf16), earlier, preferred_element_type=f32)
        slot = jnp.where(named > 0.5, slot, -1.0)
        pick = slot[:, None, :] == place_in
        rough = weight.astype(bf16).astype(f32)
        rest = weight - rough

        def table(v):
            return jnp.where(pick, v, 0.0).reshape(near * cap, tokens).astype(bf16)

        high[block] = table(rough[:, None, :])
        low[block] = table(rest[:, None, :])
        return table(jnp.ones((near, 1, tokens), f32))

    def dispatch(block, select, ref, c):
        for at in range(c * share, (c + 1) * share, 512):
            rows = jnp.dot(select, ref[:, at : at + 512], preferred_element_type=f32)
            rows_out[block, :, :, at : at + 512] = rows.astype(bf16).reshape(near, cap, 512)
        each(lambda i: send_rows(block, i, c).start())
        if c == parts_n - 1:
            keep_rows(block).start()

    def arrive(s):
        hops, from_below, block = plane_order(z, planes, s)
        way = 1 - from_below
        onward = jnp.where(from_below == 1, z + 1, z - 1)
        source = lax.rem(z - block + planes, planes)
        for kind in range(2):
            tell(kind, source).wait_recv()
        select = choose(block, names_in[block], shares_in[block])
        for c in range(parts_n):
            along(tok.at[block], block, hops - 1, way, c).wait_recv()

            @pl.when((onward >= 0) & (onward < planes))
            def _():
                along(tok.at[block], block, hops, way, c).start()

            dispatch(block, select, tok.at[block], c)
        return block

    hidden = gate.shape[1]
    flat = near * cap

    def serve(block):
        keep_rows(block).wait()
        for c in range(parts_n):
            each(lambda i: send_rows(block, i, c).wait_recv())
        tile = 256

        def lift(n, carry):
            cols = pl.ds(pl.multiple_of(n * tile, tile), tile)
            rows = rows_in[block].reshape(flat, width)
            g = jnp.minimum(jnp.dot(rows, gate[:, cols], preferred_element_type=f32), clamp_limit)
            u = jnp.dot(rows, up[:, cols], preferred_element_type=f32)
            u = jnp.clip(u, -clamp_limit, clamp_limit)
            active[:, cols] = ((u + 1.0) * g * jax.nn.sigmoid(sigmoid_slope * g)).astype(bf16)
            return carry

        lax.fori_loop(0, hidden // tile, lift, 0)

        def lower(n, carry):
            cols = pl.ds(pl.multiple_of(n * tile, tile), tile)
            y = jnp.dot(active[...], down[:, cols], preferred_element_type=f32)
            made[block, :, :, cols] = y.astype(bf16).reshape(near, cap, tile)
            return carry

        lax.fori_loop(0, width // tile, lower, 0)

    def give(block):
        each(lambda i: send_back(block, i).start())
        keep_back(block).start()

    def gathered(block, at, chunk):
        rows = back[block, :, :, at : at + chunk].reshape(flat, chunk)
        dims = (((0,), (0,)), ((), ()))
        return lax.dot_general(
            high[block], rows, dims, preferred_element_type=f32
        ) + lax.dot_general(low[block], rows, dims, preferred_element_type=f32)

    chunk = 512
    chunks = width // chunk

    def send_part(block, i, c):
        return pltpu.make_async_remote_copy(
            src_ref=part.at[block, :, c * chunk : (c + 1) * chunk],
            dst_ref=part_in.at[z, :, c * chunk : (c + 1) * chunk],
            send_sem=psend.at[i, c],
            recv_sem=precv.at[i, c],
            device_id=plane(block),
            device_id_type=MESH,
        )

    middle = planes // 2
    in_low = z < middle
    outermost = (z == 0) | (z == planes - 1)
    innermost = (z == middle - 1) | (z == middle)
    inward = jnp.where(in_low, z + 1, z - 1)

    def is_far(block):
        return in_low == (block >= middle)

    def pass_on(block, c):
        slot = lax.rem(block, middle)
        return pltpu.make_async_remote_copy(
            src_ref=part.at[block, :, c * chunk : (c + 1) * chunk],
            dst_ref=passing.at[slot, :, c * chunk : (c + 1) * chunk],
            send_sem=csend.at[slot, c],
            recv_sem=crecv.at[slot, c],
            device_id=plane(inward),
            device_id_type=MESH,
        )

    def landed(block):
        keep_back(block).wait()
        each(lambda i: send_back(block, i).wait_recv())

    def collect(block):
        landed(block)
        adds = is_far(block) & jnp.logical_not(outermost)
        inner_far = is_far(block) & jnp.logical_not(innermost)
        slot = lax.rem(block, middle)
        for c in range(chunks):
            at = c * chunk

            @pl.when(adds)
            def _():
                pass_on(block, c).wait_recv()
                value = gathered(block, at, chunk) + passing[slot, :, at : at + chunk].astype(f32)
                part[block, :, at : at + chunk] = value.astype(bf16)

            @pl.when(jnp.logical_not(adds))
            def _():
                part[block, :, at : at + chunk] = gathered(block, at, chunk).astype(bf16)

            @pl.when(inner_far)
            def _():
                pass_on(block, c).start()

            @pl.when(jnp.logical_not(inner_far))
            def _():
                send_part(block, lax.rem(block - z + planes, planes), c).start()

    blocks = [z]
    select = choose(z, names_ref[...], shares_ref[...])
    for c in range(parts_n):
        dispatch(z, select, x_ref, c)
    served = 0
    for s in range(1, planes):
        blocks.append(arrive(s))
        if s == planes - 2:
            for load in loads:
                load.wait()
            serve(blocks[0])
            served = 1
    if not served:
        for load in loads:
            load.wait()
        serve(blocks[0])
    last = list(range(middle, planes))
    first = list(range(1, middle))
    for s in last[:-1]:
        serve(blocks[s])
        give(blocks[s])
    for s in first:
        serve(blocks[s])
    for s in last[-1:]:
        serve(blocks[s])
        give(blocks[s])
    for s in first:
        give(blocks[s])
    give(blocks[0])
    for s in last + first:
        collect(blocks[s])
    landed(z)
    for at in range(0, width, chunk):
        cols = slice(at, at + chunk)
        total[:, cols] = stream_ref[:, cols] + gathered(z, at, chunk)

    def comes(source):
        near_by = jnp.logical_not(is_far(source))
        edge = (source == middle - 1) | (source == middle)
        return near_by | edge

    for i in range(1, planes):
        source = lax.rem(z - i + planes, planes)

        @pl.when(comes(source))
        def _():
            for c in range(chunks):
                cols = slice(c * chunk, (c + 1) * chunk)
                send_part(lax.rem(z + i, planes), i, c).wait_recv()
                total[:, cols] += part_in[source, :, cols].astype(f32)

    out_ref[...] = total[...].astype(bf16)
    for i in range(1, planes):
        for kind in range(2):
            tell(kind, i).wait_send()
        block = lax.rem(z + i, planes)
        inner_far = is_far(block) & jnp.logical_not(innermost)

        @pl.when(inner_far)
        def _():
            for c in range(chunks):
                pass_on(block, c).wait_send()

        @pl.when(jnp.logical_not(inner_far))
        def _():
            for c in range(chunks):
                send_part(block, i, c).wait_send()

    for block in range(planes):
        for c in range(parts_n):
            each(lambda i: send_rows(block, i, c).wait_send())
        each(lambda i: send_back(block, i).wait_send())

    @pl.when(up_open)
    def _():
        for c in range(parts_n):
            along(x_ref, z, 0, 0, c).wait_send()

    @pl.when(down_open)
    def _():
        for c in range(parts_n):
            along(x_ref, z, 0, 1, c).wait_send()

    for step in range(1, planes):

        @pl.when(up_open & (z - step >= 0))
        def _():
            for c in range(parts_n):
                along(tok.at[z], z, step, 0, c).wait_send()

        @pl.when(down_open & (z + step < planes))
        def _():
            for c in range(parts_n):
                along(tok.at[z], z, step, 1, c).wait_send()


def experts(
    planes, inner, dp_count, cap, tokens_in, stream, names, shares, gate_w, up_w, down_w
):
    near = inner * dp_count
    tokens, width = tokens_in.shape
    hidden = gate_w.shape[2]
    bf16, f32 = jnp.bfloat16, jnp.float32
    anywhere = pl.BlockSpec(memory_space=pl.ANY)
    inside = pl.BlockSpec(memory_space=pltpu.VMEM)
    dma = pltpu.SemaphoreType.DMA
    rows = pltpu.VMEM((planes, near, cap, width), bf16)
    table = pltpu.VMEM((planes, near * cap, tokens), bf16)
    blocks = pltpu.VMEM((planes, tokens, width), bf16)
    return pl.pallas_call(
        functools.partial(experts_kernel, planes, inner, dp_count, names.shape[0]),
        out_shape=jax.ShapeDtypeStruct((tokens, width), bf16),
        in_specs=[inside] * 4 + [anywhere] * 3,
        out_specs=inside,
        scratch_shapes=[
            pltpu.VMEM((width, hidden), bf16),
            pltpu.VMEM((width, hidden), bf16),
            pltpu.VMEM((hidden, width), bf16),
            blocks,
            pltpu.VMEM((planes,) + names.shape, names.dtype),
            pltpu.VMEM((planes,) + shares.shape, f32),
            rows, rows, rows, rows, table, table,
            pltpu.VMEM((near * cap, hidden), bf16),
            blocks, blocks,
            pltpu.VMEM((tokens, width), f32),
            pltpu.VMEM((planes // 2, tokens, width), bf16),
            dma((3,)), dma((2, planes)), dma((2, planes)),
            dma((2, planes, 2)), dma((2, planes, 2)), dma((planes, near, 2)),
            dma((planes, near, 2)), dma((planes, near)), dma((planes, near)),
            dma((planes, width // 512)), dma((planes, width // 512)),
            dma((planes // 2, width // 512)), dma((planes // 2, width // 512)), dma((2, planes)),
        ],
        compiler_params=pltpu.CompilerParams(
            collective_id=3, has_side_effects=True, vmem_limit_bytes=60 * 1024 * 1024
        ),
        cost_estimate=pl.CostEstimate(flops=10**11, bytes_accessed=10**8, transcendentals=0),
        name="experts",
    )(tokens_in, stream, names, shares, gate_w, up_w, down_w)


def lowest(offset):
    return offset & -offset


def mixer_kernel(
    n, inner, dp_count, x_hbm, b_hbm, c_hbm, z_hbm, r_hbm, w_hbm, step_ref, tx_ref, tb_ref, tc_ref,
    rate_ref, gain_ref, ffn_gain_ref, stream_ref, ffn_ref,
    ins, gate_v, res_v, w_all, steps, taps, rates, halo_in, halo, pad, reads, inside_ref,
    fade_f, fade_b, own_f, own_b, carry, send_f, send_b, got_f, got_b, ybuf, ytok, gated, mixed,
    cols, rows_t, squares,
    in_s, in_r, step_s, step_r, tap_s, tap_r, rate_s, rate_r, halo_s, halo_r,
    f_s, f_r, b_s, b_r, y_s, y_r, w_s, w_r, own_in, local,
):
    f32, bf16 = jnp.float32, jnp.bfloat16
    sp, dp = lax.axis_index("sp"), lax.axis_index("dp")
    z, x = sp // inner, lax.rem(sp, inner)
    planes = n // inner
    tokens, width = stream_ref.shape
    span = ins.shape[3]
    locals_n = own_f.shape[0]
    lanes = span // locals_n
    groups = locals_n * inner
    per_group = lanes // HEAD_DIM
    columns = 2 * per_group
    taps_n, wide = tx_ref.shape
    half = taps_n // 2
    depth = w_hbm.shape[0]
    piece = min(depth, 64)
    pieces = depth // piece
    bits = [1 << i for i in range(dp_count.bit_length() - 1)]
    flows = (x_hbm, b_hbm, c_hbm)
    tap_refs = (tx_ref, tb_ref, tc_ref)

    def mate(bit):
        return dp + bit * (1 - 2 * lax.rem(dp // bit, 2))

    greet([{"sp": lax.rem(sp + i, n)} for i in range(1, n)] + [{"dp": mate(b)} for b in bits])

    def remote(src, dst, send, recv, where):
        return pltpu.make_async_remote_copy(
            src_ref=src, dst_ref=dst, send_sem=send, recv_sem=recv,
            device_id=where, device_id_type=MESH,
        )

    def spot(start, size):
        return pl.ds(pl.multiple_of(start, size), size)

    def give_step(i):
        return remote(
            step_ref, steps.at[x], step_s.at[i], step_r.at[i],
            {"sp": z * inner + lax.rem(x + i, inner)},
        )

    mine = spot(sp * wide, wide)

    def give_tap(k, i):
        return remote(
            tap_refs[k], taps.at[k, 0:taps_n, mine], tap_s.at[k, i], tap_r.at[k, i],
            {"sp": lax.rem(sp + i, n)},
        )

    def give_rate(i):
        return remote(
            rate_ref, rates.at[sp], rate_s.at[i], rate_r.at[i], {"sp": lax.rem(sp + i, n)}
        )

    def give_halo(way, k, to):
        first = 0 if way else tokens - 8
        return remote(
            flows[k].at[first : first + 8, to * span : (to + 1) * span],
            halo_in.at[way, k], halo_s.at[way, k, to], halo_r.at[way, k],
            {"sp": (z + 1 - 2 * way) * inner + to},
        )

    def give_in(k, q, i):
        peer = lax.rem(x + i, inner)
        return remote(
            flows[k].at[:, spot(peer * span + q * lanes, lanes)],
            ins.at[k, x, :, spot(q * lanes, lanes)],
            in_s.at[k, q, i], in_r.at[k, q, i], {"sp": z * inner + peer},
        )

    odd_x = lax.rem(x, 2)
    shared, missing = odd_x * (pieces - 1), (1 - odd_x) * (pieces - 1)
    across = [o for o in range(2, dp_count, 2)]
    across = sorted(across, key=lambda o: (-lowest(o), o))

    def give_weight(offset, bit, c):
        rows = spot(c * piece, piece)
        src = w_hbm.at[rows] if offset == 0 else w_all.at[offset, rows]
        if bit:
            index, there = bits.index(bit), {"dp": mate(bit)}
        else:
            index, there = len(bits), {"sp": sp + 1 - 2 * odd_x}
        return remote(
            src, w_all.at[offset + bit, rows],
            w_s.at[offset, index, c], w_r.at[offset + bit, c], there,
        )

    def weight_in(offset, c):
        rows = spot(c * piece, piece)
        remote(
            w_hbm.at[rows], w_all.at[offset, rows],
            w_s.at[0, 0, c], w_r.at[offset, c], {"dp": mate(1)},
        ).wait_recv()

    def between(offset):
        return [bit for bit in bits if 1 < bit < lowest(offset)]

    has_above, has_below = z < planes - 1, z > 0
    sends_up = has_above & (x == inner - 1)
    sends_down = has_below & (x == 0)

    for i in range(1, inner):
        give_step(i).start()
    for i in range(1, n):
        for k in range(3):
            give_tap(k, i).start()
        give_rate(i).start()

    @pl.when(sends_up)
    def _():
        for k in range(3):
            for to in range(inner):
                give_halo(0, k, to).start()

    @pl.when(sends_down)
    def _():
        for k in range(3):
            for to in range(inner):
                give_halo(1, k, to).start()

    def begin(q, unused):
        for k in range(3):
            for i in range(1, inner):
                give_in(k, q, i).start()
        return unused

    lax.fori_loop(0, locals_n, begin, 0)
    owned = [
        pltpu.make_async_copy(
            flows[k].at[:, spot(x * span, span)], ins.at[k, x], own_in.at[k]
        )
        for k in range(3)
    ]
    for copy in owned:
        copy.start()
    for c in [shared] + list(range(1, pieces - 1)):
        for bit in reversed(bits[1:]):
            give_weight(0, bit, c).start()
    for c in range(pieces):
        give_weight(0, 1, c).start()
    keeps = [
        pltpu.make_async_copy(tap_refs[k], taps.at[k, 0:taps_n, mine], local.at[k])
        for k in range(3)
    ]
    keeps.append(pltpu.make_async_copy(rate_ref, rates.at[sp], local.at[3]))
    keeps.append(pltpu.make_async_copy(step_ref, steps.at[x], local.at[4]))
    for copy in keeps:
        copy.start()
    late_loads = [
        pltpu.make_async_copy(z_hbm, gate_v, local.at[5]),
        pltpu.make_async_copy(r_hbm, res_v, local.at[6]),
        pltpu.make_async_copy(w_hbm, w_all.at[0], local.at[7]),
    ]
    for copy in late_loads:
        copy.start()

    @pl.when(jnp.logical_not(has_below))
    def _():
        halo[0] = jnp.zeros(halo.shape[1:], f32)
        got_f[...] = jnp.zeros(got_f.shape, bf16)

    @pl.when(jnp.logical_not(has_above))
    def _():
        halo[1] = jnp.zeros(halo.shape[1:], f32)
        got_b[...] = jnp.zeros(got_b.shape, bf16)

    li = lax.broadcasted_iota(jnp.int32, (BLOCK, BLOCK), 0)
    si = lax.broadcasted_iota(jnp.int32, (BLOCK, BLOCK), 1)
    lower = jnp.where(li >= si, 1.0, 0.0).astype(f32)
    lane = lax.broadcasted_iota(jnp.int32, (1, lanes), 1)
    lane_head = lane // HEAD_DIM

    def spread_heads(values):
        out = values[0]
        for h in range(1, per_group):
            out = jnp.where(lane_head == h, values[h], out)
        return jnp.broadcast_to(out, (out.shape[0], lanes))

    for copy in keeps:
        copy.wait()
    for i in range(1, n):
        give_rate(i).wait_recv()
    step_columns = step_ref.shape[0]
    window = step_columns // inner
    held = rate_ref.shape[1]
    rate = jnp.zeros((1, BLOCK), f32)
    row_lane = lax.broadcasted_iota(jnp.int32, (1, BLOCK), 1)
    for t in range(planes):
        pair = rates[x * planes + t]
        for h in range(held):
            for d in range(2):
                rate = jnp.where(
                    row_lane == 2 * (t * held + h) + d, pair[d : d + 1, h : h + 1], rate
                )
    choose_row = lax.broadcasted_iota(jnp.int32, (step_columns, BLOCK), 0)
    choose_col = lax.broadcasted_iota(jnp.int32, (step_columns, BLOCK), 1)
    choose = jnp.where((choose_row == x * window + choose_col) & (choose_col < window), 1.0, 0.0)
    choose = choose.astype(bf16)
    for i in range(1, inner):
        give_step(i).wait_recv()
    for i in range(inner):
        v = lax.dot_general(
            steps[i], choose, (((0,), (0,)), ((), ())), preferred_element_type=f32
        )
        dt = jnp.maximum(v, 0.0) + jnp.log(1.0 + jnp.exp(-jnp.abs(v)))
        a = dt * rate
        inc = jnp.dot(lower, a, precision=highest, preferred_element_type=f32)
        exc = inc - a
        for k, value in enumerate((inc, exc, dt)):
            turned = value.T
            for q in range(locals_n):
                at = slice(q * columns, (q + 1) * columns)
                cols[k, i, q, :, 0:columns] = value[:, at]
                rows_t[k, i, q, 0:columns, :] = turned[at, :]

    for i in range(1, n):
        for k in range(3):
            give_tap(k, i).wait_recv()

    @pl.when(has_below)
    def _():
        for k in range(3):
            give_halo(0, k, 0).wait_recv()
        halo[0] = halo_in[0].astype(f32)

    @pl.when(has_above)
    def _():
        for k in range(3):
            give_halo(1, k, 0).wait_recv()
        halo[1] = halo_in[1].astype(f32)

    for copy in owned:
        copy.wait()

    def pass_f(q):
        return remote(
            send_f.at[q], got_f.at[q], f_s.at[q], f_r.at[q], {"sp": sp + inner}
        )

    def pass_b(q):
        return remote(
            send_b.at[q], got_b.at[q], b_s.at[q], b_r.at[q], {"sp": sp - inner}
        )

    def onward_f(q, value):
        for i in range(inner):
            value = carry[q, i, 0:1, :] * value + own_f[q, i]
        send_f[q] = value.astype(bf16)
        pass_f(q).start()

    def onward_b(q, value):
        for i in reversed(range(inner)):
            value = carry[q, i, 1:2, :] * value + own_b[q, i]
        send_b[q] = value.astype(bf16)
        pass_b(q).start()

    def local_part(q):
        at = spot(q * lanes, lanes)
        wide_at = spot(x * span + q * lanes, lanes)
        length = inner * tokens
        for k in range(3):
            pad[k, 8 - half : 8, :] = halo[0, k, 8 - half : 8, at]
            pad[k, length + 8 : length + 8 + half, :] = halo[1, k, 0:half, at]
            for i in range(inner):
                pad[k, i * tokens + 8 : (i + 1) * tokens + 8, :] = ins[k, i, :, at].astype(f32)

        def conv(k, i):
            total = None
            for j in range(taps_n):
                first = i * tokens + 8 - half + j
                term = pad[k, first : first + tokens, :] * taps[k, j : j + 1, wide_at]
                total = term if total is None else total + term
            return total * jax.nn.sigmoid(total)

        for i in range(inner):
            xs = conv(0, i)
            write = conv(1, i).astype(bf16)
            read = conv(2, i).astype(bf16)
            reads[q, i] = read
            inc, exc, dt = (cols[k, i, q, :, 0:columns] for k in range(3))
            inct, exct, dtt = (rows_t[k, i, q, 0:columns, :] for k in range(3))
            tot = inc[BLOCK - 1 : BLOCK, :]
            heads = range(per_group)
            fwd = [inc[:, 2 * h : 2 * h + 1] for h in heads]
            bwd = [exc[:, 2 * h + 1 : 2 * h + 2] for h in heads]
            tot_f = [tot[:, 2 * h : 2 * h + 1] for h in heads]
            tot_b = [tot[:, 2 * h + 1 : 2 * h + 2] for h in heads]
            wf = spread_heads(
                [dt[:, 2 * h : 2 * h + 1] * jnp.exp(fwd[h] - tot_f[h]) for h in heads]
            )
            wb = spread_heads([dt[:, 2 * h + 1 : 2 * h + 2] * jnp.exp(-bwd[h]) for h in heads])
            both = jnp.concatenate([(xs * wf).astype(bf16), (xs * wb).astype(bf16)], axis=1)
            sums = lax.dot_general(
                write, both, (((0,), (0,)), ((), ())), preferred_element_type=f32
            )
            own_f[q, i] = sums[:, 0:lanes]
            own_b[q, i] = sums[:, lanes : 2 * lanes]
            carry[q, i, 0:1, :] = spread_heads([jnp.exp(-tot_f[h]) for h in heads])
            carry[q, i, 1:2, :] = spread_heads([jnp.exp(-tot_b[h]) for h in heads])
            fade_f[q, i] = spread_heads([jnp.exp(-fwd[h]) for h in heads])
            fade_b[q, i] = spread_heads([jnp.exp(bwd[h] - tot_b[h]) for h in heads])
            scores = lax.dot_general(
                read, write, (((1,), (1,)), ((), ())), preferred_element_type=f32
            )
            inside = None
            for h in heads:
                f, b = 2 * h, 2 * h + 1
                power = jnp.where(
                    li >= si,
                    inct[f : f + 1, :] - inc[:, f : f + 1],
                    exc[:, b : b + 1] - exct[b : b + 1, :],
                )
                df, db = dtt[f : f + 1, :], dtt[b : b + 1, :]
                scale = jnp.where(li > si, df, jnp.where(li == si, df + db, db))
                weights = (scores * jnp.exp(power) * scale).astype(bf16)
                xh = jnp.where(lane_head == h, xs, 0.0).astype(bf16)
                term = jnp.dot(weights, xh, preferred_element_type=f32)
                inside = term if inside is None else inside + term
            inside_ref[q, i] = inside

        @pl.when(has_above & jnp.logical_not(has_below))
        def _():
            onward_f(q, jnp.zeros((STATE, lanes), f32))

        @pl.when(has_below & jnp.logical_not(has_above))
        def _():
            onward_b(q, jnp.zeros((STATE, lanes), f32))

    def give_y(q, to):
        i = lax.rem(to - x + inner, inner)
        return remote(
            ybuf.at[q, to], ytok.at[:, spot((x * locals_n + q) * lanes, lanes)],
            y_s.at[i, q], y_r.at[i, q], {"sp": z * inner + to},
        )

    def finish(q):
        enter_f, enter_b = [], [None] * inner
        value = got_f[q].astype(f32)
        for i in range(inner):
            enter_f.append(value.astype(bf16))
            if i < inner - 1:
                value = carry[q, i, 0:1, :] * value + own_f[q, i]
        value = got_b[q].astype(f32)
        for i in reversed(range(inner)):
            enter_b[i] = value.astype(bf16)
            if i > 0:
                value = carry[q, i, 1:2, :] * value + own_b[q, i]
        for i in range(inner):
            entering = jnp.concatenate([enter_f[i], enter_b[i]], axis=1)
            moved = jnp.dot(reads[q, i], entering, preferred_element_type=f32)
            total = (
                inside_ref[q, i]
                + moved[:, 0:lanes] * fade_f[q, i]
                + moved[:, lanes : 2 * lanes] * fade_b[q, i]
            )
            ybuf[q, i] = total.astype(bf16)

            @pl.when(x == i)
            def _():
                ytok[:, spot((x * locals_n + q) * lanes, lanes)] = ybuf[q, i]

            @pl.when(x != i)
            def _():
                give_y(q, i).start()

    gap = 2
    late_f = gap * z
    late_b = gap * (planes - 1 - z)
    late = jnp.maximum(late_f, late_b)

    def turn(t, unused):
        f, b, g = t - late_f, t - late_b, t - late

        @pl.when(t < locals_n)
        def _():
            for k in range(3):
                for i in range(1, inner):
                    give_in(k, t, i).wait_recv()
            local_part(t)

        @pl.when(t == 3 * locals_n // 4)
        def _():
            for offset in across:
                weight_in(offset, shared)
                for bit in between(offset) + [0, 1]:
                    give_weight(offset, bit, shared).start()

        @pl.when(has_below & (f >= 0) & (f < locals_n))
        def _():
            pass_f(f).wait_recv()

            @pl.when(has_above)
            def _():
                onward_f(f, got_f[f].astype(f32))

        @pl.when(has_above & (b >= 0) & (b < locals_n))
        def _():
            pass_b(b).wait_recv()

            @pl.when(has_below)
            def _():
                onward_b(b, got_b[b].astype(f32))

        @pl.when((g >= 0) & (g < locals_n))
        def _():
            finish(g)

        return unused

    lax.fori_loop(0, locals_n + gap * (planes - 1), turn, 0)

    per_norm = groups // NORM_GROUPS
    squares[...] = jnp.zeros(squares.shape, f32)
    for copy in late_loads:
        copy.wait()

    def gate_group(g, unused):
        owner, q = g // locals_n, lax.rem(g, locals_n)

        @pl.when(owner != x)
        def _():
            i = lax.rem(x - owner + inner, inner)
            remote(
                ybuf.at[q, 0], ytok.at[:, spot(g * lanes, lanes)],
                y_s.at[i, q], y_r.at[i, q], {"sp": z * inner + owner},
            ).wait_recv()

        at = spot(g * lanes, lanes)
        gate = gate_v[:, at].astype(f32)
        value = ytok[:, at].astype(f32) * (gate * jax.nn.sigmoid(gate))
        gated[g] = value
        squares[g // per_norm] += jnp.sum(value * value, axis=1, keepdims=True)
        return unused

    lax.fori_loop(0, groups, gate_group, 0)

    def scale(g, unused):
        at = spot(g * lanes, lanes)
        mean = squares[g // per_norm] * (1.0 / (per_norm * lanes))
        value = gated[g] * lax.rsqrt(mean + epsilon) * gain_ref[:, at]
        mixed[:, at] = value.astype(bf16)
        return unused

    lax.fori_loop(0, groups, scale, 0)

    stream_ref[...] = res_v[...].astype(f32)

    def come(offset, c, onward):
        weight_in(offset, c)
        for bit in onward:
            give_weight(offset, bit, c).start()

    def project(offset, first, last):
        block = dp
        for bit in bits:
            if offset & bit:
                block = block + bit * (1 - 2 * lax.rem(dp // bit, 2))
        part = mixed[:, pl.ds(pl.multiple_of(block * depth + first, 128), last - first)]

        def tile(t, unused):
            at = spot(t * 512, 512)
            stream_ref[:, at] += jnp.dot(
                part, w_all[offset, first:last, at], preferred_element_type=f32
            )
            return unused

        lax.fori_loop(0, width // 512, tile, 0)

    early = depth - 2 * piece
    odd = range(1, dp_count, 2)
    for offset in across:
        for c in range(1, pieces - 2):
            come(offset, c, between(offset) + [1])
        come(offset, missing, [1])
    for offset in odd:
        for c in list(range(pieces - 2)) + [pieces - 1]:
            come(offset, c, [])
    project(0, 0, depth)
    if early:
        for offset in range(1, dp_count):
            project(offset, 0, early)
    for offset in across:
        come(offset, pieces - 2, between(offset) + [1])
        project(offset, early, depth)
    for offset in odd:
        come(offset, pieces - 2, [])
        project(offset, early, depth)
    total = jnp.zeros((tokens, 1), f32)
    for at in range(0, width, 512):
        value = stream_ref[:, at : at + 512]
        total = total + jnp.sum(value * value, axis=1, keepdims=True)
    root = lax.rsqrt(total * (1.0 / width) + epsilon)
    for at in range(0, width, 512):
        value = stream_ref[:, at : at + 512] * root * ffn_gain_ref[:, at : at + 512]
        ffn_ref[:, at : at + 512] = value.astype(bf16)

    for i in range(1, inner):
        give_step(i).wait_send()
    for i in range(1, n):
        for k in range(3):
            give_tap(k, i).wait_send()
        give_rate(i).wait_send()

    @pl.when(sends_up)
    def _():
        for k in range(3):
            for to in range(inner):
                give_halo(0, k, to).wait_send()

    @pl.when(sends_down)
    def _():
        for k in range(3):
            for to in range(inner):
                give_halo(1, k, to).wait_send()

    def drain(q, unused):
        for k in range(3):
            for i in range(1, inner):
                give_in(k, q, i).wait_send()
        for i in range(1, inner):
            give_y(q, lax.rem(x + i, inner)).wait_send()

        @pl.when(has_above)
        def _():
            pass_f(q).wait_send()

        @pl.when(has_below)
        def _():
            pass_b(q).wait_send()

        return unused

    lax.fori_loop(0, locals_n, drain, 0)
    for offset in [0] + across:
        for c in [shared] + list(range(1, pieces - 1)):
            for bit in between(offset) if offset else bits[1:]:
                give_weight(offset, bit, c).wait_send()
        for c in range(pieces):
            give_weight(offset, 1, c).wait_send()
        if offset:
            give_weight(offset, 0, shared).wait_send()


def mixer(
    n, inner, dp_count, signal, write, read, gate, residual, weight, steps,
    conv_x, conv_b, conv_c, rates, gain, ffn_gain,
):
    f32, bf16 = jnp.float32, jnp.bfloat16
    tokens, width = signal.shape
    groups = write.shape[1] // STATE
    lanes = width // groups
    own = groups // inner
    span = width // inner
    depth = weight.shape[0]
    pieces = depth // min(depth, 64)
    bits = dp_count.bit_length() - 1
    inside = pl.BlockSpec(memory_space=pltpu.VMEM)
    anywhere = pl.BlockSpec(memory_space=pl.ANY)
    dma = pltpu.SemaphoreType.DMA
    vmem = pltpu.VMEM
    tile = vmem((own, inner, tokens, lanes), f32)
    state = vmem((own, inner, STATE, lanes), f32)
    small = vmem((own, STATE, lanes), bf16)
    flat = vmem((tokens, width), bf16)
    return pl.pallas_call(
        functools.partial(mixer_kernel, n, inner, dp_count),
        out_shape=(
            jax.ShapeDtypeStruct((tokens, width), f32),
            jax.ShapeDtypeStruct((tokens, width), bf16),
        ),
        in_specs=[anywhere] * 6 + [inside] * 7,
        out_specs=(inside, inside),
        scratch_shapes=[
            vmem((3, inner, tokens, span), bf16), flat, flat,
            vmem((dp_count, depth, width), bf16),
            vmem((inner,) + steps.shape, bf16),
            vmem((3, 8, width), f32),
            vmem((n,) + rates.shape, f32),
            vmem((2, 3, 8, span), bf16),
            vmem((2, 3, 8, span), f32),
            vmem((3, inner * tokens + 16, lanes), f32),
            vmem((own, inner, tokens, STATE), bf16),
            tile, tile, tile, state, state,
            vmem((own, inner, 8, lanes), f32),
            small, small, small, small,
            vmem((own, inner, tokens, lanes), bf16), flat,
            vmem((groups, tokens, lanes), f32), flat,
            vmem((3, inner, own, tokens, 8), f32),
            vmem((3, inner, own, 8, tokens), f32),
            vmem((NORM_GROUPS, tokens, 1), f32),
            dma((3, own, inner)), dma((3, own, inner)), dma((inner,)), dma((inner,)),
            dma((3, n)), dma((3, n)), dma((n,)), dma((n,)), dma((2, 3, inner)), dma((2, 3)),
            dma((own,)), dma((own,)), dma((own,)), dma((own,)),
            dma((inner, own)), dma((inner, own)),
            dma((dp_count, bits + 1, pieces)), dma((dp_count, pieces)), dma((3,)), dma((8,)),
        ],
        compiler_params=pltpu.CompilerParams(
            collective_id=1, has_side_effects=True, vmem_limit_bytes=56 * 1024 * 1024
        ),
        cost_estimate=pl.CostEstimate(
            flops=40 * 10**9, bytes_accessed=4 * tokens * width * 2, transcendentals=0
        ),
        name="mixer",
    )(
        signal, write, read, gate, residual, weight, steps, conv_x, conv_b, conv_c, rates,
        gain.reshape(1, width), ffn_gain.reshape(1, width),
    )


def per_device(
    residual_in, ssm_input, state_b, state_c, step_raw, gate_input, conv_x, conv_b, conv_c,
    decay_rate, mix_gain, out_weight, ffn_gain, routing, route_weight, gate_w, up_w, down_w,
):
    sp_count = lax.axis_size("sp")
    dp_count = lax.axis_size("dp")
    inner = dp_count // 2
    token_count = residual_in.shape[1]
    stream, ffn_input = mixer(
        sp_count, inner, dp_count, ssm_input[0], state_b[0], state_c[0], gate_input[0],
        residual_in[0], out_weight, step_raw[0].T, conv_x, conv_b, conv_c, decay_rate,
        mix_gain, ffn_gain,
    )
    top_count = routing.shape[2]
    planes = sp_count // inner
    capacity = 4 * token_count * top_count // (2 * sp_count * dp_count)
    return experts(
        planes, inner, dp_count, capacity, ffn_input, stream, routing[0].T, route_weight[0].T,
        gate_w, up_w, down_w,
    )[None]


def solution(mesh):
    return jax.shard_map(
        per_device,
        mesh=mesh,
        in_specs=(
            P("dp", "sp", None),
            P("dp", "sp", None),
            P("dp", "sp", None),
            P("dp", "sp", None),
            P("dp", "sp", None),
            P("dp", "sp", None),
            P(None, "sp"),
            P(None, "sp"),
            P(None, "sp"),
            P(None, "sp"),
            P(),
            P("dp", None),
            P(),
            P("dp", "sp", None),
            P("dp", "sp", None),
            P(("sp", "dp"), None, None),
            P(("sp", "dp"), None, None),
            P(("sp", "dp"), None, None),
        ),
        out_specs=P("dp", "sp", None),
        check_vma=False,
    )
```

```python
import functools

import jax
import jax.numpy as jnp
from jax import lax
from jax.experimental import pallas as pl
from jax.experimental.pallas import tpu as pltpu
from jax.sharding import PartitionSpec as P

HEAD_DIM = 64
STATE = 128
BLOCK = 128
NORM_GROUPS = 4
MESH = pl.DeviceIdType.MESH

highest = lax.Precision.HIGHEST
epsilon = 1e-05
clamp_limit = 7.0
sigmoid_slope = 1.702


def greet(peers):
    barrier = pltpu.get_barrier_semaphore()
    for peer in peers:
        pl.semaphore_signal(barrier, inc=1, device_id=peer, device_id_type=MESH)
    pl.semaphore_wait(barrier, len(peers))


def plane_order(z, planes, s):
    below, above = z, planes - 1 - z
    both = jnp.minimum(below, above)
    near = (s + 1) // 2
    low = jnp.where(below < above, 1, 0)
    turn = jnp.where(low == 1, s % 2, 1 - s % 2)
    from_below = jnp.where(s <= 2 * both, turn, 1 - low)
    hops = jnp.where(s <= 2 * both, near, s - both)
    return hops, from_below, z + hops * (1 - 2 * from_below)


def experts_kernel(
    planes, inner, dp_count, top, x_ref, stream_ref, names_ref, shares_ref, gate_hbm, up_hbm,
    down_hbm, out_ref, gate, up, down, tok, names_in, shares_in, rows_out, rows_in, made, back, high, low, active, part, part_in,
    total, passing, wsem, isend, irecv, zsend, zrecv, dsend, drecv, rsend, rrecv, psend, precv,
    csend, crecv, local,
):
    f32, bf16 = jnp.float32, jnp.bfloat16
    near = inner * dp_count
    tokens, width = x_ref.shape
    cap = rows_out.shape[2]
    sp, dp = lax.axis_index("sp"), lax.axis_index("dp")
    z, x = sp // inner, lax.rem(sp, inner)
    me = x * dp_count + dp

    def place(p):
        return {"sp": z * inner + p // dp_count, "dp": lax.rem(p, dp_count)}

    def plane(other):
        return {"sp": other * inner + x, "dp": dp}

    barrier = pltpu.get_barrier_semaphore()

    def call(i, carry):
        peer = lax.rem(me + i, near)
        pl.semaphore_signal(barrier, inc=1, device_id=place(peer), device_id_type=MESH)
        return carry

    lax.fori_loop(1, near, call, 0)
    for i in range(1, planes):
        pl.semaphore_signal(
            barrier, inc=1, device_id=plane(lax.rem(z + i, planes)), device_id_type=MESH
        )
    loads = [
        pltpu.make_async_copy(gate_hbm.at[0], gate, wsem.at[0]),
        pltpu.make_async_copy(up_hbm.at[0], up, wsem.at[1]),
        pltpu.make_async_copy(down_hbm.at[0], down, wsem.at[2]),
    ]
    for load in loads:
        load.start()
    pl.semaphore_wait(barrier, near - 1 + planes - 1)

    def tell(kind, i):
        return pltpu.make_async_remote_copy(
            src_ref=(names_ref, shares_ref)[kind],
            dst_ref=(names_in, shares_in)[kind].at[z],
            send_sem=isend.at[kind, i],
            recv_sem=irecv.at[kind, i],
            device_id=plane(lax.rem(z + i, planes)),
            device_id_type=MESH,
        )

    for i in range(1, planes):
        for kind in range(2):
            tell(kind, i).start()

    parts_n = 2
    share = width // parts_n

    def along(src, block, step, way, c):
        cut = slice(c * share, (c + 1) * share)
        return pltpu.make_async_remote_copy(
            src_ref=src.at[:, cut],
            dst_ref=tok.at[block, :, cut],
            send_sem=zsend.at[way, step, c],
            recv_sem=zrecv.at[way, step, c],
            device_id=plane(z + 1 - 2 * way),
            device_id_type=MESH,
        )

    up_open, down_open = z < planes - 1, z > 0

    @pl.when(up_open)
    def _():
        for c in range(parts_n):
            along(x_ref, z, 0, 0, c).start()

    @pl.when(down_open)
    def _():
        for c in range(parts_n):
            along(x_ref, z, 0, 1, c).start()

    ti = lax.broadcasted_iota(jnp.int32, (tokens, tokens), 0)
    tj = lax.broadcasted_iota(jnp.int32, (tokens, tokens), 1)
    earlier = jnp.where(ti < tj, 1.0, 0.0).astype(bf16)
    expert = z * near + lax.broadcasted_iota(jnp.int32, (near, tokens), 0)
    place_in = lax.broadcasted_iota(jnp.int32, (near, cap, tokens), 1).astype(f32)

    def send_rows(block, i, c):
        peer = lax.rem(me + i, near)
        cut = slice(c * share, (c + 1) * share)
        return pltpu.make_async_remote_copy(
            src_ref=rows_out.at[block, peer, :, cut],
            dst_ref=rows_in.at[block, me, :, cut],
            send_sem=dsend.at[block, i, c],
            recv_sem=drecv.at[block, i, c],
            device_id=place(peer),
            device_id_type=MESH,
        )

    def keep_rows(block):
        return pltpu.make_async_copy(
            rows_out.at[block, me], rows_in.at[block, me], local.at[0, block]
        )

    def send_back(block, i):
        peer = lax.rem(me + i, near)
        return pltpu.make_async_remote_copy(
            src_ref=made.at[block, peer],
            dst_ref=back.at[block, me],
            send_sem=rsend.at[block, i],
            recv_sem=rrecv.at[block, i],
            device_id=place(peer),
            device_id_type=MESH,
        )

    def keep_back(block):
        return pltpu.make_async_copy(made.at[block, me], back.at[block, me], local.at[1, block])

    def each(what):
        def one(i, carry):
            what(i)
            return carry

        lax.fori_loop(1, near, one, 0)

    def choose(block, names, weights):
        named, weight = None, None
        for k in range(top):
            hit = names[k : k + 1, :] == expert
            one = jnp.where(hit, 1.0, 0.0)
            share = jnp.where(hit, weights[k : k + 1, :], 0.0)
            named = one if named is None else named + one
            weight = share if weight is None else weight + share
        slot = jnp.dot(named.astype(bf16), earlier, preferred_element_type=f32)
        slot = jnp.where(named > 0.5, slot, -1.0)
        pick = slot[:, None, :] == place_in
        rough = weight.astype(bf16).astype(f32)
        rest = weight - rough

        def table(v):
            return jnp.where(pick, v, 0.0).reshape(near * cap, tokens).astype(bf16)

        high[block] = table(rough[:, None, :])
        low[block] = table(rest[:, None, :])
        return table(jnp.ones((near, 1, tokens), f32))

    def dispatch(block, select, ref, c):
        for at in range(c * share, (c + 1) * share, 512):
            rows = jnp.dot(select, ref[:, at : at + 512], preferred_element_type=f32)
            rows_out[block, :, :, at : at + 512] = rows.astype(bf16).reshape(near, cap, 512)
        each(lambda i: send_rows(block, i, c).start())
        if c == parts_n - 1:
            keep_rows(block).start()

    def arrive(s):
        hops, from_below, block = plane_order(z, planes, s)
        way = 1 - from_below
        onward = jnp.where(from_below == 1, z + 1, z - 1)
        source = lax.rem(z - block + planes, planes)
        for kind in range(2):
            tell(kind, source).wait_recv()
        select = choose(block, names_in[block], shares_in[block])
        for c in range(parts_n):
            along(tok.at[block], block, hops - 1, way, c).wait_recv()

            @pl.when((onward >= 0) & (onward < planes))
            def _():
                along(tok.at[block], block, hops, way, c).start()

            dispatch(block, select, tok.at[block], c)
        return block

    hidden = gate.shape[1]
    flat = near * cap

    def serve(block):
        keep_rows(block).wait()
        for c in range(parts_n):
            each(lambda i: send_rows(block, i, c).wait_recv())
        tile = 256

        def lift(n, carry):
            cols = pl.ds(pl.multiple_of(n * tile, tile), tile)
            rows = rows_in[block].reshape(flat, width)
            g = jnp.minimum(jnp.dot(rows, gate[:, cols], preferred_element_type=f32), clamp_limit)
            u = jnp.dot(rows, up[:, cols], preferred_element_type=f32)
            u = jnp.clip(u, -clamp_limit, clamp_limit)
            active[:, cols] = ((u + 1.0) * g * jax.nn.sigmoid(sigmoid_slope * g)).astype(bf16)
            return carry

        lax.fori_loop(0, hidden // tile, lift, 0)

        def lower(n, carry):
            cols = pl.ds(pl.multiple_of(n * tile, tile), tile)
            y = jnp.dot(active[...], down[:, cols], preferred_element_type=f32)
            made[block, :, :, cols] = y.astype(bf16).reshape(near, cap, tile)
            return carry

        lax.fori_loop(0, width // tile, lower, 0)

    def give(block):
        each(lambda i: send_back(block, i).start())
        keep_back(block).start()

    def gathered(block, at, chunk):
        rows = back[block, :, :, at : at + chunk].reshape(flat, chunk)
        dims = (((0,), (0,)), ((), ()))
        return lax.dot_general(
            high[block], rows, dims, preferred_element_type=f32
        ) + lax.dot_general(low[block], rows, dims, preferred_element_type=f32)

    chunk = 512
    chunks = width // chunk

    def send_part(block, i, c):
        return pltpu.make_async_remote_copy(
            src_ref=part.at[block, :, c * chunk : (c + 1) * chunk],
            dst_ref=part_in.at[z, :, c * chunk : (c + 1) * chunk],
            send_sem=psend.at[i, c],
            recv_sem=precv.at[i, c],
            device_id=plane(block),
            device_id_type=MESH,
        )

    middle = planes // 2
    in_low = z < middle
    outermost = (z == 0) | (z == planes - 1)
    innermost = (z == middle - 1) | (z == middle)
    inward = jnp.where(in_low, z + 1, z - 1)

    def is_far(block):
        return in_low == (block >= middle)

    def pass_on(block, c):
        slot = lax.rem(block, middle)
        return pltpu.make_async_remote_copy(
            src_ref=part.at[block, :, c * chunk : (c + 1) * chunk],
            dst_ref=passing.at[slot, :, c * chunk : (c + 1) * chunk],
            send_sem=csend.at[slot, c],
            recv_sem=crecv.at[slot, c],
            device_id=plane(inward),
            device_id_type=MESH,
        )

    def landed(block):
        keep_back(block).wait()
        each(lambda i: send_back(block, i).wait_recv())

    def collect(block):
        landed(block)
        adds = is_far(block) & jnp.logical_not(outermost)
        inner_far = is_far(block) & jnp.logical_not(innermost)
        slot = lax.rem(block, middle)
        for c in range(chunks):
            at = c * chunk

            @pl.when(adds)
            def _():
                pass_on(block, c).wait_recv()
                value = gathered(block, at, chunk) + passing[slot, :, at : at + chunk].astype(f32)
                part[block, :, at : at + chunk] = value.astype(bf16)

            @pl.when(jnp.logical_not(adds))
            def _():
                part[block, :, at : at + chunk] = gathered(block, at, chunk).astype(bf16)

            @pl.when(inner_far)
            def _():
                pass_on(block, c).start()

            @pl.when(jnp.logical_not(inner_far))
            def _():
                send_part(block, lax.rem(block - z + planes, planes), c).start()

    blocks = [z]
    select = choose(z, names_ref[...], shares_ref[...])
    for c in range(parts_n):
        dispatch(z, select, x_ref, c)
    served = 0
    for s in range(1, planes):
        blocks.append(arrive(s))
        if s == planes - 2:
            for load in loads:
                load.wait()
            serve(blocks[0])
            served = 1
    if not served:
        for load in loads:
            load.wait()
        serve(blocks[0])
    last = list(range(middle, planes))
    first = list(range(1, middle))
    for s in last[:-1]:
        serve(blocks[s])
        give(blocks[s])
    for s in first:
        serve(blocks[s])
    for s in last[-1:]:
        serve(blocks[s])
        give(blocks[s])
    for s in first:
        give(blocks[s])
    give(blocks[0])
    for s in last + first:
        collect(blocks[s])
    landed(z)
    for at in range(0, width, chunk):
        cols = slice(at, at + chunk)
        total[:, cols] = stream_ref[:, cols] + gathered(z, at, chunk)

    def comes(source):
        near_by = jnp.logical_not(is_far(source))
        edge = (source == middle - 1) | (source == middle)
        return near_by | edge

    for i in range(1, planes):
        source = lax.rem(z - i + planes, planes)

        @pl.when(comes(source))
        def _():
            for c in range(chunks):
                cols = slice(c * chunk, (c + 1) * chunk)
                send_part(lax.rem(z + i, planes), i, c).wait_recv()
                total[:, cols] += part_in[source, :, cols].astype(f32)

    out_ref[...] = total[...].astype(bf16)
    for i in range(1, planes):
        for kind in range(2):
            tell(kind, i).wait_send()
        block = lax.rem(z + i, planes)
        inner_far = is_far(block) & jnp.logical_not(innermost)

        @pl.when(inner_far)
        def _():
            for c in range(chunks):
                pass_on(block, c).wait_send()

        @pl.when(jnp.logical_not(inner_far))
        def _():
            for c in range(chunks):
                send_part(block, i, c).wait_send()

    for block in range(planes):
        for c in range(parts_n):
            each(lambda i: send_rows(block, i, c).wait_send())
        each(lambda i: send_back(block, i).wait_send())

    @pl.when(up_open)
    def _():
        for c in range(parts_n):
            along(x_ref, z, 0, 0, c).wait_send()

    @pl.when(down_open)
    def _():
        for c in range(parts_n):
            along(x_ref, z, 0, 1, c).wait_send()

    for step in range(1, planes):

        @pl.when(up_open & (z - step >= 0))
        def _():
            for c in range(parts_n):
                along(tok.at[z], z, step, 0, c).wait_send()

        @pl.when(down_open & (z + step < planes))
        def _():
            for c in range(parts_n):
                along(tok.at[z], z, step, 1, c).wait_send()


def experts(
    planes, inner, dp_count, cap, tokens_in, stream, names, shares, gate_w, up_w, down_w
):
    near = inner * dp_count
    tokens, width = tokens_in.shape
    hidden = gate_w.shape[2]
    bf16, f32 = jnp.bfloat16, jnp.float32
    anywhere = pl.BlockSpec(memory_space=pl.ANY)
    inside = pl.BlockSpec(memory_space=pltpu.VMEM)
    dma = pltpu.SemaphoreType.DMA
    rows = pltpu.VMEM((planes, near, cap, width), bf16)
    table = pltpu.VMEM((planes, near * cap, tokens), bf16)
    blocks = pltpu.VMEM((planes, tokens, width), bf16)
    return pl.pallas_call(
        functools.partial(experts_kernel, planes, inner, dp_count, names.shape[0]),
        out_shape=jax.ShapeDtypeStruct((tokens, width), bf16),
        in_specs=[inside] * 4 + [anywhere] * 3,
        out_specs=inside,
        scratch_shapes=[
            pltpu.VMEM((width, hidden), bf16),
            pltpu.VMEM((width, hidden), bf16),
            pltpu.VMEM((hidden, width), bf16),
            blocks,
            pltpu.VMEM((planes,) + names.shape, names.dtype),
            pltpu.VMEM((planes,) + shares.shape, f32),
            rows, rows, rows, rows, table, table,
            pltpu.VMEM((near * cap, hidden), bf16),
            blocks, blocks,
            pltpu.VMEM((tokens, width), f32),
            pltpu.VMEM((planes // 2, tokens, width), bf16),
            dma((3,)), dma((2, planes)), dma((2, planes)),
            dma((2, planes, 2)), dma((2, planes, 2)), dma((planes, near, 2)),
            dma((planes, near, 2)), dma((planes, near)), dma((planes, near)),
            dma((planes, width // 512)), dma((planes, width // 512)),
            dma((planes // 2, width // 512)), dma((planes // 2, width // 512)), dma((2, planes)),
        ],
        compiler_params=pltpu.CompilerParams(
            collective_id=3, has_side_effects=True, vmem_limit_bytes=60 * 1024 * 1024
        ),
        cost_estimate=pl.CostEstimate(flops=10**11, bytes_accessed=10**8, transcendentals=0),
        name="experts",
    )(tokens_in, stream, names, shares, gate_w, up_w, down_w)


def lowest(offset):
    return offset & -offset


def mixer_kernel(
    n, inner, dp_count, x_hbm, b_hbm, c_hbm, z_hbm, r_hbm, w_hbm, step_ref, tx_ref, tb_ref, tc_ref,
    rate_ref, gain_ref, ffn_gain_ref, stream_ref, ffn_ref,
    ins, gate_v, res_v, w_all, steps, taps, rates, halo_in, halo, pad, reads, inside_ref,
    fade_f, fade_b, own_f, own_b, carry, send_f, send_b, got_f, got_b, ybuf, ytok, gated, mixed,
    cols, rows_t, squares,
    in_s, in_r, step_s, step_r, tap_s, tap_r, rate_s, rate_r, halo_s, halo_r,
    f_s, f_r, b_s, b_r, y_s, y_r, w_s, w_r, own_in, local,
):
    f32, bf16 = jnp.float32, jnp.bfloat16
    sp, dp = lax.axis_index("sp"), lax.axis_index("dp")
    z, x = sp // inner, lax.rem(sp, inner)
    planes = n // inner
    tokens, width = stream_ref.shape
    span = ins.shape[3]
    locals_n = own_f.shape[0]
    lanes = span // locals_n
    groups = locals_n * inner
    per_group = lanes // HEAD_DIM
    columns = 2 * per_group
    taps_n, wide = tx_ref.shape
    half = taps_n // 2
    depth = w_hbm.shape[0]
    piece = min(depth, 64)
    pieces = depth // piece
    bits = [1 << i for i in range(dp_count.bit_length() - 1)]
    flows = (x_hbm, b_hbm, c_hbm)
    tap_refs = (tx_ref, tb_ref, tc_ref)

    def mate(bit):
        return dp + bit * (1 - 2 * lax.rem(dp // bit, 2))

    greet([{"sp": lax.rem(sp + i, n)} for i in range(1, n)] + [{"dp": mate(b)} for b in bits])

    def remote(src, dst, send, recv, where):
        return pltpu.make_async_remote_copy(
            src_ref=src, dst_ref=dst, send_sem=send, recv_sem=recv,
            device_id=where, device_id_type=MESH,
        )

    def spot(start, size):
        return pl.ds(pl.multiple_of(start, size), size)

    def give_step(i):
        return remote(
            step_ref, steps.at[x], step_s.at[i], step_r.at[i],
            {"sp": z * inner + lax.rem(x + i, inner)},
        )

    mine = spot(sp * wide, wide)

    def give_tap(k, i):
        return remote(
            tap_refs[k], taps.at[k, 0:taps_n, mine], tap_s.at[k, i], tap_r.at[k, i],
            {"sp": lax.rem(sp + i, n)},
        )

    def give_rate(i):
        return remote(
            rate_ref, rates.at[sp], rate_s.at[i], rate_r.at[i], {"sp": lax.rem(sp + i, n)}
        )

    def give_halo(way, k, to):
        first = 0 if way else tokens - 8
        return remote(
            flows[k].at[first : first + 8, to * span : (to + 1) * span],
            halo_in.at[way, k], halo_s.at[way, k, to], halo_r.at[way, k],
            {"sp": (z + 1 - 2 * way) * inner + to},
        )

    def give_in(k, q, i):
        peer = lax.rem(x + i, inner)
        return remote(
            flows[k].at[:, spot(peer * span + q * lanes, lanes)],
            ins.at[k, x, :, spot(q * lanes, lanes)],
            in_s.at[k, q, i], in_r.at[k, q, i], {"sp": z * inner + peer},
        )

    odd_x = lax.rem(x, 2)
    shared, missing = odd_x * (pieces - 1), (1 - odd_x) * (pieces - 1)
    across = [o for o in range(2, dp_count, 2)]
    across = sorted(across, key=lambda o: (-lowest(o), o))

    def give_weight(offset, bit, c):
        rows = spot(c * piece, piece)
        src = w_hbm.at[rows] if offset == 0 else w_all.at[offset, rows]
        if bit:
            index, there = bits.index(bit), {"dp": mate(bit)}
        else:
            index, there = len(bits), {"sp": sp + 1 - 2 * odd_x}
        return remote(
            src, w_all.at[offset + bit, rows],
            w_s.at[offset, index, c], w_r.at[offset + bit, c], there,
        )

    def weight_in(offset, c):
        rows = spot(c * piece, piece)
        remote(
            w_hbm.at[rows], w_all.at[offset, rows],
            w_s.at[0, 0, c], w_r.at[offset, c], {"dp": mate(1)},
        ).wait_recv()

    def between(offset):
        return [bit for bit in bits if 1 < bit < lowest(offset)]

    has_above, has_below = z < planes - 1, z > 0
    sends_up = has_above & (x == inner - 1)
    sends_down = has_below & (x == 0)

    for i in range(1, inner):
        give_step(i).start()
    for i in range(1, n):
        for k in range(3):
            give_tap(k, i).start()
        give_rate(i).start()

    @pl.when(sends_up)
    def _():
        for k in range(3):
            for to in range(inner):
                give_halo(0, k, to).start()

    @pl.when(sends_down)
    def _():
        for k in range(3):
            for to in range(inner):
                give_halo(1, k, to).start()

    def begin(q, unused):
        for k in range(3):
            for i in range(1, inner):
                give_in(k, q, i).start()
        return unused

    lax.fori_loop(0, locals_n, begin, 0)
    owned = [
        pltpu.make_async_copy(
            flows[k].at[:, spot(x * span, span)], ins.at[k, x], own_in.at[k]
        )
        for k in range(3)
    ]
    for copy in owned:
        copy.start()
    for c in [shared] + list(range(1, pieces - 1)):
        for bit in reversed(bits[1:]):
            give_weight(0, bit, c).start()
    for c in range(pieces):
        give_weight(0, 1, c).start()
    keeps = [
        pltpu.make_async_copy(tap_refs[k], taps.at[k, 0:taps_n, mine], local.at[k])
        for k in range(3)
    ]
    keeps.append(pltpu.make_async_copy(rate_ref, rates.at[sp], local.at[3]))
    keeps.append(pltpu.make_async_copy(step_ref, steps.at[x], local.at[4]))
    for copy in keeps:
        copy.start()
    late_loads = [
        pltpu.make_async_copy(z_hbm, gate_v, local.at[5]),
        pltpu.make_async_copy(r_hbm, res_v, local.at[6]),
        pltpu.make_async_copy(w_hbm, w_all.at[0], local.at[7]),
    ]
    for copy in late_loads:
        copy.start()

    @pl.when(jnp.logical_not(has_below))
    def _():
        halo[0] = jnp.zeros(halo.shape[1:], f32)
        got_f[...] = jnp.zeros(got_f.shape, bf16)

    @pl.when(jnp.logical_not(has_above))
    def _():
        halo[1] = jnp.zeros(halo.shape[1:], f32)
        got_b[...] = jnp.zeros(got_b.shape, bf16)

    li = lax.broadcasted_iota(jnp.int32, (BLOCK, BLOCK), 0)
    si = lax.broadcasted_iota(jnp.int32, (BLOCK, BLOCK), 1)
    lower = jnp.where(li >= si, 1.0, 0.0).astype(f32)
    lane = lax.broadcasted_iota(jnp.int32, (1, lanes), 1)
    lane_head = lane // HEAD_DIM

    def spread_heads(values):
        out = values[0]
        for h in range(1, per_group):
            out = jnp.where(lane_head == h, values[h], out)
        return jnp.broadcast_to(out, (out.shape[0], lanes))

    for copy in keeps:
        copy.wait()
    for i in range(1, n):
        give_rate(i).wait_recv()
    step_columns = step_ref.shape[0]
    window = step_columns // inner
    held = rate_ref.shape[1]
    rate = jnp.zeros((1, BLOCK), f32)
    row_lane = lax.broadcasted_iota(jnp.int32, (1, BLOCK), 1)
    for t in range(planes):
        pair = rates[x * planes + t]
        for h in range(held):
            for d in range(2):
                rate = jnp.where(
                    row_lane == 2 * (t * held + h) + d, pair[d : d + 1, h : h + 1], rate
                )
    choose_row = lax.broadcasted_iota(jnp.int32, (step_columns, BLOCK), 0)
    choose_col = lax.broadcasted_iota(jnp.int32, (step_columns, BLOCK), 1)
    choose = jnp.where((choose_row == x * window + choose_col) & (choose_col < window), 1.0, 0.0)
    choose = choose.astype(bf16)
    for i in range(1, inner):
        give_step(i).wait_recv()
    for i in range(inner):
        v = lax.dot_general(
            steps[i], choose, (((0,), (0,)), ((), ())), preferred_element_type=f32
        )
        dt = jnp.maximum(v, 0.0) + jnp.log(1.0 + jnp.exp(-jnp.abs(v)))
        a = dt * rate
        inc = jnp.dot(lower, a, precision=highest, preferred_element_type=f32)
        exc = inc - a
        for k, value in enumerate((inc, exc, dt)):
            turned = value.T
            for q in range(locals_n):
                at = slice(q * columns, (q + 1) * columns)
                cols[k, i, q, :, 0:columns] = value[:, at]
                rows_t[k, i, q, 0:columns, :] = turned[at, :]

    for i in range(1, n):
        for k in range(3):
            give_tap(k, i).wait_recv()

    @pl.when(has_below)
    def _():
        for k in range(3):
            give_halo(0, k, 0).wait_recv()
        halo[0] = halo_in[0].astype(f32)

    @pl.when(has_above)
    def _():
        for k in range(3):
            give_halo(1, k, 0).wait_recv()
        halo[1] = halo_in[1].astype(f32)

    for copy in owned:
        copy.wait()

    def pass_f(q):
        return remote(
            send_f.at[q], got_f.at[q], f_s.at[q], f_r.at[q], {"sp": sp + inner}
        )

    def pass_b(q):
        return remote(
            send_b.at[q], got_b.at[q], b_s.at[q], b_r.at[q], {"sp": sp - inner}
        )

    def onward_f(q, value):
        for i in range(inner):
            value = carry[q, i, 0:1, :] * value + own_f[q, i]
        send_f[q] = value.astype(bf16)
        pass_f(q).start()

    def onward_b(q, value):
        for i in reversed(range(inner)):
            value = carry[q, i, 1:2, :] * value + own_b[q, i]
        send_b[q] = value.astype(bf16)
        pass_b(q).start()

    def local_part(q):
        at = spot(q * lanes, lanes)
        wide_at = spot(x * span + q * lanes, lanes)
        length = inner * tokens
        for k in range(3):
            pad[k, 8 - half : 8, :] = halo[0, k, 8 - half : 8, at]
            pad[k, length + 8 : length + 8 + half, :] = halo[1, k, 0:half, at]
            for i in range(inner):
                pad[k, i * tokens + 8 : (i + 1) * tokens + 8, :] = ins[k, i, :, at].astype(f32)

        def conv(k, i):
            total = None
            for j in range(taps_n):
                first = i * tokens + 8 - half + j
                term = pad[k, first : first + tokens, :] * taps[k, j : j + 1, wide_at]
                total = term if total is None else total + term
            return total * jax.nn.sigmoid(total)

        for i in range(inner):
            xs = conv(0, i)
            write = conv(1, i).astype(bf16)
            read = conv(2, i).astype(bf16)
            reads[q, i] = read
            inc, exc, dt = (cols[k, i, q, :, 0:columns] for k in range(3))
            inct, exct, dtt = (rows_t[k, i, q, 0:columns, :] for k in range(3))
            tot = inc[BLOCK - 1 : BLOCK, :]
            heads = range(per_group)
            fwd = [inc[:, 2 * h : 2 * h + 1] for h in heads]
            bwd = [exc[:, 2 * h + 1 : 2 * h + 2] for h in heads]
            tot_f = [tot[:, 2 * h : 2 * h + 1] for h in heads]
            tot_b = [tot[:, 2 * h + 1 : 2 * h + 2] for h in heads]
            wf = spread_heads(
                [dt[:, 2 * h : 2 * h + 1] * jnp.exp(fwd[h] - tot_f[h]) for h in heads]
            )
            wb = spread_heads([dt[:, 2 * h + 1 : 2 * h + 2] * jnp.exp(-bwd[h]) for h in heads])
            both = jnp.concatenate([(xs * wf).astype(bf16), (xs * wb).astype(bf16)], axis=1)
            sums = lax.dot_general(
                write, both, (((0,), (0,)), ((), ())), preferred_element_type=f32
            )
            own_f[q, i] = sums[:, 0:lanes]
            own_b[q, i] = sums[:, lanes : 2 * lanes]
            carry[q, i, 0:1, :] = spread_heads([jnp.exp(-tot_f[h]) for h in heads])
            carry[q, i, 1:2, :] = spread_heads([jnp.exp(-tot_b[h]) for h in heads])
            fade_f[q, i] = spread_heads([jnp.exp(-fwd[h]) for h in heads])
            fade_b[q, i] = spread_heads([jnp.exp(bwd[h] - tot_b[h]) for h in heads])
            scores = lax.dot_general(
                read, write, (((1,), (1,)), ((), ())), preferred_element_type=f32
            )
            inside = None
            for h in heads:
                f, b = 2 * h, 2 * h + 1
                power = jnp.where(
                    li >= si,
                    inct[f : f + 1, :] - inc[:, f : f + 1],
                    exc[:, b : b + 1] - exct[b : b + 1, :],
                )
                df, db = dtt[f : f + 1, :], dtt[b : b + 1, :]
                scale = jnp.where(li > si, df, jnp.where(li == si, df + db, db))
                weights = (scores * jnp.exp(power) * scale).astype(bf16)
                xh = jnp.where(lane_head == h, xs, 0.0).astype(bf16)
                term = jnp.dot(weights, xh, preferred_element_type=f32)
                inside = term if inside is None else inside + term
            inside_ref[q, i] = inside

        @pl.when(has_above & jnp.logical_not(has_below))
        def _():
            onward_f(q, jnp.zeros((STATE, lanes), f32))

        @pl.when(has_below & jnp.logical_not(has_above))
        def _():
            onward_b(q, jnp.zeros((STATE, lanes), f32))

    def give_y(q, to):
        i = lax.rem(to - x + inner, inner)
        return remote(
            ybuf.at[q, to], ytok.at[:, spot((x * locals_n + q) * lanes, lanes)],
            y_s.at[i, q], y_r.at[i, q], {"sp": z * inner + to},
        )

    def finish(q):
        enter_f, enter_b = [], [None] * inner
        value = got_f[q].astype(f32)
        for i in range(inner):
            enter_f.append(value.astype(bf16))
            if i < inner - 1:
                value = carry[q, i, 0:1, :] * value + own_f[q, i]
        value = got_b[q].astype(f32)
        for i in reversed(range(inner)):
            enter_b[i] = value.astype(bf16)
            if i > 0:
                value = carry[q, i, 1:2, :] * value + own_b[q, i]
        for i in range(inner):
            entering = jnp.concatenate([enter_f[i], enter_b[i]], axis=1)
            moved = jnp.dot(reads[q, i], entering, preferred_element_type=f32)
            total = (
                inside_ref[q, i]
                + moved[:, 0:lanes] * fade_f[q, i]
                + moved[:, lanes : 2 * lanes] * fade_b[q, i]
            )
            ybuf[q, i] = total.astype(bf16)

            @pl.when(x == i)
            def _():
                ytok[:, spot((x * locals_n + q) * lanes, lanes)] = ybuf[q, i]

            @pl.when(x != i)
            def _():
                give_y(q, i).start()

    gap = 2
    late_f = gap * z
    late_b = gap * (planes - 1 - z)
    late = jnp.maximum(late_f, late_b)

    def turn(t, unused):
        f, b, g = t - late_f, t - late_b, t - late

        @pl.when(t == 3 * locals_n // 4)
        def _():
            for offset in across:
                weight_in(offset, shared)
                for bit in between(offset) + [0, 1]:
                    give_weight(offset, bit, shared).start()

        @pl.when(has_below & (f >= 0) & (f < locals_n))
        def _():
            pass_f(f).wait_recv()

            @pl.when(has_above)
            def _():
                onward_f(f, got_f[f].astype(f32))

        @pl.when(has_above & (b >= 0) & (b < locals_n))
        def _():
            pass_b(b).wait_recv()

            @pl.when(has_below)
            def _():
                onward_b(b, got_b[b].astype(f32))

        @pl.when(t < locals_n)
        def _():
            for k in range(3):
                for i in range(1, inner):
                    give_in(k, t, i).wait_recv()
            local_part(t)

        @pl.when((g >= 0) & (g < locals_n))
        def _():
            finish(g)

        return unused

    lax.fori_loop(0, locals_n + gap * (planes - 1), turn, 0)

    per_norm = groups // NORM_GROUPS
    squares[...] = jnp.zeros(squares.shape, f32)
    for copy in late_loads:
        copy.wait()

    def gate_group(g, unused):
        owner, q = g // locals_n, lax.rem(g, locals_n)

        @pl.when(owner != x)
        def _():
            i = lax.rem(x - owner + inner, inner)
            remote(
                ybuf.at[q, 0], ytok.at[:, spot(g * lanes, lanes)],
                y_s.at[i, q], y_r.at[i, q], {"sp": z * inner + owner},
            ).wait_recv()

        at = spot(g * lanes, lanes)
        gate = gate_v[:, at].astype(f32)
        value = ytok[:, at].astype(f32) * (gate * jax.nn.sigmoid(gate))
        gated[g] = value
        squares[g // per_norm] += jnp.sum(value * value, axis=1, keepdims=True)
        return unused

    lax.fori_loop(0, groups, gate_group, 0)

    def scale(g, unused):
        at = spot(g * lanes, lanes)
        mean = squares[g // per_norm] * (1.0 / (per_norm * lanes))
        value = gated[g] * lax.rsqrt(mean + epsilon) * gain_ref[:, at]
        mixed[:, at] = value.astype(bf16)
        return unused

    lax.fori_loop(0, groups, scale, 0)

    stream_ref[...] = res_v[...].astype(f32)

    def come(offset, c, onward):
        weight_in(offset, c)
        for bit in onward:
            give_weight(offset, bit, c).start()

    def project(offset, first, last):
        block = dp
        for bit in bits:
            if offset & bit:
                block = block + bit * (1 - 2 * lax.rem(dp // bit, 2))
        part = mixed[:, pl.ds(pl.multiple_of(block * depth + first, 128), last - first)]

        def tile(t, unused):
            at = spot(t * 512, 512)
            stream_ref[:, at] += jnp.dot(
                part, w_all[offset, first:last, at], preferred_element_type=f32
            )
            return unused

        lax.fori_loop(0, width // 512, tile, 0)

    early = depth - 2 * piece
    odd = range(1, dp_count, 2)
    for offset in across:
        for c in range(1, pieces - 2):
            come(offset, c, between(offset) + [1])
        come(offset, missing, [1])
    for offset in odd:
        for c in list(range(pieces - 2)) + [pieces - 1]:
            come(offset, c, [])
    project(0, 0, depth)
    if early:
        for offset in range(1, dp_count):
            project(offset, 0, early)
    for offset in across:
        come(offset, pieces - 2, between(offset) + [1])
        project(offset, early, depth)
    for offset in odd:
        come(offset, pieces - 2, [])
        project(offset, early, depth)
    total = jnp.zeros((tokens, 1), f32)
    for at in range(0, width, 512):
        value = stream_ref[:, at : at + 512]
        total = total + jnp.sum(value * value, axis=1, keepdims=True)
    root = lax.rsqrt(total * (1.0 / width) + epsilon)
    for at in range(0, width, 512):
        value = stream_ref[:, at : at + 512] * root * ffn_gain_ref[:, at : at + 512]
        ffn_ref[:, at : at + 512] = value.astype(bf16)

    for i in range(1, inner):
        give_step(i).wait_send()
    for i in range(1, n):
        for k in range(3):
            give_tap(k, i).wait_send()
        give_rate(i).wait_send()

    @pl.when(sends_up)
    def _():
        for k in range(3):
            for to in range(inner):
                give_halo(0, k, to).wait_send()

    @pl.when(sends_down)
    def _():
        for k in range(3):
            for to in range(inner):
                give_halo(1, k, to).wait_send()

    def drain(q, unused):
        for k in range(3):
            for i in range(1, inner):
                give_in(k, q, i).wait_send()
        for i in range(1, inner):
            give_y(q, lax.rem(x + i, inner)).wait_send()

        @pl.when(has_above)
        def _():
            pass_f(q).wait_send()

        @pl.when(has_below)
        def _():
            pass_b(q).wait_send()

        return unused

    lax.fori_loop(0, locals_n, drain, 0)
    for offset in [0] + across:
        for c in [shared] + list(range(1, pieces - 1)):
            for bit in between(offset) if offset else bits[1:]:
                give_weight(offset, bit, c).wait_send()
        for c in range(pieces):
            give_weight(offset, 1, c).wait_send()
        if offset:
            give_weight(offset, 0, shared).wait_send()


def mixer(
    n, inner, dp_count, signal, write, read, gate, residual, weight, steps,
    conv_x, conv_b, conv_c, rates, gain, ffn_gain,
):
    f32, bf16 = jnp.float32, jnp.bfloat16
    tokens, width = signal.shape
    groups = write.shape[1] // STATE
    lanes = width // groups
    own = groups // inner
    span = width // inner
    depth = weight.shape[0]
    pieces = depth // min(depth, 64)
    bits = dp_count.bit_length() - 1
    inside = pl.BlockSpec(memory_space=pltpu.VMEM)
    anywhere = pl.BlockSpec(memory_space=pl.ANY)
    dma = pltpu.SemaphoreType.DMA
    vmem = pltpu.VMEM
    tile = vmem((own, inner, tokens, lanes), f32)
    state = vmem((own, inner, STATE, lanes), f32)
    small = vmem((own, STATE, lanes), bf16)
    flat = vmem((tokens, width), bf16)
    return pl.pallas_call(
        functools.partial(mixer_kernel, n, inner, dp_count),
        out_shape=(
            jax.ShapeDtypeStruct((tokens, width), f32),
            jax.ShapeDtypeStruct((tokens, width), bf16),
        ),
        in_specs=[anywhere] * 6 + [inside] * 7,
        out_specs=(inside, inside),
        scratch_shapes=[
            vmem((3, inner, tokens, span), bf16), flat, flat,
            vmem((dp_count, depth, width), bf16),
            vmem((inner,) + steps.shape, bf16),
            vmem((3, 8, width), f32),
            vmem((n,) + rates.shape, f32),
            vmem((2, 3, 8, span), bf16),
            vmem((2, 3, 8, span), f32),
            vmem((3, inner * tokens + 16, lanes), f32),
            vmem((own, inner, tokens, STATE), bf16),
            tile, tile, tile, state, state,
            vmem((own, inner, 8, lanes), f32),
            small, small, small, small,
            vmem((own, inner, tokens, lanes), bf16), flat,
            vmem((groups, tokens, lanes), f32), flat,
            vmem((3, inner, own, tokens, 8), f32),
            vmem((3, inner, own, 8, tokens), f32),
            vmem((NORM_GROUPS, tokens, 1), f32),
            dma((3, own, inner)), dma((3, own, inner)), dma((inner,)), dma((inner,)),
            dma((3, n)), dma((3, n)), dma((n,)), dma((n,)), dma((2, 3, inner)), dma((2, 3)),
            dma((own,)), dma((own,)), dma((own,)), dma((own,)),
            dma((inner, own)), dma((inner, own)),
            dma((dp_count, bits + 1, pieces)), dma((dp_count, pieces)), dma((3,)), dma((8,)),
        ],
        compiler_params=pltpu.CompilerParams(
            collective_id=1, has_side_effects=True, vmem_limit_bytes=56 * 1024 * 1024
        ),
        cost_estimate=pl.CostEstimate(
            flops=40 * 10**9, bytes_accessed=4 * tokens * width * 2, transcendentals=0
        ),
        name="mixer",
    )(
        signal, write, read, gate, residual, weight, steps, conv_x, conv_b, conv_c, rates,
        gain.reshape(1, width), ffn_gain.reshape(1, width),
    )


def per_device(
    residual_in, ssm_input, state_b, state_c, step_raw, gate_input, conv_x, conv_b, conv_c,
    decay_rate, mix_gain, out_weight, ffn_gain, routing, route_weight, gate_w, up_w, down_w,
):
    sp_count = lax.axis_size("sp")
    dp_count = lax.axis_size("dp")
    inner = dp_count // 2
    token_count = residual_in.shape[1]
    stream, ffn_input = mixer(
        sp_count, inner, dp_count, ssm_input[0], state_b[0], state_c[0], gate_input[0],
        residual_in[0], out_weight, step_raw[0].T, conv_x, conv_b, conv_c, decay_rate,
        mix_gain, ffn_gain,
    )
    top_count = routing.shape[2]
    planes = sp_count // inner
    capacity = 4 * token_count * top_count // (2 * sp_count * dp_count)
    return experts(
        planes, inner, dp_count, capacity, ffn_input, stream, routing[0].T, route_weight[0].T,
        gate_w, up_w, down_w,
    )[None]


def solution(mesh):
    return jax.shard_map(
        per_device,
        mesh=mesh,
        in_specs=(
            P("dp", "sp", None),
            P("dp", "sp", None),
            P("dp", "sp", None),
            P("dp", "sp", None),
            P("dp", "sp", None),
            P("dp", "sp", None),
            P(None, "sp"),
            P(None, "sp"),
            P(None, "sp"),
            P(None, "sp"),
            P(),
            P("dp", None),
            P(),
            P("dp", "sp", None),
            P("dp", "sp", None),
            P(("sp", "dp"), None, None),
            P(("sp", "dp"), None, None),
            P(("sp", "dp"), None, None),
        ),
        out_specs=P("dp", "sp", None),
        check_vma=False,
    )
```
